32 devices in a mesh: sp: 8 (over z, x), tp: 4 (over y, core).
Axes of the slice: x: 2, y: 2, z: 4, core: 2. Of those that a mesh axis runs over, the one named last changes fastest.
Arguments:
- pool_in: bfloat16 [2048, 512], P('sp', 'tp'), may hold values from -6 to 6
- pool_weight: bfloat16 [4, 128, 128], P('tp'), may hold values from -0.5 to 0.5
- pool_scale: float32 [512], P('tp'), may hold values from 0.1 to 1.9
- pool_norm: float32 [512], replicated, may hold values from 0.1 to 1.9
- out_weight: bfloat16 [512, 2048], replicated, may hold values from -0.25 to 0.25
- stream: bfloat16 [2048, 2048], P('sp'), may hold values from -6 to 6
- mix_norm: float32 [2048], replicated, may hold values from 0.1 to 1.9
- ffn_norm: float32 [2048], replicated, may hold values from 0.1 to 1.9
- routes: int32 [2048, 4], P('sp'), may hold values from 0 to 7, all different within a row; in each aligned block of 256 rows (0 to 255, 256 to 511, ...) at most 192 rows name the same one
- route_weights: float32 [2048, 4], P('sp'), may hold values from 0.1 to 1
- w_gate: bfloat16 [8, 2048, 2048], P('sp', None, 'tp'), may hold values from -0.125 to 0.125
- w_up: bfloat16 [8, 2048, 2048], P('sp', None, 'tp'), may hold values from -0.125 to 0.125
- gate_bias: float32 [8, 2048], P('sp', 'tp'), may hold values from -12 to 12
- up_bias: float32 [8, 2048], P('sp', 'tp'), may hold values from -12 to 12
- w_down: bfloat16 [8, 2048, 2048], P('sp', 'tp'), may hold values from -2 to 2
- expert_norm: float32 [2048], P('tp'), may hold values from 0.1 to 1.9
Outputs:
- result: bfloat16 [2048, 2048], P('sp', 'tp')
The draws below stay inside these ranges and needn't reach their ends.
Inputs may be any that keep to these rules, and one draw needn't show every extreme that they name: `routes`: each row names 4 different experts. In each aligned block of 256 tokens no expert is named by more than 192 tokens, a bound that some block reaches.
All inputs are finite; a program needn't handle non-finite values.
Results may differ from the reference program's by a relative error of at most 0.012.
Values may be sent and summed in bfloat16 or wider, within the bound.
A program may use at most 128 MiB of HBM per device.

```python
import math
import jax
import jax.numpy as jnp
import numpy as np
from jax import lax

D = 2048
POOL_WIDTH = 512
GROUPS = 4
GROUP_WIDTH = 128
D_EXPERT = 2048
TOP_K = 4
TOK_DEV = 256
TOKENS = 2048
EXPERTS = 8
CAP = 192
N_SP = 8
N_TP = 4


def draw_w_down(key, part):
    first_key, second_key = jax.random.split(jax.random.fold_in(key, 17))
    raw_normal = jax.random.truncated_normal(first_key, -5.0, 5.0, (EXPERTS, D_EXPERT, D), jnp.float32) * D_EXPERT ** (-0.5)
    block_order = jax.random.permutation(second_key, N_TP).astype(jnp.float32)
    block_scale = 0.6 * jnp.power(3.0, block_order / max(N_TP - 1, 1))
    column_block = jnp.arange(D) * N_TP // D
    return (raw_normal * block_scale[column_block][None, None, :]).astype(jnp.bfloat16)


def shard_levels(rng, shape, cuts, low, high):
    gain, own = 1.0, jax.random.fold_in(rng, 6)
    for dim, parts in cuts:
        draws = jnp.exp(jax.random.uniform(jax.random.fold_in(own, dim), (parts,), jnp.float32, low / len(cuts), high / len(cuts)))
        gain = gain * jnp.repeat(draws, shape[dim] // parts).reshape([-1 if axis == dim else 1 for axis in range(len(shape))])
    return gain


def routed_block(key, own, number, rows, count, top, most, slope):
    ranking = jax.random.permutation(key, count)
    packed, ordinary = portions_of(count, rows * top, most, slope, True), portions_of(count, rows * top, most, slope, False)
    places = jnp.arange(count)

    def named(lengths, rotation):
        used = int((lengths > 0).sum())
        fixed = max(1, used // 4)
        shifted = fixed + (places - fixed + rotation * (used - fixed)) % max(1, count - fixed)
        return jnp.zeros((count,), jnp.int32).at[ranking[jnp.where(places < fixed, places, shifted)]].set(jnp.asarray(lengths, jnp.int32))

    lengths = jnp.where(number % 4 == 0, named(packed, number // 4), named(ordinary, number - number // 4 - 1))
    mixed = jax.random.permutation(jax.random.fold_in(own, 3), count)
    donor, receiver = mixed[0:count // 2 * 2:2], mixed[1:count // 2 * 2:2]
    margin = jnp.minimum(lengths[donor] - 1, most - lengths[receiver]) // 2
    margin = jnp.where((donor == ranking[0]) | (receiver == ranking[0]) | (lengths[receiver] == 0), 0, jnp.maximum(margin, 0))
    shifted = jax.random.randint(jax.random.fold_in(own, 4), (count // 2,), 0, 1 << 20) % (margin + 1)
    lengths = lengths.at[donor].add(-shifted).at[receiver].add(shifted)
    items = jnp.searchsorted(jnp.cumsum(lengths), jnp.arange(rows * top), side="right").astype(jnp.int32)
    listing = items.reshape(top, rows).T
    listing = listing[jax.random.permutation(jax.random.fold_in(own, 1), rows)]
    rotation = jax.random.randint(jax.random.fold_in(own, 2), (rows, 1), 0, top)
    return jnp.take_along_axis(listing, (jnp.arange(top)[None, :] + rotation) % top, axis=1)


def portions_of(number_of, total, limit, skew, full):
    loads = [(1 << 20) // math.isqrt(grade ** skew) + 1 for grade in range(1, number_of + 1)]
    largest = limit if full else min(limit, max(-(-total // number_of), total * loads[0] // sum(loads)))
    least = 1 if total - largest >= number_of - 1 else 0
    given, rest = [largest] + [least] * (number_of - 1), total - largest - least * (number_of - 1)
    while rest > 0:
        candidates = [i for i in range(1, number_of) if given[i] < largest] or [i for i in range(1, number_of) if given[i] < limit]
        mass, left = sum([loads[i] for i in candidates]), rest
        for i in candidates:
            addition = min(limit - given[i], max(1, left * loads[i] // mass), rest)
            given[i] = given[i] + addition
            rest = rest - addition
    return np.array(given)


def noise(stream_key, dims, width, reach, cuts=(), held_as=jnp.bfloat16):
    gain = shard_levels(stream_key, dims, cuts, -0.22, 0.18) if cuts else 1.0
    array = jax.random.normal(stream_key, dims, jnp.float32) * width * gain
    return jnp.minimum(jnp.maximum(array, -reach), reach).astype(held_as)


def setup_inputs(seed: int = 0) -> dict:
    key_list = jax.random.split(jax.random.key(seed), 17)
    pool_in = noise(key_list[0], (TOKENS, POOL_WIDTH), 1.0, 6.0, ((0, 8), (1, 4)))
    pool_weight = noise(key_list[1], (GROUPS, GROUP_WIDTH, GROUP_WIDTH), GROUP_WIDTH ** -0.5, 0.5, ((0, 4),))
    pool_scale = jnp.clip(1.0 + 0.18 * jax.random.normal(key_list[2], (POOL_WIDTH,), jnp.float32), 0.1, 1.9)
    pool_norm = jnp.clip(1.0 + 0.18 * jax.random.normal(key_list[3], (POOL_WIDTH,), jnp.float32), 0.1, 1.9)
    out_weight = noise(key_list[4], (POOL_WIDTH, D), POOL_WIDTH ** -0.5, 0.25)
    stream = noise(key_list[5], (TOKENS, D), 1.0, 6.0, ((0, 8),))
    mix_norm = jnp.clip(1.0 + 0.18 * jax.random.normal(key_list[6], (D,), jnp.float32), 0.1, 1.9)
    ffn_norm = jnp.clip(1.0 + 0.18 * jax.random.normal(key_list[7], (D,), jnp.float32), 0.1, 1.9)
    routes_keys = jax.random.split(jax.random.fold_in(key_list[8], 1), TOKENS // TOK_DEV)
    routes_turns = jax.random.permutation(jax.random.fold_in(key_list[8], 3), TOKENS // TOK_DEV)
    routes = jax.vmap(lambda own, number: routed_block(jax.random.fold_in(key_list[8], 2), own, number, TOK_DEV, EXPERTS, TOP_K, CAP, 2))(routes_keys, routes_turns).reshape((TOKENS, TOP_K))
    route_weights = jnp.clip(jnp.exp(math.log(1.0) - 2.3025851 * jax.random.uniform(key_list[9], (TOKENS, TOP_K), jnp.float32) ** shard_levels(key_list[9], (TOKENS, TOP_K), ((0, 8),), -0.2, 0.2)), 0.1, 1.0)
    w_gate = noise(key_list[10], (EXPERTS, D, D_EXPERT), D ** -0.5, 0.125, ((0, 8), (2, 4)))
    w_up = noise(key_list[11], (EXPERTS, D, D_EXPERT), D ** -0.5, 0.125, ((0, 8), (2, 4)))
    gate_bias = noise(key_list[12], (EXPERTS, D_EXPERT), 3.0, 12.0, ((0, 8), (1, 4)), jnp.float32)
    up_bias = noise(key_list[13], (EXPERTS, D_EXPERT), 3.0, 12.0, ((0, 8), (1, 4)), jnp.float32)
    w_down = draw_w_down(jax.random.fold_in(key_list[16], 71), 0)
    expert_norm = jnp.clip(1.0 + 0.18 * jax.random.normal(key_list[15], (D,), jnp.float32), 0.1, 1.9)
    return dict(pool_in=pool_in, pool_weight=pool_weight, pool_scale=pool_scale, pool_norm=pool_norm, out_weight=out_weight, stream=stream, mix_norm=mix_norm, ffn_norm=ffn_norm, routes=routes, route_weights=route_weights, w_gate=w_gate, w_up=w_up, gate_bias=gate_bias, up_bias=up_bias, w_down=w_down, expert_norm=expert_norm)


epsilon = 1e-06
reach_rows = 8
clamp_limit = 7.0
sigmoid_alpha = 1.702

def rms_scale(values):
    return values * lax.rsqrt(lax.optimization_barrier(jnp.mean(values * values, axis=-1, keepdims=True)) + epsilon)

def clamped_unit(gate_pre, up_pre):
    gate_cut = jnp.minimum(gate_pre, clamp_limit)
    up_cut = jnp.clip(up_pre, -clamp_limit, clamp_limit)
    return ((up_cut + 1.0) * (gate_cut * jax.nn.sigmoid(sigmoid_alpha * gate_cut))).astype(jnp.bfloat16)

def reference(pool_in, pool_weight, pool_scale, pool_norm, out_weight, stream, mix_norm, ffn_norm, routes, route_weights, w_gate, w_up, gate_bias, up_bias, w_down, expert_norm):
    values = pool_in.astype(jnp.float32)
    length = values.shape[0]
    positions = jnp.arange(length)
    radius = jnp.left_shift(1, jnp.arange(POOL_WIDTH) // GROUP_WIDTH)
    padded = jnp.pad(values, ((reach_rows, reach_rows), (0, 0)))
    window_sum = jnp.zeros_like(values)
    counts = jnp.zeros_like(values)
    for offset in range(-reach_rows, reach_rows + 1):
        inside = ((positions + offset >= 0) & (positions + offset < length))[:, None] & (abs(offset) <= radius)[None, :]
        window_sum = window_sum + jnp.where(inside, padded[reach_rows + offset:reach_rows + offset + length], 0.0)
        counts = counts + inside.astype(jnp.float32)
    deviation = (window_sum / counts - values).astype(jnp.bfloat16)
    grouped = deviation.reshape(length, GROUPS, GROUP_WIDTH).astype(jnp.float32)
    projected = jnp.einsum('tgc,gce->tge', grouped, pool_weight.astype(jnp.float32)).reshape(length, POOL_WIDTH)
    pool_out = (projected * pool_scale).astype(jnp.bfloat16)
    normed = (rms_scale(pool_out.astype(jnp.float32)) * pool_norm).astype(jnp.bfloat16)
    mix_out = jnp.dot(normed, out_weight, preferred_element_type=jnp.float32)
    mixed = (stream.astype(jnp.float32) + rms_scale(mix_out) * mix_norm).astype(jnp.bfloat16)
    expert_in = (rms_scale(mixed.astype(jnp.float32)) * ffn_norm).astype(jnp.bfloat16)
    assigned = routes.reshape(N_SP, TOK_DEV * TOP_K).astype(jnp.int32)
    onehot = (assigned[:, :, None] == jnp.arange(EXPERTS, dtype=jnp.int32)[None, None, :]).astype(jnp.int32)
    slot_ids = (lax.optimization_barrier(jnp.sum(jnp.cumsum(onehot, axis=1) * onehot, axis=-1)) - 1).astype(jnp.int32)
    block_ids = jnp.broadcast_to(jnp.arange(N_SP, dtype=jnp.int32)[:, None], assigned.shape)
    token_ids = (block_ids * TOK_DEV + jnp.arange(TOK_DEV * TOP_K, dtype=jnp.int32)[None, :] // TOP_K).astype(jnp.int32)
    slot_table = jnp.full((EXPERTS, N_SP, CAP), length, jnp.int32).at[assigned, block_ids, slot_ids].set(token_ids)
    extended = jnp.concatenate([expert_in, jnp.zeros((1, D), jnp.bfloat16)], axis=0)
    hidden_block = D_EXPERT // N_TP

    def one_expert(inputs):
        indices, gate_weights, up_weights, gate_b, up_b, down_weights = inputs
        row_block = extended[indices.reshape(-1)]
        gate_pre = jnp.dot(row_block, gate_weights, preferred_element_type=jnp.float32) + gate_b
        up_pre = jnp.dot(row_block, up_weights, preferred_element_type=jnp.float32) + up_b
        activation = clamped_unit(gate_pre, up_pre)
        total = jnp.zeros((row_block.shape[0], D), jnp.float32)
        for part_id in range(N_TP):
            first_row = part_id * hidden_block
            partial_value = jnp.dot(activation[:, first_row:first_row + hidden_block], down_weights[first_row:first_row + hidden_block], preferred_element_type=jnp.float32).astype(jnp.bfloat16)
            partial_value = lax.optimization_barrier(partial_value)
            total = total + partial_value.astype(jnp.float32)
        return total.astype(jnp.bfloat16).reshape(N_SP, CAP, D)
    expert_out = lax.map(one_expert, (slot_table, w_gate, w_up, gate_bias, up_bias, w_down))
    picked = expert_out[assigned, block_ids, slot_ids].astype(jnp.float32).reshape(length, TOP_K, D)
    combined = lax.optimization_barrier(jnp.sum(picked * route_weights[:, :, None], axis=1))
    return (mixed.astype(jnp.float32) + rms_scale(combined) * expert_norm).astype(jnp.bfloat16)
```

```python
import functools

import jax
import jax.numpy as jnp
from jax import lax
from jax.experimental import pallas as pl
from jax.experimental.pallas import tpu as pltpu
from jax.sharding import PartitionSpec as P

MESH = pl.DeviceIdType.MESH

epsilon = 1e-06
reach_rows = 8
clamp_limit = 7.0
sigmoid_alpha = 1.702
chunk_counts = (2,)


def extended_2(shard, sides, width):
    for axis, dim in sides:
        count, length = (lax.axis_size(axis), shard.shape[dim])
        up = [(i, (i + 1) % count) for i in range(count - 1)]
        down = [(j, i) for i, j in up]
        last = lax.slice_in_dim(shard, length - width, length, axis=dim)
        leading = lax.slice_in_dim(shard, 0, width, axis=dim)
        before = lax.ppermute(last, axis, up)
        after = lax.ppermute(leading, axis, down)
        shard = jnp.concatenate([before, shard, after], axis=dim)
    return shard


def rms_scale(values):
    return values * lax.rsqrt(jnp.mean(values * values, axis=-1, keepdims=True) + epsilon)


def routed_shards(
    pool_in,
    pool_weight,
    pool_scale,
    pool_norm,
    out_weight,
    stream,
    mix_norm,
    ffn_norm,
    routes,
    route_weights,
    w_gate,
    w_up,
    gate_bias,
    up_bias,
    w_down,
    expert_norm,
):
    rows_dev = pool_in.shape[0]
    length = rows_dev * lax.axis_size("sp")
    radius = jnp.left_shift(1, lax.axis_index("tp"))
    positions = lax.axis_index("sp") * rows_dev + jnp.arange(rows_dev)
    padded = extended_2(pool_in, (("sp", 0),), reach_rows).astype(jnp.float32)
    window_sum = jnp.zeros((rows_dev, pool_in.shape[1]), jnp.float32)
    counts = jnp.zeros((rows_dev,), jnp.float32)
    for offset in range(-reach_rows, reach_rows + 1):
        inside = (positions + offset >= 0) & (positions + offset < length) & (abs(offset) <= radius)
        window_sum = window_sum + jnp.where(
            inside[:, None], padded[reach_rows + offset : reach_rows + offset + rows_dev], 0.0
        )
        counts = counts + inside.astype(jnp.float32)
    deviation = (window_sum / counts[:, None] - padded[reach_rows : reach_rows + rows_dev]).astype(
        jnp.bfloat16
    )
    pool_out = (
        jnp.dot(deviation, pool_weight[0], preferred_element_type=jnp.float32) * pool_scale
    ).astype(jnp.bfloat16)
    all_groups = lax.all_gather(pool_out, "tp", axis=1, tiled=True)
    normed = (rms_scale(all_groups.astype(jnp.float32)) * pool_norm).astype(jnp.bfloat16)
    mix_out = jnp.dot(normed, out_weight, preferred_element_type=jnp.float32)
    mixed = (stream.astype(jnp.float32) + rms_scale(mix_out) * mix_norm).astype(jnp.bfloat16)
    expert_in = (rms_scale(mixed.astype(jnp.float32)) * ffn_norm).astype(jnp.bfloat16)
    model_width = mixed.shape[1]
    experts = lax.axis_size("sp") * w_gate.shape[0]
    top_count = routes.shape[1]
    capacity = rows_dev * top_count * 3 // (2 * experts)
    quarter = capacity // lax.axis_size("tp")
    chunks = next((n for n in chunk_counts if quarter % (8 * n) == 0), 1)
    chunk_rows, own_rows = capacity // chunks, quarter // chunks

    names = routes.T[:, None, :] == jnp.arange(experts, dtype=jnp.int32)[None, :, None]
    member = jnp.any(names, axis=0)
    weight = jnp.sum(jnp.where(names, route_weights.T[:, None, :], 0.0), axis=0)
    order = jnp.arange(rows_dev)
    earlier = (order[:, None] < order[None, :]).astype(jnp.bfloat16)
    place = jnp.dot(
        member.astype(jnp.bfloat16), earlier, preferred_element_type=jnp.float32
    ).astype(jnp.int32)
    place = jnp.where(member, place, -1)

    def dispatched(chunk):
        first = chunk * chunk_rows + lax.axis_index("tp") * own_rows
        slots = first + jnp.arange(own_rows, dtype=jnp.int32)
        pick = (place[:, None, :] == slots[None, :, None]).astype(jnp.bfloat16)
        rows = jnp.dot(pick.reshape(experts * own_rows, rows_dev), expert_in)
        own_slots = rows.reshape(experts, own_rows, model_width)
        arrived = lax.all_to_all(own_slots, "sp", split_axis=0, concat_axis=0, tiled=True)
        return lax.all_gather(arrived, "tp", axis=1, tiled=True)

    def expert(slot_block):
        row_block = slot_block.reshape(-1, model_width)
        gate_pre = jnp.dot(row_block, w_gate[0], preferred_element_type=jnp.float32) + gate_bias[0]
        up_pre = jnp.dot(row_block, w_up[0], preferred_element_type=jnp.float32) + up_bias[0]
        gate_cut = jnp.minimum(gate_pre, clamp_limit)
        up_cut = jnp.clip(up_pre, -clamp_limit, clamp_limit)
        activation = (
            (up_cut + 1.0) * (gate_cut * jax.nn.sigmoid(sigmoid_alpha * gate_cut))
        ).astype(jnp.bfloat16)
        partial_value = jnp.dot(activation, w_down[0], preferred_element_type=jnp.float32).astype(
            jnp.bfloat16
        )
        partial_value = partial_value.reshape(slot_block.shape)
        summed = lax.psum_scatter(partial_value, "tp", scatter_dimension=2, tiled=True)
        return lax.all_to_all(summed, "sp", split_axis=0, concat_axis=0, tiled=True)

    def weighted(chunk, returned):
        slots = chunk * chunk_rows + jnp.arange(chunk_rows, dtype=jnp.int32)
        spread = jnp.where(place[:, None, :] == slots[None, :, None], weight[:, None, :], 0.0)
        spread = spread.reshape(experts * chunk_rows, rows_dev)
        high = spread.astype(jnp.bfloat16)
        low = (spread - high.astype(jnp.float32)).astype(jnp.bfloat16)
        flat = returned.reshape(experts * chunk_rows, -1)
        over_slots = (((0,), (0,)), ((), ()))
        return lax.dot_general(
            high, flat, over_slots, preferred_element_type=jnp.float32
        ) + lax.dot_general(low, flat, over_slots, preferred_element_type=jnp.float32)

    blocks = [dispatched(chunk) for chunk in range(chunks)]
    parts = [expert(block) for block in blocks]
    col_count = parts[0].shape[2]
    combined = sum(weighted(chunk, part) for chunk, part in enumerate(parts))
    squares = lax.psum(jnp.sum(combined * combined, axis=1), "tp")
    row_scale = lax.rsqrt(squares / model_width + epsilon)
    own_cols = lax.dynamic_slice_in_dim(
        mixed.astype(jnp.float32), lax.axis_index("tp") * col_count, col_count, 1
    )
    return (own_cols + combined * row_scale[:, None] * expert_norm).astype(jnp.bfloat16)


x_size = 2
core_count = 2
first_rows = 48
vmem_limit = 60 * 1024 * 1024
UP, DOWN, ACROSS, SIBLING = range(4)
XF, ZF = range(2)


def layer_kernel(
    nz,
    pool_in,
    pool_weight,
    pool_scale,
    pool_norm,
    out_weight_hbm,
    stream_hbm,
    mix_norm,
    ffn_norm,
    routes,
    route_weights,
    w_gate_hbm,
    w_up_hbm,
    gate_bias,
    up_bias,
    w_down_hbm,
    expert_norm,
    out_ref,
    tokens,
    w_gate,
    w_up,
    w_down,
    out_weight,
    stream,
    pool_all,
    pool_edges,
    weight_all,
    scale_all,
    padded,
    normed,
    mix_out,
    mixed,
    route_all,
    hidden,
    parts,
    parts_in,
    pair_out,
    pair_keep,
    pair_in,
    side_out,
    side_in,
    total,
    far_out,
    far_in,
    squares,
    load_sem,
    ag_send,
    ag_recv,
    front_send,
    front_recv,
    edge_send,
    edge_recv,
    route_send,
    route_recv,
    part_send,
    part_recv,
    pair_send,
    pair_recv,
    side_send,
    side_recv,
    far_send,
    far_recv,
    sq_send,
    sq_recv,
):
    sp, tp = lax.axis_index("sp"), lax.axis_index("tp")
    n_sp = nz * x_size
    n_tp = pool_all.shape[0]
    z, x = sp // x_size, sp % x_size
    y, core = tp // core_count, tp % core_count
    rows, width = stream.shape
    cols = out_ref.shape[1]
    group_width = pool_in.shape[1]
    half_rows = rows // core_count
    sibling = y * core_count + (1 - core)
    opposite = (1 - y) * core_count + core
    far_z = nz - 1

    def remote(src, dst, send, recv, to_sp, to_tp):
        return pltpu.make_async_remote_copy(
            src_ref=src,
            dst_ref=dst,
            send_sem=send,
            recv_sem=recv,
            device_id=(to_sp, to_tp),
            device_id_type=MESH,
        )

    loads = [
        pltpu.make_async_copy(src, dst, load_sem.at[i])
        for i, (src, dst) in enumerate(
            (
                (out_weight_hbm, out_weight),
                (stream_hbm, stream),
                (w_gate_hbm.at[0], w_gate),
                (w_up_hbm.at[0], w_up),
                (w_down_hbm.at[0], w_down),
            )
        )
    ]
    for load in loads:
        load.start()

    barrier = pltpu.get_barrier_semaphore()

    def greet(to_sp, to_tp):
        pl.semaphore_signal(barrier, inc=1, device_id=(to_sp, to_tp), device_id_type=MESH)

    for d in range(1, n_sp):
        greet((sp + d) % n_sp, tp)
    for d in range(1, n_tp):
        greet(sp, (tp + d) % n_tp)

    @pl.when(sp > 0)
    def _():
        for d in range(1, n_tp):
            greet(sp - 1, (tp + d) % n_tp)

    @pl.when(sp < n_sp - 1)
    def _():
        for d in range(1, n_tp):
            greet(sp + 1, (tp + d) % n_tp)

    near = (sp > 0).astype(jnp.int32) + (sp < n_sp - 1).astype(jnp.int32)
    pl.semaphore_wait(barrier, (n_sp - 1) + (n_tp - 1) * (1 + near))

    edge = pool_edges.shape[2]

    def edge_copy(side, to_tp, d):
        src = pool_in.at[pl.ds(rows - edge, edge)] if side == 0 else pool_in.at[pl.ds(0, edge)]
        return remote(
            src,
            pool_edges.at[tp, side],
            edge_send.at[side, d],
            edge_recv.at[tp, side],
            sp + 1 if side == 0 else sp - 1,
            to_tp,
        )

    def edge_loop(side, act):
        @pl.when(sp < n_sp - 1 if side == 0 else sp > 0)
        def _():
            for d in range(n_tp):
                act(edge_copy(side, (tp + d) % n_tp, d))

    for side in range(2):
        edge_loop(side, lambda copy: copy.start())

    def front_copies(d):
        to = (tp + d) % n_tp
        return [
            remote(pool_in, pool_all.at[tp], front_send.at[d, 0], front_recv.at[tp, 0], sp, to),
            remote(
                pool_weight.at[0], weight_all.at[tp], front_send.at[d, 1], front_recv.at[tp, 1], sp, to
            ),
            remote(pool_scale, scale_all.at[tp], front_send.at[d, 2], front_recv.at[tp, 2], sp, to),
        ]

    for d in range(1, n_tp):
        for copy in front_copies(d):
            copy.start()
    pool_all[tp] = pool_in[...]
    weight_all[tp] = pool_weight[0]
    scale_all[tp] = pool_scale[...]

    lanes = lax.broadcasted_iota(jnp.int32, (rows, 128), 1)
    by_expert = jnp.zeros((rows, 128), jnp.float32)
    for k in range(routes.shape[1]):
        by_expert += jnp.where(routes[:, k : k + 1] == lanes, route_weights[:, k : k + 1], 0.0)
    route_rows = route_all.shape[1]
    route_all[sp] = by_expert.T[:route_rows]

    def route_copy(d):
        to = (sp + d) % n_sp
        return remote(
            route_all.at[sp], route_all.at[sp], route_send.at[d], route_recv.at[sp], to, tp
        )

    for d in range(1, n_sp):
        route_copy(d).start()

    for d in range(1, n_tp):
        src_tp = (tp + d) % n_tp
        for i, (src, dst) in enumerate(
            (
                (pool_in, pool_all),
                (pool_weight.at[0], weight_all),
                (pool_scale, scale_all),
            )
        ):
            remote(
                src, dst.at[src_tp], front_send.at[d, i], front_recv.at[src_tp, i], sp, src_tp
            ).wait_recv()

    @pl.when(sp > 0)
    def _():
        for g in range(n_tp):
            remote(
                pool_in.at[pl.ds(0, edge)],
                pool_edges.at[g, 0],
                edge_send.at[0, 0],
                edge_recv.at[g, 0],
                sp - 1,
                tp,
            ).wait_recv()
            padded[g, 0:reach_rows, :] = pool_edges[g, 0].astype(jnp.float32)[edge - reach_rows :]

    @pl.when(sp == 0)
    def _():
        padded[:, 0:reach_rows, :] = jnp.zeros((n_tp, reach_rows, group_width), jnp.float32)

    @pl.when(sp < n_sp - 1)
    def _():
        for g in range(n_tp):
            remote(
                pool_in.at[pl.ds(0, edge)],
                pool_edges.at[g, 1],
                edge_send.at[0, 0],
                edge_recv.at[g, 1],
                sp + 1,
                tp,
            ).wait_recv()
            padded[g, reach_rows + rows :, :] = pool_edges[g, 1].astype(jnp.float32)[:reach_rows]

    @pl.when(sp == n_sp - 1)
    def _():
        padded[:, reach_rows + rows :, :] = jnp.zeros((n_tp, reach_rows, group_width), jnp.float32)

    positions = sp * rows + lax.broadcasted_iota(jnp.int32, (rows, group_width), 0)
    mean_square = jnp.zeros((rows, 1), jnp.float32)
    for g in range(n_tp):
        radius = 1 << g
        values = pool_all[g].astype(jnp.float32)
        padded[g, reach_rows : reach_rows + rows, :] = values
        window_sum = values
        for offset in range(1, radius + 1):
            window_sum += padded[g, reach_rows + offset : reach_rows + offset + rows, :]
            window_sum += padded[g, reach_rows - offset : reach_rows - offset + rows, :]
        last = jnp.minimum(positions + radius, n_sp * rows - 1)
        counts = last - jnp.maximum(positions - radius, 0) + 1
        deviation = (window_sum / counts.astype(jnp.float32) - values).astype(jnp.bfloat16)
        pool_out = (
            jnp.dot(deviation, weight_all[g], preferred_element_type=jnp.float32) * scale_all[g]
        ).astype(jnp.bfloat16)
        normed[:, g * group_width : (g + 1) * group_width] = pool_out
        wide = pool_out.astype(jnp.float32)
        mean_square += jnp.sum(wide * wide, axis=1, keepdims=True)
    pool_width = n_tp * group_width
    row_scale = lax.rsqrt(mean_square / pool_width + epsilon)
    normed[...] = (normed[...].astype(jnp.float32) * row_scale * pool_norm[...]).astype(jnp.bfloat16)

    for load in loads[:2]:
        load.wait()
    for t in range(width // cols):
        mix_out[:, t * cols : (t + 1) * cols] = jnp.dot(
            normed[...], out_weight[:, t * cols : (t + 1) * cols], preferred_element_type=jnp.float32
        )

    tile = 32

    def mix_rows(i, carry):
        part = pl.ds(pl.multiple_of(i * tile, tile), tile)
        value = mix_out[part, :]
        scaled = value * lax.rsqrt(jnp.mean(value * value, axis=1, keepdims=True) + epsilon)
        summed = (stream[part, :].astype(jnp.float32) + scaled * mix_norm[...]).astype(jnp.bfloat16)
        mixed[part, :] = summed
        wide = summed.astype(jnp.float32)
        wide = wide * lax.rsqrt(jnp.mean(wide * wide, axis=1, keepdims=True) + epsilon)
        tokens[sp, part, :] = (wide * ffn_norm[...]).astype(jnp.bfloat16)
        return carry

    lax.fori_loop(0, rows // tile, mix_rows, 0)

    def piece(block, kind, whose):
        start = whose * half_rows + (0 if kind == XF else first_rows)
        count = first_rows if kind == XF else half_rows - first_rows
        return tokens.at[block, pl.ds(pl.multiple_of(start, 16), count), :]

    def ag_copy(block, kind, way):
        to_sp = {UP: sp + x_size, DOWN: sp - x_size, ACROSS: z * x_size + (1 - x), SIBLING: sp}[way]
        recv = ag_recv.at[block, kind + (2 if way == SIBLING else 0)]
        ref = piece(block, kind, core)
        return remote(
            ref, ref, ag_send.at[block, kind, way], recv, to_sp, sibling if way == SIBLING else tp
        )

    def ag_arrived(block, kind, from_sibling):
        whose = 1 - core if from_sibling else core
        ref = piece(block, kind, whose)
        recv = ag_recv.at[block, kind + (2 if from_sibling else 0)]
        remote(ref, ref, ag_send.at[block, kind, SIBLING], recv, sp, sibling).wait_recv()

    def ag_ways(zc, col_is_own, kind, act):
        block = zc * x_size + (x if col_is_own else 1 - x)
        along = col_is_own or kind == XF

        if along:

            @pl.when((zc <= z) & (z < far_z))
            def _():
                act(ag_copy(block, kind, UP))

            @pl.when((zc >= z) & (z > 0))
            def _():
                act(ag_copy(block, kind, DOWN))

        if col_is_own and kind == ZF:
            act(ag_copy(block, kind, ACROSS))
        if col_is_own and kind == XF:

            @pl.when(zc == z)
            def _():
                act(ag_copy(block, kind, ACROSS))

        if col_is_own:

            @pl.when(zc != z)
            def _():
                act(ag_copy(block, kind, SIBLING))

        else:
            act(ag_copy(block, kind, SIBLING))

    def start(copy):
        copy.start()

    def take(zc, col_is_own, kind):
        block = zc * x_size + (x if col_is_own else 1 - x)
        ag_arrived(block, kind, False)
        ag_ways(zc, col_is_own, kind, start)

    def take_set(zc):
        take(zc, True, ZF)
        take(zc, True, XF)
        take(zc, False, XF)
        take(zc, False, ZF)

    ag_ways(z, True, XF, start)
    ag_ways(z, True, ZF, start)

    for d in range(1, n_sp):
        src_sp = (sp + d) % n_sp
        remote(
            route_all.at[sp], route_all.at[src_sp], route_send.at[d], route_recv.at[src_sp], src_sp, tp
        ).wait_recv()
    for load in loads[2:]:
        load.wait()

    upper = z >= (nz + 1) // 2
    low_z = jnp.where(upper, far_z - z, z)

    def plane_at(step):
        plane = jnp.where(step <= low_z, low_z - step, step)
        return jnp.where(upper, far_z - plane, plane)

    n_hidden = hidden.shape[1]
    hidden_tile = min(256, n_hidden)

    def part_copy(block, q_y):
        q = q_y * core_count + (1 - core)
        return remote(
            parts.at[block, q],
            parts_in.at[block, q_y],
            part_send.at[block, q_y],
            part_recv.at[block, q_y],
            sp,
            sibling,
        )

    def pair_copy(block):
        return remote(
            pair_out.at[block], pair_in.at[block], pair_send.at[block], pair_recv.at[block], sp, opposite
        )

    def side_copy(zc):
        return remote(
            side_out.at[zc],
            side_in.at[zc],
            side_send.at[zc],
            side_recv.at[zc],
            z * x_size + (1 - x),
            tp,
        )

    def far_copy(zc):
        return remote(
            far_out.at[zc], far_in.at[z], far_send.at[zc], far_recv.at[z], zc * x_size + x, tp
        )

    def compute(block):
        own_row = lax.broadcasted_iota(jnp.int32, (route_rows, rows), 0) == sp
        weight = jnp.sum(jnp.where(own_row, route_all[block], 0.0), axis=0, keepdims=True)
        weight = jnp.broadcast_to(weight, (128, rows)).T
        for j in range(n_hidden // hidden_tile):
            span = slice(j * hidden_tile, (j + 1) * hidden_tile)
            data = tokens[block]
            gate = jnp.dot(data, w_gate[:, span], preferred_element_type=jnp.float32)
            up = jnp.dot(data, w_up[:, span], preferred_element_type=jnp.float32)
            gate_cut = jnp.minimum(gate + gate_bias[:, span], clamp_limit)
            up_cut = jnp.clip(up + up_bias[:, span], -clamp_limit, clamp_limit)
            active = (up_cut + 1.0) * (gate_cut * jax.nn.sigmoid(sigmoid_alpha * gate_cut))
            for i in range(hidden_tile // 128):
                lane = slice(i * 128, (i + 1) * 128)
                at = j * hidden_tile + i * 128
                hidden[:, at : at + 128] = (active[:, lane] * weight).astype(jnp.bfloat16)

        def down(i, carry):
            whose = jnp.where(i < 2, 1 - core, core)
            q = (i % 2) * core_count + whose
            at = pl.ds(pl.multiple_of(q * cols, cols), cols)
            parts[block, q] = jnp.dot(
                hidden[...], w_down[:, at], preferred_element_type=jnp.float32
            ).astype(jnp.bfloat16)

            @pl.when(i < 2)
            def _():
                part_copy(block, i % 2).start()

            return carry

        lax.fori_loop(0, n_tp, down, 0)

    def join_cores(block):
        for q_y in range(n_tp // core_count):
            part_copy(block, q_y).wait_recv()
        away = parts[block, opposite].astype(jnp.float32) + parts_in[block, 1 - y].astype(jnp.float32)
        pair_out[block] = away.astype(jnp.bfloat16)
        pair_copy(block).start()
        pair_keep[block] = parts[block, tp].astype(jnp.float32) + parts_in[block, y].astype(
            jnp.float32
        )

    def join_pair_other(step):
        zc = plane_at(step)
        block = zc * x_size + (1 - x)
        pair_copy(block).wait_recv()
        side_out[zc] = (pair_keep[block] + pair_in[block].astype(jnp.float32)).astype(jnp.bfloat16)
        side_copy(zc).start()

    def join_pair_own(step):
        zc = plane_at(step)
        block = zc * x_size + x
        pair_copy(block).wait_recv()
        total[zc] = pair_keep[block] + pair_in[block].astype(jnp.float32)

    def join_sides(step):
        zc = plane_at(step)
        side_copy(zc).wait_recv()
        value = total[zc] + side_in[zc].astype(jnp.float32)
        total[zc] = value

        @pl.when(zc != z)
        def _():
            far_out[zc] = value.astype(jnp.bfloat16)
            far_copy(zc).start()

    def step_body(step, carry):
        zc = plane_at(step)
        inner = low_z > 0

        @pl.when((step >= 1) & ((step != 2) | (low_z == 0)))
        def _():
            take_set(zc)

        if nz > 2:

            @pl.when((step == 1) & inner)
            def _():
                take_set(plane_at(2))

        col = jnp.where(step == 0, x, 1 - x)
        first, second = zc * x_size + col, zc * x_size + (1 - col)

        @pl.when(step >= 1)
        def _():
            ag_arrived(first, XF, True)
            ag_arrived(first, ZF, True)

        compute(first)
        join_cores(first)

        @pl.when(step == 0)
        def _():
            take(z, False, XF)
            take(z, False, ZF)

        @pl.when(step >= 1)
        def _():
            join_pair_other(step - 1)
            join_pair_own(step - 1)

        @pl.when(step >= 2)
        def _():
            join_sides(step - 2)

        ag_arrived(second, XF, True)
        ag_arrived(second, ZF, True)
        compute(second)
        join_cores(second)
        return carry

    lax.fori_loop(0, nz, step_body, 0)
    join_pair_other(nz - 1)
    if nz > 1:
        join_sides(nz - 2)
    join_pair_own(nz - 1)
    join_sides(nz - 1)

    combined = total[z]
    for d in range(1, nz):
        src_z = (z + d) % nz
        remote(
            far_out.at[src_z],
            far_in.at[src_z],
            far_send.at[src_z],
            far_recv.at[src_z],
            src_z * x_size + x,
            tp,
        ).wait_recv()
        combined += far_in[src_z].astype(jnp.float32)
    total[z] = combined

    own_squares = jnp.sum(combined * combined, axis=1, keepdims=True)
    squares[tp] = jnp.broadcast_to(own_squares, (rows, 128)).T[:8]

    def squares_copy(d):
        return remote(
            squares.at[tp], squares.at[tp], sq_send.at[d], sq_recv.at[tp], sp, (tp + d) % n_tp
        )

    for d in range(1, n_tp):
        squares_copy(d).start()
    summed = squares[tp]
    for d in range(1, n_tp):
        src_tp = (tp + d) % n_tp
        remote(
            squares.at[tp], squares.at[src_tp], sq_send.at[d], sq_recv.at[src_tp], sp, src_tp
        ).wait_recv()
        summed += squares[src_tp]
    row_scale = lax.rsqrt(summed[:1] / width + epsilon)
    row_scale = jnp.broadcast_to(row_scale, (128, rows)).T
    for i in range(cols // 128):
        lane = slice(i * 128, (i + 1) * 128)
        own = mixed[:, pl.ds(pl.multiple_of(tp * cols + i * 128, 128), 128)].astype(jnp.float32)
        out_ref[:, lane] = (own + total[z, :, lane] * row_scale * expert_norm[:, lane]).astype(
            jnp.bfloat16
        )

    def sent(copy):
        copy.wait_send()

    for side in range(2):
        edge_loop(side, sent)
    for d in range(1, n_tp):
        for copy in front_copies(d):
            sent(copy)
        sent(squares_copy(d))
    for d in range(1, n_sp):
        sent(route_copy(d))

    def all_sent(zc, carry):
        for col_is_own in (True, False):
            for kind in (XF, ZF):
                ag_ways(zc, col_is_own, kind, sent)
        for i in range(x_size):
            block = zc * x_size + i
            for q_y in range(n_tp // core_count):
                sent(part_copy(block, q_y))
            sent(pair_copy(block))
        sent(side_copy(zc))

        @pl.when(zc != z)
        def _():
            sent(far_copy(zc))

        return carry

    lax.fori_loop(0, nz, all_sent, 0)


def gathered_shards(*args):
    pool_in, pool_norm, out_weight, stream = args[0], args[3], args[4], args[5]
    w_gate, w_down = args[10], args[14]
    n_sp, n_tp = lax.axis_size("sp"), lax.axis_size("tp")
    nz = n_sp // x_size
    rows, width = stream.shape
    n_hidden = w_gate.shape[2]
    cols = width // n_tp
    group_width = pool_in.shape[1]
    bf16, f32 = jnp.bfloat16, jnp.float32
    row_args = (2, 3, 6, 7, 15)
    args = [a.reshape(1, -1) if i in row_args else a for i, a in enumerate(args)]
    in_hbm = (4, 5, 10, 11, 14)
    in_specs = [
        pl.BlockSpec(memory_space=pl.ANY if i in in_hbm else pltpu.VMEM) for i in range(len(args))
    ]
    edge = 2 * reach_rows
    route_rows = -(-n_sp // 8) * 8
    dma = pltpu.SemaphoreType.DMA
    scratch = [
        pltpu.VMEM((n_sp, rows, width), bf16),
        pltpu.VMEM((width, n_hidden), bf16),
        pltpu.VMEM((width, n_hidden), bf16),
        pltpu.VMEM((n_hidden, width), bf16),
        pltpu.VMEM(out_weight.shape, bf16),
        pltpu.VMEM((rows, width), bf16),
        pltpu.VMEM((n_tp, rows, group_width), bf16),
        pltpu.VMEM((n_tp, 2, edge, group_width), bf16),
        pltpu.VMEM((n_tp, group_width, group_width), bf16),
        pltpu.VMEM((n_tp, 1, group_width), f32),
        pltpu.VMEM((n_tp, rows + 2 * reach_rows, group_width), f32),
        pltpu.VMEM((rows, n_tp * group_width), bf16),
        pltpu.VMEM((rows, width), f32),
        pltpu.VMEM((rows, width), bf16),
        pltpu.VMEM((n_sp, route_rows, rows), f32),
        pltpu.VMEM((rows, n_hidden), bf16),
        pltpu.VMEM((n_sp, n_tp, rows, cols), bf16),
        pltpu.VMEM((n_sp, n_tp // core_count, rows, cols), bf16),
        pltpu.VMEM((n_sp, rows, cols), bf16),
        pltpu.VMEM((n_sp, rows, cols), f32),
        pltpu.VMEM((n_sp, rows, cols), bf16),
        pltpu.VMEM((nz, rows, cols), bf16),
        pltpu.VMEM((nz, rows, cols), bf16),
        pltpu.VMEM((nz, rows, cols), f32),
        pltpu.VMEM((nz, rows, cols), bf16),
        pltpu.VMEM((nz, rows, cols), bf16),
        pltpu.VMEM((n_tp, 8, rows), f32),
        dma((5,)),
        dma((n_sp, 2, 4)),
        dma((n_sp, 4)),
        dma((n_tp, 3)),
        dma((n_tp, 3)),
        dma((2, n_tp)),
        dma((n_tp, 2)),
        dma((n_sp,)),
        dma((n_sp,)),
        dma((n_sp, n_tp // core_count)),
        dma((n_sp, n_tp // core_count)),
        dma((n_sp,)),
        dma((n_sp,)),
        dma((nz,)),
        dma((nz,)),
        dma((nz,)),
        dma((nz,)),
        dma((n_tp,)),
        dma((n_tp,)),
    ]
    return pl.pallas_call(
        functools.partial(layer_kernel, nz),
        out_shape=jax.ShapeDtypeStruct((rows, cols), bf16),
        in_specs=in_specs,
        out_specs=pl.BlockSpec(memory_space=pltpu.VMEM),
        scratch_shapes=scratch,
        compiler_params=pltpu.CompilerParams(
            collective_id=0, has_side_effects=True, vmem_limit_bytes=vmem_limit
        ),
        name="layer",
    )(*args)


def shards(*args):
    pool_in, out_weight, stream, w_gate = args[0], args[4], args[5], args[10]
    n_sp, n_tp = lax.axis_size("sp"), lax.axis_size("tp")
    rows, width = stream.shape
    cols, n_hidden = width // n_tp, w_gate.shape[2]
    slots = n_sp * rows * (2 * width + (2 + 1 + 1 + 2 + 1) * 2 * cols + 2 * width + 2 * width)
    fixed = 2 * (3 * width * n_hidden + out_weight.size) + 10 * rows * width
    fits = slots + fixed < vmem_limit * 9 // 10
    shaped = (
        n_tp == 2 * core_count
        and n_sp % x_size == 0
        and w_gate.shape[0] == 1
        and rows % 128 == 0
        and rows // core_count > first_rows
        and cols % 128 == 0
        and n_hidden % 256 == 0
        and pool_in.shape[1] == 128
        and n_sp <= 128
    )
    return (gathered_shards if fits and shaped else routed_shards)(*args)


def solution(mesh):
    in_specs = (
        P("sp", "tp"),
        P("tp", None, None),
        P("tp"),
        P(),
        P(),
        P("sp", None),
        P(),
        P(),
        P("sp", None),
        P("sp", None),
        P("sp", None, "tp"),
        P("sp", None, "tp"),
        P("sp", "tp"),
        P("sp", "tp"),
        P("sp", "tp", None),
        P("tp"),
    )
    out_specs = P("sp", "tp")
    return jax.shard_map(shards, mesh=mesh, in_specs=in_specs, out_specs=out_specs, check_vma=False)
```

```python
import functools

import jax
import jax.numpy as jnp
from jax import lax
from jax.experimental import pallas as pl
from jax.experimental.pallas import tpu as pltpu
from jax.sharding import PartitionSpec as P

MESH = pl.DeviceIdType.MESH

epsilon = 1e-06
reach_rows = 8
clamp_limit = 7.0
sigmoid_alpha = 1.702
chunk_counts = (2,)


def extended_2(shard, sides, width):
    for axis, dim in sides:
        count, length = (lax.axis_size(axis), shard.shape[dim])
        up = [(i, (i + 1) % count) for i in range(count - 1)]
        down = [(j, i) for i, j in up]
        last = lax.slice_in_dim(shard, length - width, length, axis=dim)
        leading = lax.slice_in_dim(shard, 0, width, axis=dim)
        before = lax.ppermute(last, axis, up)
        after = lax.ppermute(leading, axis, down)
        shard = jnp.concatenate([before, shard, after], axis=dim)
    return shard


def rms_scale(values):
    return values * lax.rsqrt(jnp.mean(values * values, axis=-1, keepdims=True) + epsilon)


def routed_shards(
    pool_in,
    pool_weight,
    pool_scale,
    pool_norm,
    out_weight,
    stream,
    mix_norm,
    ffn_norm,
    routes,
    route_weights,
    w_gate,
    w_up,
    gate_bias,
    up_bias,
    w_down,
    expert_norm,
):
    rows_dev = pool_in.shape[0]
    length = rows_dev * lax.axis_size("sp")
    radius = jnp.left_shift(1, lax.axis_index("tp"))
    positions = lax.axis_index("sp") * rows_dev + jnp.arange(rows_dev)
    padded = extended_2(pool_in, (("sp", 0),), reach_rows).astype(jnp.float32)
    window_sum = jnp.zeros((rows_dev, pool_in.shape[1]), jnp.float32)
    counts = jnp.zeros((rows_dev,), jnp.float32)
    for offset in range(-reach_rows, reach_rows + 1):
        inside = (positions + offset >= 0) & (positions + offset < length) & (abs(offset) <= radius)
        window_sum = window_sum + jnp.where(
            inside[:, None], padded[reach_rows + offset : reach_rows + offset + rows_dev], 0.0
        )
        counts = counts + inside.astype(jnp.float32)
    deviation = (window_sum / counts[:, None] - padded[reach_rows : reach_rows + rows_dev]).astype(
        jnp.bfloat16
    )
    pool_out = (
        jnp.dot(deviation, pool_weight[0], preferred_element_type=jnp.float32) * pool_scale
    ).astype(jnp.bfloat16)
    all_groups = lax.all_gather(pool_out, "tp", axis=1, tiled=True)
    normed = (rms_scale(all_groups.astype(jnp.float32)) * pool_norm).astype(jnp.bfloat16)
    mix_out = jnp.dot(normed, out_weight, preferred_element_type=jnp.float32)
    mixed = (stream.astype(jnp.float32) + rms_scale(mix_out) * mix_norm).astype(jnp.bfloat16)
    expert_in = (rms_scale(mixed.astype(jnp.float32)) * ffn_norm).astype(jnp.bfloat16)
    model_width = mixed.shape[1]
    experts = lax.axis_size("sp") * w_gate.shape[0]
    top_count = routes.shape[1]
    capacity = rows_dev * top_count * 3 // (2 * experts)
    quarter = capacity // lax.axis_size("tp")
    chunks = next((n for n in chunk_counts if quarter % (8 * n) == 0), 1)
    chunk_rows, own_rows = capacity // chunks, quarter // chunks

    names = routes.T[:, None, :] == jnp.arange(experts, dtype=jnp.int32)[None, :, None]
    member = jnp.any(names, axis=0)
    weight = jnp.sum(jnp.where(names, route_weights.T[:, None, :], 0.0), axis=0)
    order = jnp.arange(rows_dev)
    earlier = (order[:, None] < order[None, :]).astype(jnp.bfloat16)
    place = jnp.dot(
        member.astype(jnp.bfloat16), earlier, preferred_element_type=jnp.float32
    ).astype(jnp.int32)
    place = jnp.where(member, place, -1)

    def dispatched(chunk):
        first = chunk * chunk_rows + lax.axis_index("tp") * own_rows
        slots = first + jnp.arange(own_rows, dtype=jnp.int32)
        pick = (place[:, None, :] == slots[None, :, None]).astype(jnp.bfloat16)
        rows = jnp.dot(pick.reshape(experts * own_rows, rows_dev), expert_in)
        own_slots = rows.reshape(experts, own_rows, model_width)
        arrived = lax.all_to_all(own_slots, "sp", split_axis=0, concat_axis=0, tiled=True)
        return lax.all_gather(arrived, "tp", axis=1, tiled=True)

    def expert(slot_block):
        row_block = slot_block.reshape(-1, model_width)
        gate_pre = jnp.dot(row_block, w_gate[0], preferred_element_type=jnp.float32) + gate_bias[0]
        up_pre = jnp.dot(row_block, w_up[0], preferred_element_type=jnp.float32) + up_bias[0]
        gate_cut = jnp.minimum(gate_pre, clamp_limit)
        up_cut = jnp.clip(up_pre, -clamp_limit, clamp_limit)
        activation = (
            (up_cut + 1.0) * (gate_cut * jax.nn.sigmoid(sigmoid_alpha * gate_cut))
        ).astype(jnp.bfloat16)
        partial_value = jnp.dot(activation, w_down[0], preferred_element_type=jnp.float32).astype(
            jnp.bfloat16
        )
        partial_value = partial_value.reshape(slot_block.shape)
        summed = lax.psum_scatter(partial_value, "tp", scatter_dimension=2, tiled=True)
        return lax.all_to_all(summed, "sp", split_axis=0, concat_axis=0, tiled=True)

    def weighted(chunk, returned):
        slots = chunk * chunk_rows + jnp.arange(chunk_rows, dtype=jnp.int32)
        spread = jnp.where(place[:, None, :] == slots[None, :, None], weight[:, None, :], 0.0)
        spread = spread.reshape(experts * chunk_rows, rows_dev)
        high = spread.astype(jnp.bfloat16)
        low = (spread - high.astype(jnp.float32)).astype(jnp.bfloat16)
        flat = returned.reshape(experts * chunk_rows, -1)
        over_slots = (((0,), (0,)), ((), ()))
        return lax.dot_general(
            high, flat, over_slots, preferred_element_type=jnp.float32
        ) + lax.dot_general(low, flat, over_slots, preferred_element_type=jnp.float32)

    blocks = [dispatched(chunk) for chunk in range(chunks)]
    parts = [expert(block) for block in blocks]
    col_count = parts[0].shape[2]
    combined = sum(weighted(chunk, part) for chunk, part in enumerate(parts))
    squares = lax.psum(jnp.sum(combined * combined, axis=1), "tp")
    row_scale = lax.rsqrt(squares / model_width + epsilon)
    own_cols = lax.dynamic_slice_in_dim(
        mixed.astype(jnp.float32), lax.axis_index("tp") * col_count, col_count, 1
    )
    return (own_cols + combined * row_scale[:, None] * expert_norm).astype(jnp.bfloat16)


x_size = 2
core_count = 2
halves = 2
first_share = 8, 3
vmem_limit = 60 * 1024 * 1024
UP, DOWN, ACROSS, SIBLING = range(4)
XF, ZF = range(2)


def layer_kernel(
    nz,
    pool_in,
    pool_weight,
    pool_scale,
    pool_norm,
    out_weight_hbm,
    stream_hbm,
    mix_norm,
    ffn_norm,
    routes,
    route_weights,
    w_gate_hbm,
    w_up_hbm,
    gate_bias,
    up_bias,
    w_down_hbm,
    expert_norm,
    out_ref,
    tokens,
    w_gate,
    w_up,
    w_down,
    out_weight,
    stream,
    pool_all,
    pool_edges,
    weight_all,
    scale_all,
    padded,
    normed,
    mix_out,
    mixed,
    route_all,
    hidden,
    parts,
    parts_in,
    pair_out,
    pair_keep,
    pair_in,
    side_out,
    side_in,
    total,
    far_out,
    far_in,
    squares,
    load_sem,
    ag_send,
    ag_recv,
    front_send,
    front_recv,
    edge_send,
    edge_recv,
    route_send,
    route_recv,
    part_send,
    part_recv,
    pair_send,
    pair_recv,
    side_send,
    side_recv,
    far_send,
    far_recv,
    sq_send,
    sq_recv,
):
    sp, tp = lax.axis_index("sp"), lax.axis_index("tp")
    n_sp = nz * x_size
    n_tp = pool_all.shape[0]
    z, x = sp // x_size, sp % x_size
    y, core = tp // core_count, tp % core_count
    rows, width = stream.shape
    cols = out_ref.shape[1]
    group_width = pool_in.shape[1]
    half_rows = rows // halves
    core_rows = half_rows // core_count
    first_cols = width * first_share[1] // first_share[0]
    sibling = y * core_count + (1 - core)
    opposite = (1 - y) * core_count + core
    far_z = nz - 1

    def remote(src, dst, send, recv, to_sp, to_tp):
        return pltpu.make_async_remote_copy(
            src_ref=src,
            dst_ref=dst,
            send_sem=send,
            recv_sem=recv,
            device_id=(to_sp, to_tp),
            device_id_type=MESH,
        )

    loads = [
        pltpu.make_async_copy(src, dst, load_sem.at[i])
        for i, (src, dst) in enumerate(
            (
                (out_weight_hbm, out_weight),
                (stream_hbm, stream),
                (w_gate_hbm.at[0], w_gate),
                (w_up_hbm.at[0], w_up),
                (w_down_hbm.at[0], w_down),
            )
        )
    ]
    for load in loads:
        load.start()

    barrier = pltpu.get_barrier_semaphore()

    def greet(to_sp, to_tp):
        pl.semaphore_signal(barrier, inc=1, device_id=(to_sp, to_tp), device_id_type=MESH)

    for d in range(1, n_sp):
        greet((sp + d) % n_sp, tp)
    for d in range(1, n_tp):
        greet(sp, (tp + d) % n_tp)

    @pl.when(sp > 0)
    def _():
        for d in range(1, n_tp):
            greet(sp - 1, (tp + d) % n_tp)

    @pl.when(sp < n_sp - 1)
    def _():
        for d in range(1, n_tp):
            greet(sp + 1, (tp + d) % n_tp)

    near = (sp > 0).astype(jnp.int32) + (sp < n_sp - 1).astype(jnp.int32)
    pl.semaphore_wait(barrier, (n_sp - 1) + (n_tp - 1) * (1 + near))

    edge = pool_edges.shape[2]

    def edge_copy(side, to_tp, d):
        src = pool_in.at[pl.ds(rows - edge, edge)] if side == 0 else pool_in.at[pl.ds(0, edge)]
        return remote(
            src,
            pool_edges.at[tp, side],
            edge_send.at[side, d],
            edge_recv.at[tp, side],
            sp + 1 if side == 0 else sp - 1,
            to_tp,
        )

    def edge_loop(side, act):
        @pl.when(sp < n_sp - 1 if side == 0 else sp > 0)
        def _():
            for d in range(n_tp):
                act(edge_copy(side, (tp + d) % n_tp, d))

    for side in range(2):
        edge_loop(side, lambda copy: copy.start())

    def front_copies(d):
        to = (tp + d) % n_tp
        return [
            remote(pool_in, pool_all.at[tp], front_send.at[d, 0], front_recv.at[tp, 0], sp, to),
            remote(
                pool_weight.at[0], weight_all.at[tp], front_send.at[d, 1], front_recv.at[tp, 1], sp, to
            ),
            remote(pool_scale, scale_all.at[tp], front_send.at[d, 2], front_recv.at[tp, 2], sp, to),
        ]

    for d in range(1, n_tp):
        for copy in front_copies(d):
            copy.start()
    pool_all[tp] = pool_in[...]
    weight_all[tp] = pool_weight[0]
    scale_all[tp] = pool_scale[...]

    route_rows = route_all.shape[1]
    names = lax.broadcasted_iota(jnp.int32, (route_rows, rows), 0)
    by_expert = jnp.zeros((route_rows, rows), jnp.float32)
    for k in range(routes.shape[0]):
        by_expert += jnp.where(routes[k : k + 1, :] == names, route_weights[k : k + 1, :], 0.0)
    route_all[sp] = by_expert

    def route_copy(d):
        to = (sp + d) % n_sp
        return remote(
            route_all.at[sp], route_all.at[sp], route_send.at[d], route_recv.at[sp], to, tp
        )

    for d in range(1, n_sp):
        route_copy(d).start()

    for d in range(1, n_tp):
        src_tp = (tp + d) % n_tp
        for i, (src, dst) in enumerate(
            (
                (pool_in, pool_all),
                (pool_weight.at[0], weight_all),
                (pool_scale, scale_all),
            )
        ):
            remote(
                src, dst.at[src_tp], front_send.at[d, i], front_recv.at[src_tp, i], sp, src_tp
            ).wait_recv()

    @pl.when(sp > 0)
    def _():
        for g in range(n_tp):
            remote(
                pool_in.at[pl.ds(0, edge)],
                pool_edges.at[g, 0],
                edge_send.at[0, 0],
                edge_recv.at[g, 0],
                sp - 1,
                tp,
            ).wait_recv()
            padded[g, 0:reach_rows, :] = pool_edges[g, 0].astype(jnp.float32)[edge - reach_rows :]

    @pl.when(sp == 0)
    def _():
        padded[:, 0:reach_rows, :] = jnp.zeros((n_tp, reach_rows, group_width), jnp.float32)

    @pl.when(sp < n_sp - 1)
    def _():
        for g in range(n_tp):
            remote(
                pool_in.at[pl.ds(0, edge)],
                pool_edges.at[g, 1],
                edge_send.at[0, 0],
                edge_recv.at[g, 1],
                sp + 1,
                tp,
            ).wait_recv()
            padded[g, reach_rows + rows :, :] = pool_edges[g, 1].astype(jnp.float32)[:reach_rows]

    @pl.when(sp == n_sp - 1)
    def _():
        padded[:, reach_rows + rows :, :] = jnp.zeros((n_tp, reach_rows, group_width), jnp.float32)

    positions = sp * rows + lax.broadcasted_iota(jnp.int32, (rows, group_width), 0)
    mean_square = jnp.zeros((rows, 1), jnp.float32)
    for g in range(n_tp):
        radius = 1 << g
        values = pool_all[g].astype(jnp.float32)
        padded[g, reach_rows : reach_rows + rows, :] = values
        window_sum = values
        for offset in range(1, radius + 1):
            window_sum += padded[g, reach_rows + offset : reach_rows + offset + rows, :]
            window_sum += padded[g, reach_rows - offset : reach_rows - offset + rows, :]
        last = jnp.minimum(positions + radius, n_sp * rows - 1)
        counts = last - jnp.maximum(positions - radius, 0) + 1
        deviation = (window_sum / counts.astype(jnp.float32) - values).astype(jnp.bfloat16)
        pool_out = (
            jnp.dot(deviation, weight_all[g], preferred_element_type=jnp.float32) * scale_all[g]
        ).astype(jnp.bfloat16)
        normed[:, g * group_width : (g + 1) * group_width] = pool_out
        wide = pool_out.astype(jnp.float32)
        mean_square += jnp.sum(wide * wide, axis=1, keepdims=True)
    pool_width = n_tp * group_width
    row_scale = lax.rsqrt(mean_square / pool_width + epsilon)
    normed[...] = (normed[...].astype(jnp.float32) * row_scale * pool_norm[...]).astype(jnp.bfloat16)

    for load in loads[:2]:
        load.wait()
    for t in range(width // cols):
        mix_out[:, t * cols : (t + 1) * cols] = jnp.dot(
            normed[...], out_weight[:, t * cols : (t + 1) * cols], preferred_element_type=jnp.float32
        )

    tile = 32

    def mix_rows(first, count):
        def body(i, carry):
            part = pl.ds(pl.multiple_of(first + i * tile, tile), tile)
            value = mix_out[part, :]
            scaled = value * lax.rsqrt(jnp.mean(value * value, axis=1, keepdims=True) + epsilon)
            summed = stream[part, :].astype(jnp.float32) + scaled * mix_norm[...]
            summed = summed.astype(jnp.bfloat16)
            mixed[part, :] = summed
            wide = summed.astype(jnp.float32)
            wide = wide * lax.rsqrt(jnp.mean(wide * wide, axis=1, keepdims=True) + epsilon)
            tokens[sp, part, :] = (wide * ffn_norm[...]).astype(jnp.bfloat16)
            return carry

        lax.fori_loop(0, count // tile, body, 0)

    def piece(block, half, kind, whose):
        first = pl.multiple_of(half * half_rows + whose * core_rows, 16)
        span = pl.ds(0, first_cols) if kind == XF else pl.ds(first_cols, width - first_cols)
        return tokens.at[block, pl.ds(first, core_rows), span]

    def ag_copy(block, half, kind, way):
        to_sp = {UP: sp + x_size, DOWN: sp - x_size, ACROSS: z * x_size + (1 - x), SIBLING: sp}[way]
        recv = ag_recv.at[block, half, kind + (2 if way == SIBLING else 0)]
        ref = piece(block, half, kind, core)
        return remote(
            ref,
            ref,
            ag_send.at[block, half, kind, way],
            recv,
            to_sp,
            sibling if way == SIBLING else tp,
        )

    def ag_arrived(block, half, kind, from_sibling):
        whose = 1 - core if from_sibling else core
        ref = piece(block, half, kind, whose)
        recv = ag_recv.at[block, half, kind + (2 if from_sibling else 0)]
        remote(ref, ref, ag_send.at[block, half, kind, SIBLING], recv, sp, sibling).wait_recv()

    def ag_ways(zc, half, col_is_own, kind, act):
        block = zc * x_size + (x if col_is_own else 1 - x)

        if col_is_own and kind == XF:

            @pl.when(zc == z)
            def _():
                act(ag_copy(block, half, kind, ACROSS))

        if col_is_own or kind == XF:

            @pl.when((zc <= z) & (z < far_z))
            def _():
                act(ag_copy(block, half, kind, UP))

            @pl.when((zc >= z) & (z > 0))
            def _():
                act(ag_copy(block, half, kind, DOWN))

        if col_is_own and kind == ZF:
            act(ag_copy(block, half, kind, ACROSS))
        if col_is_own:

            @pl.when(zc != z)
            def _():
                act(ag_copy(block, half, kind, SIBLING))

        else:
            act(ag_copy(block, half, kind, SIBLING))

    def start(copy):
        copy.start()

    def take(zc, half, col_is_own, kind):
        block = zc * x_size + (x if col_is_own else 1 - x)
        ag_arrived(block, half, kind, False)
        ag_ways(zc, half, col_is_own, kind, start)

    for whose in range(core_count):
        for half in range(halves):
            mix_rows(half * half_rows + (core if whose == 0 else 1 - core) * core_rows, core_rows)
            if whose == 0:
                ag_ways(z, half, True, XF, start)
                ag_ways(z, half, True, ZF, start)

    for d in range(1, n_sp):
        src_sp = (sp + d) % n_sp
        remote(
            route_all.at[sp], route_all.at[src_sp], route_send.at[d], route_recv.at[src_sp], src_sp, tp
        ).wait_recv()
    for load in loads[2:]:
        load.wait()

    upper = z >= (nz + 1) // 2
    low_z = jnp.where(upper, far_z - z, z)

    def plane_at(step):
        plane = jnp.where(step <= low_z, low_z - step, step)
        return jnp.where(upper, far_z - plane, plane)

    inner = low_z > 0

    def unit_at(k):
        paired = inner & (k >= 2) & (k < 6)
        step = jnp.where(paired, 1 + k % 2, k // halves)
        return plane_at(step), jnp.where(paired, k // 4, k % halves)

    n_hidden = hidden.shape[1]
    hidden_tile = min(256, n_hidden)

    def span_of(half):
        return pl.ds(pl.multiple_of(half * half_rows, half_rows), half_rows)

    def part_copy(block, half, q_y):
        q = q_y * core_count + (1 - core)
        return remote(
            parts.at[block, q, span_of(half)],
            parts_in.at[block, q_y, span_of(half)],
            part_send.at[block, half, q_y],
            part_recv.at[block, half, q_y],
            sp,
            sibling,
        )

    def pair_copy(block, half):
        return remote(
            pair_out.at[block, span_of(half)],
            pair_in.at[block, span_of(half)],
            pair_send.at[block, half],
            pair_recv.at[block, half],
            sp,
            opposite,
        )

    def side_copy(zc, half):
        return remote(
            side_out.at[zc, span_of(half)],
            side_in.at[zc, span_of(half)],
            side_send.at[zc, half],
            side_recv.at[zc, half],
            z * x_size + (1 - x),
            tp,
        )

    def far_copy(zc, half):
        return remote(
            far_out.at[zc, span_of(half)],
            far_in.at[z, span_of(half)],
            far_send.at[zc, half],
            far_recv.at[z, half],
            zc * x_size + x,
            tp,
        )

    def compute(block, half):
        own_row = lax.broadcasted_iota(jnp.int32, (route_rows, half_rows), 0) == sp
        weight = jnp.sum(
            jnp.where(own_row, route_all[block, :, span_of(half)], 0.0), axis=0, keepdims=True
        )
        weight = jnp.broadcast_to(weight, (128, half_rows)).T
        for j in range(n_hidden // hidden_tile):
            span = slice(j * hidden_tile, (j + 1) * hidden_tile)
            data = tokens[block, span_of(half), :]
            gate = jnp.dot(data, w_gate[:, span], preferred_element_type=jnp.float32)
            up = jnp.dot(data, w_up[:, span], preferred_element_type=jnp.float32)
            gate_cut = jnp.minimum(gate + gate_bias[:, span], clamp_limit)
            up_cut = jnp.clip(up + up_bias[:, span], -clamp_limit, clamp_limit)
            active = (up_cut + 1.0) * (gate_cut * jax.nn.sigmoid(sigmoid_alpha * gate_cut))
            for i in range(hidden_tile // 128):
                lane = slice(i * 128, (i + 1) * 128)
                at = j * hidden_tile + i * 128
                hidden[:, at : at + 128] = (active[:, lane] * weight).astype(jnp.bfloat16)

        def down(i, carry):
            whose = jnp.where(i < 2, 1 - core, core)
            q = (i % 2) * core_count + whose
            at = pl.ds(pl.multiple_of(q * cols, cols), cols)
            parts[block, q, span_of(half), :] = jnp.dot(
                hidden[...], w_down[:, at], preferred_element_type=jnp.float32
            ).astype(jnp.bfloat16)

            @pl.when(i < 2)
            def _():
                part_copy(block, half, i % 2).start()

            return carry

        lax.fori_loop(0, n_tp, down, 0)

    def wide_of(ref, *at):
        return ref[at].astype(jnp.float32)

    def join_cores(block, half):
        at = span_of(half)
        for q_y in range(n_tp // core_count):
            part_copy(block, half, q_y).wait_recv()
        away = wide_of(parts, block, opposite, at) + wide_of(parts_in, block, 1 - y, at)
        pair_out[block, at, :] = away.astype(jnp.bfloat16)
        pair_copy(block, half).start()
        pair_keep[block, at, :] = wide_of(parts, block, tp, at) + wide_of(parts_in, block, y, at)

    def join_pair_other(k):
        zc, half = unit_at(k)
        at = span_of(half)
        block = zc * x_size + (1 - x)
        pair_copy(block, half).wait_recv()
        both = pair_keep[block, at, :] + wide_of(pair_in, block, at)
        side_out[zc, at, :] = both.astype(jnp.bfloat16)
        side_copy(zc, half).start()

    def join_pair_own(k):
        zc, half = unit_at(k)
        at = span_of(half)
        block = zc * x_size + x
        pair_copy(block, half).wait_recv()
        total[zc, at, :] = pair_keep[block, at, :] + wide_of(pair_in, block, at)

    def join_sides(k):
        zc, half = unit_at(k)
        at = span_of(half)
        side_copy(zc, half).wait_recv()
        value = total[zc, at, :] + wide_of(side_in, zc, at)
        total[zc, at, :] = value

        @pl.when(zc != z)
        def _():
            far_out[zc, at, :] = value.astype(jnp.bfloat16)
            far_copy(zc, half).start()

    units = nz * halves

    def unit_body(k, carry):
        zc, half = unit_at(k)
        own, other = zc * x_size + x, zc * x_size + (1 - x)

        @pl.when(inner & (k >= 1) & (k + 1 < units))
        def _():
            z_next, half_next = unit_at(k + 1)
            take(z_next, half_next, True, ZF)
            take(z_next, half_next, True, XF)
            take(z_next, half_next, False, XF)

        @pl.when((~inner) & (k >= halves))
        def _():
            take(zc, half, True, ZF)
            take(zc, half, True, XF)

        @pl.when(k >= halves)
        def _():
            ag_arrived(own, half, XF, True)
            ag_arrived(own, half, ZF, True)

        compute(own, half)
        join_cores(own, half)

        @pl.when((~inner) | (k < halves))
        def _():
            take(zc, half, False, XF)

        @pl.when(k >= 1)
        def _():
            join_pair_own(k - 1)
            join_pair_other(k - 1)

        @pl.when((~inner) & (k >= 2))
        def _():
            join_sides(k - 2)

        take(zc, half, False, ZF)
        ag_arrived(other, half, XF, True)
        ag_arrived(other, half, ZF, True)
        compute(other, half)
        join_cores(other, half)
        return carry

    lax.fori_loop(0, units, unit_body, 0)

    @pl.when(inner)
    def _():
        def sides(k, carry):
            join_sides(k)
            return carry

        lax.fori_loop(0, units - 2, sides, 0)

    join_pair_own(units - 1)
    join_pair_other(units - 1)
    join_sides(units - 2)
    join_sides(units - 1)

    combined = total[z]
    for d in range(1, nz):
        src_z = (z + d) % nz
        for half in range(halves):
            remote(
                far_out.at[src_z, span_of(half)],
                far_in.at[src_z, span_of(half)],
                far_send.at[src_z, half],
                far_recv.at[src_z, half],
                src_z * x_size + x,
                tp,
            ).wait_recv()
        combined += far_in[src_z].astype(jnp.float32)
    total[z] = combined

    own_squares = jnp.sum(combined * combined, axis=1, keepdims=True)
    squares[tp] = jnp.broadcast_to(own_squares, (rows, 128)).T[:8]

    def squares_copy(d):
        return remote(
            squares.at[tp], squares.at[tp], sq_send.at[d], sq_recv.at[tp], sp, (tp + d) % n_tp
        )

    for d in range(1, n_tp):
        squares_copy(d).start()
    summed = squares[tp]
    for d in range(1, n_tp):
        src_tp = (tp + d) % n_tp
        remote(
            squares.at[tp], squares.at[src_tp], sq_send.at[d], sq_recv.at[src_tp], sp, src_tp
        ).wait_recv()
        summed += squares[src_tp]
    row_scale = lax.rsqrt(summed[:1] / width + epsilon)
    row_scale = jnp.broadcast_to(row_scale, (128, rows)).T
    for i in range(cols // 128):
        lane = slice(i * 128, (i + 1) * 128)
        own = mixed[:, pl.ds(pl.multiple_of(tp * cols + i * 128, 128), 128)].astype(jnp.float32)
        out_ref[:, lane] = (own + total[z, :, lane] * row_scale * expert_norm[:, lane]).astype(
            jnp.bfloat16
        )

    def sent(copy):
        copy.wait_send()

    for side in range(2):
        edge_loop(side, sent)
    for d in range(1, n_tp):
        for copy in front_copies(d):
            sent(copy)
        sent(squares_copy(d))
    for d in range(1, n_sp):
        sent(route_copy(d))

    def all_sent(k, carry):
        zc, half = k // halves, k % halves
        for col_is_own in (True, False):
            for kind in (XF, ZF):
                ag_ways(zc, half, col_is_own, kind, sent)
        for i in range(x_size):
            block = zc * x_size + i
            for q_y in range(n_tp // core_count):
                sent(part_copy(block, half, q_y))
            sent(pair_copy(block, half))
        sent(side_copy(zc, half))

        @pl.when(zc != z)
        def _():
            sent(far_copy(zc, half))

        return carry

    lax.fori_loop(0, units, all_sent, 0)


def gathered_shards(*args):
    pool_in, pool_norm, out_weight, stream = args[0], args[3], args[4], args[5]
    w_gate, w_down = args[10], args[14]
    n_sp, n_tp = lax.axis_size("sp"), lax.axis_size("tp")
    nz = n_sp // x_size
    rows, width = stream.shape
    n_hidden = w_gate.shape[2]
    cols = width // n_tp
    group_width = pool_in.shape[1]
    bf16, f32 = jnp.bfloat16, jnp.float32
    row_args = (2, 3, 6, 7, 15)
    args = [a.reshape(1, -1) if i in row_args else a for i, a in enumerate(args)]
    args[8], args[9] = args[8].T, args[9].T
    in_hbm = (4, 5, 10, 11, 14)
    in_specs = [
        pl.BlockSpec(memory_space=pl.ANY if i in in_hbm else pltpu.VMEM) for i in range(len(args))
    ]
    edge = 2 * reach_rows
    route_rows = -(-n_sp // 8) * 8
    dma = pltpu.SemaphoreType.DMA
    scratch = [
        pltpu.VMEM((n_sp, rows, width), bf16),
        pltpu.VMEM((width, n_hidden), bf16),
        pltpu.VMEM((width, n_hidden), bf16),
        pltpu.VMEM((n_hidden, width), bf16),
        pltpu.VMEM(out_weight.shape, bf16),
        pltpu.VMEM((rows, width), bf16),
        pltpu.VMEM((n_tp, rows, group_width), bf16),
        pltpu.VMEM((n_tp, 2, edge, group_width), bf16),
        pltpu.VMEM((n_tp, group_width, group_width), bf16),
        pltpu.VMEM((n_tp, 1, group_width), f32),
        pltpu.VMEM((n_tp, rows + 2 * reach_rows, group_width), f32),
        pltpu.VMEM((rows, n_tp * group_width), bf16),
        pltpu.VMEM((rows, width), f32),
        pltpu.VMEM((rows, width), bf16),
        pltpu.VMEM((n_sp, route_rows, rows), f32),
        pltpu.VMEM((rows // halves, n_hidden), bf16),
        pltpu.VMEM((n_sp, n_tp, rows, cols), bf16),
        pltpu.VMEM((n_sp, n_tp // core_count, rows, cols), bf16),
        pltpu.VMEM((n_sp, rows, cols), bf16),
        pltpu.VMEM((n_sp, rows, cols), f32),
        pltpu.VMEM((n_sp, rows, cols), bf16),
        pltpu.VMEM((nz, rows, cols), bf16),
        pltpu.VMEM((nz, rows, cols), bf16),
        pltpu.VMEM((nz, rows, cols), f32),
        pltpu.VMEM((nz, rows, cols), bf16),
        pltpu.VMEM((nz, rows, cols), bf16),
        pltpu.VMEM((n_tp, 8, rows), f32),
        dma((5,)),
        dma((n_sp, halves, 2, 4)),
        dma((n_sp, halves, 4)),
        dma((n_tp, 3)),
        dma((n_tp, 3)),
        dma((2, n_tp)),
        dma((n_tp, 2)),
        dma((n_sp,)),
        dma((n_sp,)),
        dma((n_sp, halves, n_tp // core_count)),
        dma((n_sp, halves, n_tp // core_count)),
        dma((n_sp, halves)),
        dma((n_sp, halves)),
        dma((nz, halves)),
        dma((nz, halves)),
        dma((nz, halves)),
        dma((nz, halves)),
        dma((n_tp,)),
        dma((n_tp,)),
    ]
    return pl.pallas_call(
        functools.partial(layer_kernel, nz),
        out_shape=jax.ShapeDtypeStruct((rows, cols), bf16),
        in_specs=in_specs,
        out_specs=pl.BlockSpec(memory_space=pltpu.VMEM),
        scratch_shapes=scratch,
        compiler_params=pltpu.CompilerParams(
            collective_id=0, has_side_effects=True, vmem_limit_bytes=vmem_limit
        ),
        name="layer",
    )(*args)


def shards(*args):
    pool_in, out_weight, stream, w_gate = args[0], args[4], args[5], args[10]
    n_sp, n_tp = lax.axis_size("sp"), lax.axis_size("tp")
    rows, width = stream.shape
    cols, n_hidden = width // n_tp, w_gate.shape[2]
    slots = n_sp * rows * (2 * width + (2 + 1 + 1 + 2 + 1) * 2 * cols + 2 * width + 2 * width)
    fixed = 2 * (3 * width * n_hidden + out_weight.size) + 10 * rows * width
    fits = slots + fixed < vmem_limit * 9 // 10
    shaped = (
        n_tp == 2 * core_count
        and n_sp % x_size == 0
        and w_gate.shape[0] == 1
        and rows % (128 * halves) == 0
        and width % (128 * first_share[0]) == 0
        and cols % 128 == 0
        and n_hidden % 256 == 0
        and pool_in.shape[1] == 128
        and n_sp <= 128
    )
    return (gathered_shards if fits and shaped else routed_shards)(*args)


def solution(mesh):
    in_specs = (
        P("sp", "tp"),
        P("tp", None, None),
        P("tp"),
        P(),
        P(),
        P("sp", None),
        P(),
        P(),
        P("sp", None),
        P("sp", None),
        P("sp", None, "tp"),
        P("sp", None, "tp"),
        P("sp", "tp"),
        P("sp", "tp"),
        P("sp", "tp", None),
        P("tp"),
    )
    out_specs = P("sp", "tp")
    return jax.shard_map(shards, mesh=mesh, in_specs=in_specs, out_specs=out_specs, check_vma=False)
```

```python
import functools

import jax
import jax.numpy as jnp
from jax import lax
from jax.experimental import pallas as pl
from jax.experimental.pallas import tpu as pltpu
from jax.sharding import PartitionSpec as P

MESH = pl.DeviceIdType.MESH

epsilon = 1e-06
reach_rows = 8
clamp_limit = 7.0
sigmoid_alpha = 1.702
chunk_counts = (2,)


def extended_2(shard, sides, width):
    for axis, dim in sides:
        count, length = (lax.axis_size(axis), shard.shape[dim])
        up = [(i, (i + 1) % count) for i in range(count - 1)]
        down = [(j, i) for i, j in up]
        last = lax.slice_in_dim(shard, length - width, length, axis=dim)
        leading = lax.slice_in_dim(shard, 0, width, axis=dim)
        before = lax.ppermute(last, axis, up)
        after = lax.ppermute(leading, axis, down)
        shard = jnp.concatenate([before, shard, after], axis=dim)
    return shard


def rms_scale(values):
    return values * lax.rsqrt(jnp.mean(values * values, axis=-1, keepdims=True) + epsilon)


def routed_shards(
    pool_in,
    pool_weight,
    pool_scale,
    pool_norm,
    out_weight,
    stream,
    mix_norm,
    ffn_norm,
    routes,
    route_weights,
    w_gate,
    w_up,
    gate_bias,
    up_bias,
    w_down,
    expert_norm,
):
    rows_dev = pool_in.shape[0]
    length = rows_dev * lax.axis_size("sp")
    radius = jnp.left_shift(1, lax.axis_index("tp"))
    positions = lax.axis_index("sp") * rows_dev + jnp.arange(rows_dev)
    padded = extended_2(pool_in, (("sp", 0),), reach_rows).astype(jnp.float32)
    window_sum = jnp.zeros((rows_dev, pool_in.shape[1]), jnp.float32)
    counts = jnp.zeros((rows_dev,), jnp.float32)
    for offset in range(-reach_rows, reach_rows + 1):
        inside = (positions + offset >= 0) & (positions + offset < length) & (abs(offset) <= radius)
        window_sum = window_sum + jnp.where(
            inside[:, None], padded[reach_rows + offset : reach_rows + offset + rows_dev], 0.0
        )
        counts = counts + inside.astype(jnp.float32)
    deviation = (window_sum / counts[:, None] - padded[reach_rows : reach_rows + rows_dev]).astype(
        jnp.bfloat16
    )
    pool_out = (
        jnp.dot(deviation, pool_weight[0], preferred_element_type=jnp.float32) * pool_scale
    ).astype(jnp.bfloat16)
    all_groups = lax.all_gather(pool_out, "tp", axis=1, tiled=True)
    normed = (rms_scale(all_groups.astype(jnp.float32)) * pool_norm).astype(jnp.bfloat16)
    mix_out = jnp.dot(normed, out_weight, preferred_element_type=jnp.float32)
    mixed = (stream.astype(jnp.float32) + rms_scale(mix_out) * mix_norm).astype(jnp.bfloat16)
    expert_in = (rms_scale(mixed.astype(jnp.float32)) * ffn_norm).astype(jnp.bfloat16)
    model_width = mixed.shape[1]
    experts = lax.axis_size("sp") * w_gate.shape[0]
    top_count = routes.shape[1]
    capacity = rows_dev * top_count * 3 // (2 * experts)
    quarter = capacity // lax.axis_size("tp")
    chunks = next((n for n in chunk_counts if quarter % (8 * n) == 0), 1)
    chunk_rows, own_rows = capacity // chunks, quarter // chunks

    names = routes.T[:, None, :] == jnp.arange(experts, dtype=jnp.int32)[None, :, None]
    member = jnp.any(names, axis=0)
    weight = jnp.sum(jnp.where(names, route_weights.T[:, None, :], 0.0), axis=0)
    order = jnp.arange(rows_dev)
    earlier = (order[:, None] < order[None, :]).astype(jnp.bfloat16)
    place = jnp.dot(
        member.astype(jnp.bfloat16), earlier, preferred_element_type=jnp.float32
    ).astype(jnp.int32)
    place = jnp.where(member, place, -1)

    def dispatched(chunk):
        first = chunk * chunk_rows + lax.axis_index("tp") * own_rows
        slots = first + jnp.arange(own_rows, dtype=jnp.int32)
        pick = (place[:, None, :] == slots[None, :, None]).astype(jnp.bfloat16)
        rows = jnp.dot(pick.reshape(experts * own_rows, rows_dev), expert_in)
        own_slots = rows.reshape(experts, own_rows, model_width)
        arrived = lax.all_to_all(own_slots, "sp", split_axis=0, concat_axis=0, tiled=True)
        return lax.all_gather(arrived, "tp", axis=1, tiled=True)

    def expert(slot_block):
        row_block = slot_block.reshape(-1, model_width)
        gate_pre = jnp.dot(row_block, w_gate[0], preferred_element_type=jnp.float32) + gate_bias[0]
        up_pre = jnp.dot(row_block, w_up[0], preferred_element_type=jnp.float32) + up_bias[0]
        gate_cut = jnp.minimum(gate_pre, clamp_limit)
        up_cut = jnp.clip(up_pre, -clamp_limit, clamp_limit)
        activation = (
            (up_cut + 1.0) * (gate_cut * jax.nn.sigmoid(sigmoid_alpha * gate_cut))
        ).astype(jnp.bfloat16)
        partial_value = jnp.dot(activation, w_down[0], preferred_element_type=jnp.float32).astype(
            jnp.bfloat16
        )
        partial_value = partial_value.reshape(slot_block.shape)
        summed = lax.psum_scatter(partial_value, "tp", scatter_dimension=2, tiled=True)
        return lax.all_to_all(summed, "sp", split_axis=0, concat_axis=0, tiled=True)

    def weighted(chunk, returned):
        slots = chunk * chunk_rows + jnp.arange(chunk_rows, dtype=jnp.int32)
        spread = jnp.where(place[:, None, :] == slots[None, :, None], weight[:, None, :], 0.0)
        spread = spread.reshape(experts * chunk_rows, rows_dev)
        high = spread.astype(jnp.bfloat16)
        low = (spread - high.astype(jnp.float32)).astype(jnp.bfloat16)
        flat = returned.reshape(experts * chunk_rows, -1)
        over_slots = (((0,), (0,)), ((), ()))
        return lax.dot_general(
            high, flat, over_slots, preferred_element_type=jnp.float32
        ) + lax.dot_general(low, flat, over_slots, preferred_element_type=jnp.float32)

    blocks = [dispatched(chunk) for chunk in range(chunks)]
    parts = [expert(block) for block in blocks]
    col_count = parts[0].shape[2]
    combined = sum(weighted(chunk, part) for chunk, part in enumerate(parts))
    squares = lax.psum(jnp.sum(combined * combined, axis=1), "tp")
    row_scale = lax.rsqrt(squares / model_width + epsilon)
    own_cols = lax.dynamic_slice_in_dim(
        mixed.astype(jnp.float32), lax.axis_index("tp") * col_count, col_count, 1
    )
    return (own_cols + combined * row_scale[:, None] * expert_norm).astype(jnp.bfloat16)


x_size = 2
core_count = 2
halves = 2
first_share = 8, 3
vmem_limit = 60 * 1024 * 1024
UP, DOWN, ACROSS, SIBLING = range(4)
XF, ZF = range(2)


def layer_kernel(
    nz,
    pool_in,
    pool_weight,
    pool_scale,
    pool_norm,
    out_weight_hbm,
    stream_hbm,
    mix_norm,
    ffn_norm,
    routes,
    route_weights,
    w_gate_hbm,
    w_up_hbm,
    gate_bias,
    up_bias,
    w_down_hbm,
    expert_norm,
    out_ref,
    tokens,
    w_gate,
    w_up,
    w_down,
    out_weight,
    stream,
    pool_all,
    pool_edges,
    weight_all,
    scale_all,
    padded,
    normed,
    mix_out,
    mixed,
    route_all,
    hidden,
    parts,
    parts_in,
    pair_out,
    pair_keep,
    pair_in,
    side_out,
    side_in,
    total,
    far_out,
    far_in,
    squares,
    load_sem,
    ag_send,
    ag_recv,
    front_send,
    front_recv,
    edge_send,
    edge_recv,
    route_send,
    route_recv,
    part_send,
    part_recv,
    pair_send,
    pair_recv,
    side_send,
    side_recv,
    far_send,
    far_recv,
    sq_send,
    sq_recv,
):
    sp, tp = lax.axis_index("sp"), lax.axis_index("tp")
    n_sp = nz * x_size
    n_tp = pool_all.shape[0]
    z, x = sp // x_size, sp % x_size
    y, core = tp // core_count, tp % core_count
    rows, width = stream.shape
    cols = out_ref.shape[1]
    group_width = pool_in.shape[1]
    half_rows = rows // halves
    core_rows = half_rows // core_count
    first_cols = width * first_share[1] // first_share[0]
    sibling = y * core_count + (1 - core)
    opposite = (1 - y) * core_count + core
    far_z = nz - 1

    def remote(src, dst, send, recv, to_sp, to_tp):
        return pltpu.make_async_remote_copy(
            src_ref=src,
            dst_ref=dst,
            send_sem=send,
            recv_sem=recv,
            device_id=(to_sp, to_tp),
            device_id_type=MESH,
        )

    def wait_bytes(ref, sem):
        pltpu.make_async_copy(ref, ref, sem).wait()

    loads = [
        pltpu.make_async_copy(src, dst, load_sem.at[i])
        for i, (src, dst) in enumerate(
            (
                (out_weight_hbm, out_weight),
                (stream_hbm, stream),
                (w_gate_hbm.at[0], w_gate),
                (w_up_hbm.at[0], w_up),
                (w_down_hbm.at[0], w_down),
            )
        )
    ]
    for load in loads:
        load.start()

    barrier = pltpu.get_barrier_semaphore()

    def greet(to_sp, to_tp):
        pl.semaphore_signal(barrier, inc=1, device_id=(to_sp, to_tp), device_id_type=MESH)

    for d in range(1, n_sp):
        greet((sp + d) % n_sp, tp)
    for d in range(1, n_tp):
        greet(sp, (tp + d) % n_tp)

    @pl.when(sp > 0)
    def _():
        for d in range(1, n_tp):
            greet(sp - 1, (tp + d) % n_tp)

    @pl.when(sp < n_sp - 1)
    def _():
        for d in range(1, n_tp):
            greet(sp + 1, (tp + d) % n_tp)

    near = (sp > 0).astype(jnp.int32) + (sp < n_sp - 1).astype(jnp.int32)
    pl.semaphore_wait(barrier, (n_sp - 1) + (n_tp - 1) * (1 + near))

    edge = pool_edges.shape[2]

    def edge_copy(side, to_tp):
        src = pool_in.at[pl.ds(rows - edge, edge)] if side == 0 else pool_in.at[pl.ds(0, edge)]
        return remote(
            src,
            pool_edges.at[tp, side],
            edge_send.at[side],
            edge_recv.at[side],
            sp + 1 if side == 0 else sp - 1,
            to_tp,
        )

    for side in range(2):

        @pl.when(sp < n_sp - 1 if side == 0 else sp > 0)
        def _():
            for d in range(n_tp):
                edge_copy(side, (tp + d) % n_tp).start()

    def front_copies(d):
        to = (tp + d) % n_tp
        return [
            remote(pool_in, pool_all.at[tp], front_send.at[0], front_recv.at[0], sp, to),
            remote(pool_weight.at[0], weight_all.at[tp], front_send.at[1], front_recv.at[1], sp, to),
            remote(pool_scale, scale_all.at[tp], front_send.at[2], front_recv.at[2], sp, to),
        ]

    for d in range(1, n_tp):
        for copy in front_copies(d):
            copy.start()
    pool_all[tp] = pool_in[...]
    weight_all[tp] = pool_weight[0]
    scale_all[tp] = pool_scale[...]

    route_rows = route_all.shape[1]
    names = lax.broadcasted_iota(jnp.int32, (route_rows, rows), 0)
    by_expert = jnp.zeros((route_rows, rows), jnp.float32)
    for k in range(routes.shape[0]):
        by_expert += jnp.where(routes[k : k + 1, :] == names, route_weights[k : k + 1, :], 0.0)
    route_all[sp] = by_expert

    def route_copy(d):
        to = (sp + d) % n_sp
        return remote(
            route_all.at[sp], route_all.at[sp], route_send.at[0], route_recv.at[0], to, tp
        )

    for d in range(1, n_sp):
        route_copy(d).start()

    others = pl.ds(0, n_tp - 1)
    front_all = (pool_all, weight_all, scale_all)
    for i, ref in enumerate(front_all):
        wait_bytes(ref.at[others], front_recv.at[i])

    @pl.when(sp > 0)
    def _():
        wait_bytes(pool_edges.at[:, 0], edge_recv.at[0])
        for g in range(n_tp):
            padded[g, 0:reach_rows, :] = pool_edges[g, 0].astype(jnp.float32)[edge - reach_rows :]

    @pl.when(sp == 0)
    def _():
        padded[:, 0:reach_rows, :] = jnp.zeros((n_tp, reach_rows, group_width), jnp.float32)

    @pl.when(sp < n_sp - 1)
    def _():
        wait_bytes(pool_edges.at[:, 1], edge_recv.at[1])
        for g in range(n_tp):
            padded[g, reach_rows + rows :, :] = pool_edges[g, 1].astype(jnp.float32)[:reach_rows]

    @pl.when(sp == n_sp - 1)
    def _():
        padded[:, reach_rows + rows :, :] = jnp.zeros((n_tp, reach_rows, group_width), jnp.float32)

    positions = sp * rows + lax.broadcasted_iota(jnp.int32, (rows, group_width), 0)
    mean_square = jnp.zeros((rows, 1), jnp.float32)
    for g in range(n_tp):
        radius = 1 << g
        values = pool_all[g].astype(jnp.float32)
        padded[g, reach_rows : reach_rows + rows, :] = values
        window_sum = values
        for offset in range(1, radius + 1):
            window_sum += padded[g, reach_rows + offset : reach_rows + offset + rows, :]
            window_sum += padded[g, reach_rows - offset : reach_rows - offset + rows, :]
        last = jnp.minimum(positions + radius, n_sp * rows - 1)
        counts = last - jnp.maximum(positions - radius, 0) + 1
        deviation = (window_sum / counts.astype(jnp.float32) - values).astype(jnp.bfloat16)
        pool_out = (
            jnp.dot(deviation, weight_all[g], preferred_element_type=jnp.float32) * scale_all[g]
        ).astype(jnp.bfloat16)
        normed[:, g * group_width : (g + 1) * group_width] = pool_out
        wide = pool_out.astype(jnp.float32)
        mean_square += jnp.sum(wide * wide, axis=1, keepdims=True)
    pool_width = n_tp * group_width
    row_scale = lax.rsqrt(mean_square / pool_width + epsilon)
    normed[...] = (normed[...].astype(jnp.float32) * row_scale * pool_norm[...]).astype(jnp.bfloat16)

    for load in loads[:2]:
        load.wait()
    for t in range(width // cols):
        mix_out[:, t * cols : (t + 1) * cols] = jnp.dot(
            normed[...], out_weight[:, t * cols : (t + 1) * cols], preferred_element_type=jnp.float32
        )

    tile = 32

    def mix_rows(first, count):
        def body(i, carry):
            part = pl.ds(pl.multiple_of(first + i * tile, tile), tile)
            value = mix_out[part, :]
            scaled = value * lax.rsqrt(jnp.mean(value * value, axis=1, keepdims=True) + epsilon)
            summed = stream[part, :].astype(jnp.float32) + scaled * mix_norm[...]
            summed = summed.astype(jnp.bfloat16)
            mixed[part, :] = summed
            wide = summed.astype(jnp.float32)
            wide = wide * lax.rsqrt(jnp.mean(wide * wide, axis=1, keepdims=True) + epsilon)
            tokens[sp, part, :] = (wide * ffn_norm[...]).astype(jnp.bfloat16)
            return carry

        lax.fori_loop(0, count // tile, body, 0)

    def piece(block, half, kind, whose):
        first = pl.multiple_of(half * half_rows + whose * core_rows, 16)
        span = pl.ds(0, first_cols) if kind == XF else pl.ds(first_cols, width - first_cols)
        return tokens.at[block, pl.ds(first, core_rows), span]

    def ag_copy(block, half, kind, way, lane_of=0):
        to_sp = {UP: sp + x_size, DOWN: sp - x_size, ACROSS: z * x_size + (1 - x), SIBLING: sp}[way]
        recv = ag_recv.at[block, half, 2 if way == SIBLING else kind]
        ref = piece(block, half, kind, core)
        to_tp = sibling if way == SIBLING else tp
        return remote(ref, ref, ag_send.at[way, lane_of], recv, to_sp, to_tp)

    def ag_arrived(block, half, kind):
        wait_bytes(piece(block, half, kind, core), ag_recv.at[block, half, kind])

    def sibling_arrived(block, half):
        first = pl.multiple_of(half * half_rows + (1 - core) * core_rows, 16)
        wait_bytes(tokens.at[block, pl.ds(first, core_rows), :], ag_recv.at[block, half, 2])

    def ag_start(zc, half, col_is_own, kind):
        block = zc * x_size + (x if col_is_own else 1 - x)

        if col_is_own and kind == XF:

            @pl.when(zc == z)
            def _():
                ag_copy(block, half, kind, ACROSS).start()

        lane_of = 0 if col_is_own else 1
        if col_is_own or kind == XF:

            @pl.when((zc <= z) & (z < far_z))
            def _():
                ag_copy(block, half, kind, UP, lane_of).start()

            @pl.when((zc >= z) & (z > 0))
            def _():
                ag_copy(block, half, kind, DOWN, lane_of).start()

        if col_is_own and kind == ZF:

            @pl.when(zc == z)
            def _():
                ag_copy(block, half, kind, ACROSS).start()

            @pl.when(zc != z)
            def _():
                ag_copy(block, half, kind, ACROSS, 1).start()

        if col_is_own:

            @pl.when(zc != z)
            def _():
                ag_copy(block, half, kind, SIBLING).start()

        else:
            ag_copy(block, half, kind, SIBLING).start()

    def ag_sent():
        carried = pl.ds(0, halves * core_rows)
        xf, zf = pl.ds(0, first_cols), pl.ds(first_cols, width - first_cols)
        wait_bytes(tokens.at[pl.ds(0, n_sp - 1), carried, :], ag_send.at[SIBLING, 0])
        wait_bytes(tokens.at[0, carried, :], ag_send.at[ACROSS, 0])
        if nz > 1:
            wait_bytes(tokens.at[pl.ds(0, nz - 1), carried, zf], ag_send.at[ACROSS, 1])
        for at_z in range(nz):

            @pl.when(z == at_z)
            def _():
                if at_z < far_z:
                    wait_bytes(tokens.at[pl.ds(0, at_z + 1), carried, :], ag_send.at[UP, 0])
                    wait_bytes(tokens.at[pl.ds(0, at_z + 1), carried, xf], ag_send.at[UP, 1])
                if at_z > 0:
                    wait_bytes(tokens.at[pl.ds(0, nz - at_z), carried, :], ag_send.at[DOWN, 0])
                    wait_bytes(tokens.at[pl.ds(0, nz - at_z), carried, xf], ag_send.at[DOWN, 1])

    def take(zc, half, col_is_own, kind):
        block = zc * x_size + (x if col_is_own else 1 - x)
        ag_arrived(block, half, kind)
        ag_start(zc, half, col_is_own, kind)

    for whose in range(core_count):
        for half in range(halves):
            mix_rows(half * half_rows + (core if whose == 0 else 1 - core) * core_rows, core_rows)
            if whose == 0:
                ag_start(z, half, True, XF)
                ag_start(z, half, True, ZF)

    wait_bytes(route_all.at[pl.ds(0, n_sp - 1)], route_recv.at[0])
    for load in loads[2:]:
        load.wait()

    upper = z >= (nz + 1) // 2
    low_z = jnp.where(upper, far_z - z, z)

    def plane_at(step):
        plane = jnp.where(step <= low_z, low_z - step, step)
        return jnp.where(upper, far_z - plane, plane)

    inner = low_z > 0

    def unit_at(k):
        paired = inner & (k >= 2) & (k < 6)
        step = jnp.where(paired, 1 + k % 2, k // halves)
        return plane_at(step), jnp.where(paired, k // 4, k % halves)

    n_hidden = hidden.shape[1]
    hidden_tile = min(256, n_hidden)

    def span_of(half):
        return pl.ds(pl.multiple_of(half * half_rows, half_rows), half_rows)

    def part_copy(block, half, q_y):
        q = q_y * core_count + (1 - core)
        return remote(
            parts.at[block, q, span_of(half)],
            parts_in.at[block, q_y, span_of(half)],
            part_send.at[0],
            part_recv.at[block, half],
            sp,
            sibling,
        )

    def pair_copy(block, half):
        return remote(
            pair_out.at[block, span_of(half)],
            pair_in.at[block, span_of(half)],
            pair_send.at[0],
            pair_recv.at[block, half],
            sp,
            opposite,
        )

    def side_copy(zc, half):
        return remote(
            side_out.at[zc, span_of(half)],
            side_in.at[zc, span_of(half)],
            side_send.at[0],
            side_recv.at[zc, half],
            z * x_size + (1 - x),
            tp,
        )

    def far_copy(zc, half):
        return remote(
            far_out.at[zc, span_of(half)],
            far_in.at[z, span_of(half)],
            far_send.at[0],
            far_recv.at[0],
            zc * x_size + x,
            tp,
        )

    def compute(block, half):
        own_row = lax.broadcasted_iota(jnp.int32, (route_rows, half_rows), 0) == sp
        weight = jnp.sum(
            jnp.where(own_row, route_all[block, :, span_of(half)], 0.0), axis=0, keepdims=True
        )
        weight = jnp.broadcast_to(weight, (128, half_rows)).T
        for j in range(n_hidden // hidden_tile):
            span = slice(j * hidden_tile, (j + 1) * hidden_tile)
            data = tokens[block, span_of(half), :]
            gate = jnp.dot(data, w_gate[:, span], preferred_element_type=jnp.float32)
            up = jnp.dot(data, w_up[:, span], preferred_element_type=jnp.float32)
            gate_cut = jnp.minimum(gate + gate_bias[:, span], clamp_limit)
            up_cut = jnp.clip(up + up_bias[:, span], -clamp_limit, clamp_limit)
            active = (up_cut + 1.0) * (gate_cut * jax.nn.sigmoid(sigmoid_alpha * gate_cut))
            for i in range(hidden_tile // 128):
                lane = slice(i * 128, (i + 1) * 128)
                at = j * hidden_tile + i * 128
                hidden[:, at : at + 128] = (active[:, lane] * weight).astype(jnp.bfloat16)

        def down(i, carry):
            whose = jnp.where(i < 2, 1 - core, core)
            q = (i % 2) * core_count + whose
            at = pl.ds(pl.multiple_of(q * cols, cols), cols)
            parts[block, q, span_of(half), :] = jnp.dot(
                hidden[...], w_down[:, at], preferred_element_type=jnp.float32
            ).astype(jnp.bfloat16)

            @pl.when(i < 2)
            def _():
                part_copy(block, half, i % 2).start()

            return carry

        lax.fori_loop(0, n_tp, down, 0)

    def wide_of(ref, *at):
        return ref[at].astype(jnp.float32)

    def join_cores(block, half):
        at = span_of(half)
        wait_bytes(parts_in.at[block, :, at], part_recv.at[block, half])
        away = wide_of(parts, block, opposite, at) + wide_of(parts_in, block, 1 - y, at)
        pair_out[block, at, :] = away.astype(jnp.bfloat16)
        pair_copy(block, half).start()
        pair_keep[block, at, :] = wide_of(parts, block, tp, at) + wide_of(parts_in, block, y, at)

    def join_own_cores(k):
        zc, half = unit_at(k)
        join_cores(zc * x_size + x, half)

    def join_other_cores(k):
        zc, half = unit_at(k)
        join_cores(zc * x_size + (1 - x), half)

    def join_pair_other(k):
        zc, half = unit_at(k)
        at = span_of(half)
        block = zc * x_size + (1 - x)
        pair_copy(block, half).wait_recv()
        both = pair_keep[block, at, :] + wide_of(pair_in, block, at)
        side_out[zc, at, :] = both.astype(jnp.bfloat16)
        side_copy(zc, half).start()

    def join_pair_own(k):
        zc, half = unit_at(k)
        at = span_of(half)
        block = zc * x_size + x
        pair_copy(block, half).wait_recv()
        total[zc, at, :] = pair_keep[block, at, :] + wide_of(pair_in, block, at)

    def join_sides(k):
        zc, half = unit_at(k)
        at = span_of(half)
        side_copy(zc, half).wait_recv()
        value = total[zc, at, :] + wide_of(side_in, zc, at)
        total[zc, at, :] = value

        @pl.when(zc != z)
        def _():
            far_out[zc, at, :] = value.astype(jnp.bfloat16)
            far_copy(zc, half).start()

    units = nz * halves

    def take_first(k):
        z_next, half_next = unit_at(k)
        take(z_next, half_next, True, ZF)

    def take_ahead(k):
        z_next, half_next = unit_at(k)
        take(z_next, half_next, True, ZF)
        take(z_next, half_next, True, XF)
        take(z_next, half_next, False, XF)

    def compute_own(k):
        zc, half = unit_at(k)
        block = zc * x_size + x

        @pl.when(k >= halves)
        def _():
            sibling_arrived(block, half)

        compute(block, half)

    def compute_other(k):
        zc, half = unit_at(k)
        block = zc * x_size + (1 - x)
        sibling_arrived(block, half)
        compute(block, half)

    def take_other(k):
        zc, half = unit_at(k)
        take(zc, half, False, ZF)

    for k in range(halves):
        compute_own(k)
        if k == 0:
            take(z, 0, False, XF)
    take_other(0)
    join_own_cores(0)
    compute_other(0)
    join_own_cores(1)
    take(z, 1, False, XF)
    if units > halves:

        @pl.when(~inner)
        def _():
            take_first(2)

    join_other_cores(0)
    take_other(1)
    join_pair_own(0)
    if units > halves:

        @pl.when(inner)
        def _():
            take_ahead(2)
            take_ahead(3)

    def sides(k, carry):
        join_sides(k)
        return carry

    def unit_body(k, carry):
        zc, half = unit_at(k)

        @pl.when(~inner)
        def _():
            take(zc, half, True, XF)

        compute_other(k - 1)

        @pl.when((~inner) & (k + 1 < units))
        def _():
            take_first(k + 1)

        compute_own(k)

        @pl.when(~inner)
        def _():
            take(zc, half, False, XF)

        @pl.when(inner & (k == 2))
        def _():
            take_ahead(4)
            take_ahead(5)

        @pl.when(inner & ((k == 3) | (k >= 5)))
        def _():
            ahead = jnp.where(k == 3, 6, k + 2)

            @pl.when(ahead < units)
            def _():
                take_ahead(ahead)

        take_other(k)
        join_other_cores(k - 1)
        join_own_cores(k)
        join_pair_own(k - 1)
        join_pair_other(k - 2)

        @pl.when(((~inner) & (k >= 3)) | (inner & (k >= 7)))
        def _():
            join_sides(k - 3)

        @pl.when(inner & (k == 6))
        def _():
            lax.fori_loop(0, 4, sides, 0)

        return carry

    lax.fori_loop(halves, units, unit_body, 0)
    compute_other(units - 1)
    join_other_cores(units - 1)
    join_pair_other(units - 2)

    join_pair_own(units - 1)
    if units > 2:
        join_sides(units - 3)
    join_pair_other(units - 1)
    join_sides(units - 2)
    join_sides(units - 1)

    for side in range(2):

        @pl.when(sp < n_sp - 1 if side == 0 else sp > 0)
        def _():
            wait_bytes(pool_edges.at[:, side], edge_send.at[side])

    for i, ref in enumerate(front_all):
        wait_bytes(ref.at[others], front_send.at[i])
    wait_bytes(route_all.at[pl.ds(0, n_sp - 1)], route_send.at[0])
    ag_sent()
    wait_bytes(parts_in, part_send.at[0])
    wait_bytes(pair_out, pair_send.at[0])
    wait_bytes(side_out, side_send.at[0])

    combined = total[z]
    if nz > 1:
        wait_bytes(far_in.at[pl.ds(0, nz - 1)], far_recv.at[0])
    for d in range(1, nz):
        combined += far_in[(z + d) % nz].astype(jnp.float32)
    total[z] = combined

    own_squares = jnp.sum(combined * combined, axis=1, keepdims=True)
    squares[tp] = jnp.broadcast_to(own_squares, (rows, 128)).T[:8]

    def squares_copy(d):
        return remote(
            squares.at[tp], squares.at[tp], sq_send.at[0], sq_recv.at[0], sp, (tp + d) % n_tp
        )

    for d in range(1, n_tp):
        squares_copy(d).start()
    wait_bytes(squares.at[others], sq_recv.at[0])
    summed = squares[0]
    for i in range(1, n_tp):
        summed += squares[i]
    row_scale = lax.rsqrt(summed[:1] / width + epsilon)
    row_scale = jnp.broadcast_to(row_scale, (128, rows)).T
    for i in range(cols // 128):
        lane = slice(i * 128, (i + 1) * 128)
        own = mixed[:, pl.ds(pl.multiple_of(tp * cols + i * 128, 128), 128)].astype(jnp.float32)
        out_ref[:, lane] = (own + total[z, :, lane] * row_scale * expert_norm[:, lane]).astype(
            jnp.bfloat16
        )

    wait_bytes(squares.at[others], sq_send.at[0])
    if nz > 1:
        wait_bytes(far_out.at[pl.ds(0, nz - 1)], far_send.at[0])


def gathered_shards(*args):
    pool_in, pool_norm, out_weight, stream = args[0], args[3], args[4], args[5]
    w_gate, w_down = args[10], args[14]
    n_sp, n_tp = lax.axis_size("sp"), lax.axis_size("tp")
    nz = n_sp // x_size
    rows, width = stream.shape
    n_hidden = w_gate.shape[2]
    cols = width // n_tp
    group_width = pool_in.shape[1]
    bf16, f32 = jnp.bfloat16, jnp.float32
    row_args = (2, 3, 6, 7, 15)
    args = [a.reshape(1, -1) if i in row_args else a for i, a in enumerate(args)]
    args[8], args[9] = args[8].T, args[9].T
    in_hbm = (4, 5, 10, 11, 14)
    in_specs = [
        pl.BlockSpec(memory_space=pl.ANY if i in in_hbm else pltpu.VMEM) for i in range(len(args))
    ]
    edge = 2 * reach_rows
    route_rows = -(-n_sp // 8) * 8
    dma = pltpu.SemaphoreType.DMA
    scratch = [
        pltpu.VMEM((n_sp, rows, width), bf16),
        pltpu.VMEM((width, n_hidden), bf16),
        pltpu.VMEM((width, n_hidden), bf16),
        pltpu.VMEM((n_hidden, width), bf16),
        pltpu.VMEM(out_weight.shape, bf16),
        pltpu.VMEM((rows, width), bf16),
        pltpu.VMEM((n_tp, rows, group_width), bf16),
        pltpu.VMEM((n_tp, 2, edge, group_width), bf16),
        pltpu.VMEM((n_tp, group_width, group_width), bf16),
        pltpu.VMEM((n_tp, 1, group_width), f32),
        pltpu.VMEM((n_tp, rows + 2 * reach_rows, group_width), f32),
        pltpu.VMEM((rows, n_tp * group_width), bf16),
        pltpu.VMEM((rows, width), f32),
        pltpu.VMEM((rows, width), bf16),
        pltpu.VMEM((n_sp, route_rows, rows), f32),
        pltpu.VMEM((rows // halves, n_hidden), bf16),
        pltpu.VMEM((n_sp, n_tp, rows, cols), bf16),
        pltpu.VMEM((n_sp, n_tp // core_count, rows, cols), bf16),
        pltpu.VMEM((n_sp, rows, cols), bf16),
        pltpu.VMEM((n_sp, rows, cols), f32),
        pltpu.VMEM((n_sp, rows, cols), bf16),
        pltpu.VMEM((nz, rows, cols), bf16),
        pltpu.VMEM((nz, rows, cols), bf16),
        pltpu.VMEM((nz, rows, cols), f32),
        pltpu.VMEM((nz, rows, cols), bf16),
        pltpu.VMEM((nz, rows, cols), bf16),
        pltpu.VMEM((n_tp, 8, rows), f32),
        dma((5,)),
        dma((4, 2)),
        dma((n_sp, halves, 3)),
        dma((3,)),
        dma((3,)),
        dma((2,)),
        dma((2,)),
        dma((1,)),
        dma((1,)),
        dma((1,)),
        dma((n_sp, halves)),
        dma((1,)),
        dma((n_sp, halves)),
        dma((1,)),
        dma((nz, halves)),
        dma((1,)),
        dma((1,)),
        dma((1,)),
        dma((1,)),
    ]
    return pl.pallas_call(
        functools.partial(layer_kernel, nz),
        out_shape=jax.ShapeDtypeStruct((rows, cols), bf16),
        in_specs=in_specs,
        out_specs=pl.BlockSpec(memory_space=pltpu.VMEM),
        scratch_shapes=scratch,
        compiler_params=pltpu.CompilerParams(
            collective_id=0, has_side_effects=True, vmem_limit_bytes=vmem_limit
        ),
        name="layer",
    )(*args)


def shards(*args):
    pool_in, out_weight, stream, w_gate = args[0], args[4], args[5], args[10]
    n_sp, n_tp = lax.axis_size("sp"), lax.axis_size("tp")
    rows, width = stream.shape
    cols, n_hidden = width // n_tp, w_gate.shape[2]
    slots = n_sp * rows * (2 * width + (2 + 1 + 1 + 2 + 1) * 2 * cols + 2 * width + 2 * width)
    fixed = 2 * (3 * width * n_hidden + out_weight.size) + 10 * rows * width
    fits = slots + fixed < vmem_limit * 9 // 10
    shaped = (
        n_tp == 2 * core_count
        and n_sp % x_size == 0
        and w_gate.shape[0] == 1
        and rows % (128 * halves) == 0
        and width % (128 * first_share[0]) == 0
        and cols % 128 == 0
        and n_hidden % 256 == 0
        and pool_in.shape[1] == 128
        and n_sp <= 128
    )
    return (gathered_shards if fits and shaped else routed_shards)(*args)


def solution(mesh):
    in_specs = (
        P("sp", "tp"),
        P("tp", None, None),
        P("tp"),
        P(),
        P(),
        P("sp", None),
        P(),
        P(),
        P("sp", None),
        P("sp", None),
        P("sp", None, "tp"),
        P("sp", None, "tp"),
        P("sp", "tp"),
        P("sp", "tp"),
        P("sp", "tp", None),
        P("tp"),
    )
    out_specs = P("sp", "tp")
    return jax.shard_map(shards, mesh=mesh, in_specs=in_specs, out_specs=out_specs, check_vma=False)
```

```python
import functools

import jax
import jax.numpy as jnp
from jax import lax
from jax.experimental import pallas as pl
from jax.experimental.pallas import tpu as pltpu
from jax.sharding import PartitionSpec as P

MESH = pl.DeviceIdType.MESH

epsilon = 1e-06
reach_rows = 8
clamp_limit = 7.0
sigmoid_alpha = 1.702
chunk_counts = (2,)


def extended_2(shard, sides, width):
    for axis, dim in sides:
        count, length = (lax.axis_size(axis), shard.shape[dim])
        up = [(i, (i + 1) % count) for i in range(count - 1)]
        down = [(j, i) for i, j in up]
        last = lax.slice_in_dim(shard, length - width, length, axis=dim)
        leading = lax.slice_in_dim(shard, 0, width, axis=dim)
        before = lax.ppermute(last, axis, up)
        after = lax.ppermute(leading, axis, down)
        shard = jnp.concatenate([before, shard, after], axis=dim)
    return shard


def rms_scale(values):
    return values * lax.rsqrt(jnp.mean(values * values, axis=-1, keepdims=True) + epsilon)


def routed_shards(
    pool_in,
    pool_weight,
    pool_scale,
    pool_norm,
    out_weight,
    stream,
    mix_norm,
    ffn_norm,
    routes,
    route_weights,
    w_gate,
    w_up,
    gate_bias,
    up_bias,
    w_down,
    expert_norm,
):
    rows_dev = pool_in.shape[0]
    length = rows_dev * lax.axis_size("sp")
    radius = jnp.left_shift(1, lax.axis_index("tp"))
    positions = lax.axis_index("sp") * rows_dev + jnp.arange(rows_dev)
    padded = extended_2(pool_in, (("sp", 0),), reach_rows).astype(jnp.float32)
    window_sum = jnp.zeros((rows_dev, pool_in.shape[1]), jnp.float32)
    counts = jnp.zeros((rows_dev,), jnp.float32)
    for offset in range(-reach_rows, reach_rows + 1):
        inside = (positions + offset >= 0) & (positions + offset < length) & (abs(offset) <= radius)
        window_sum = window_sum + jnp.where(
            inside[:, None], padded[reach_rows + offset : reach_rows + offset + rows_dev], 0.0
        )
        counts = counts + inside.astype(jnp.float32)
    deviation = (window_sum / counts[:, None] - padded[reach_rows : reach_rows + rows_dev]).astype(
        jnp.bfloat16
    )
    pool_out = (
        jnp.dot(deviation, pool_weight[0], preferred_element_type=jnp.float32) * pool_scale
    ).astype(jnp.bfloat16)
    all_groups = lax.all_gather(pool_out, "tp", axis=1, tiled=True)
    normed = (rms_scale(all_groups.astype(jnp.float32)) * pool_norm).astype(jnp.bfloat16)
    mix_out = jnp.dot(normed, out_weight, preferred_element_type=jnp.float32)
    mixed = (stream.astype(jnp.float32) + rms_scale(mix_out) * mix_norm).astype(jnp.bfloat16)
    expert_in = (rms_scale(mixed.astype(jnp.float32)) * ffn_norm).astype(jnp.bfloat16)
    model_width = mixed.shape[1]
    experts = lax.axis_size("sp") * w_gate.shape[0]
    top_count = routes.shape[1]
    capacity = rows_dev * top_count * 3 // (2 * experts)
    quarter = capacity // lax.axis_size("tp")
    chunks = next((n for n in chunk_counts if quarter % (8 * n) == 0), 1)
    chunk_rows, own_rows = capacity // chunks, quarter // chunks

    names = routes.T[:, None, :] == jnp.arange(experts, dtype=jnp.int32)[None, :, None]
    member = jnp.any(names, axis=0)
    weight = jnp.sum(jnp.where(names, route_weights.T[:, None, :], 0.0), axis=0)
    order = jnp.arange(rows_dev)
    earlier = (order[:, None] < order[None, :]).astype(jnp.bfloat16)
    place = jnp.dot(
        member.astype(jnp.bfloat16), earlier, preferred_element_type=jnp.float32
    ).astype(jnp.int32)
    place = jnp.where(member, place, -1)

    def dispatched(chunk):
        first = chunk * chunk_rows + lax.axis_index("tp") * own_rows
        slots = first + jnp.arange(own_rows, dtype=jnp.int32)
        pick = (place[:, None, :] == slots[None, :, None]).astype(jnp.bfloat16)
        rows = jnp.dot(pick.reshape(experts * own_rows, rows_dev), expert_in)
        own_slots = rows.reshape(experts, own_rows, model_width)
        arrived = lax.all_to_all(own_slots, "sp", split_axis=0, concat_axis=0, tiled=True)
        return lax.all_gather(arrived, "tp", axis=1, tiled=True)

    def expert(slot_block):
        row_block = slot_block.reshape(-1, model_width)
        gate_pre = jnp.dot(row_block, w_gate[0], preferred_element_type=jnp.float32) + gate_bias[0]
        up_pre = jnp.dot(row_block, w_up[0], preferred_element_type=jnp.float32) + up_bias[0]
        gate_cut = jnp.minimum(gate_pre, clamp_limit)
        up_cut = jnp.clip(up_pre, -clamp_limit, clamp_limit)
        activation = (
            (up_cut + 1.0) * (gate_cut * jax.nn.sigmoid(sigmoid_alpha * gate_cut))
        ).astype(jnp.bfloat16)
        partial_value = jnp.dot(activation, w_down[0], preferred_element_type=jnp.float32).astype(
            jnp.bfloat16
        )
        partial_value = partial_value.reshape(slot_block.shape)
        summed = lax.psum_scatter(partial_value, "tp", scatter_dimension=2, tiled=True)
        return lax.all_to_all(summed, "sp", split_axis=0, concat_axis=0, tiled=True)

    def weighted(chunk, returned):
        slots = chunk * chunk_rows + jnp.arange(chunk_rows, dtype=jnp.int32)
        spread = jnp.where(place[:, None, :] == slots[None, :, None], weight[:, None, :], 0.0)
        spread = spread.reshape(experts * chunk_rows, rows_dev)
        high = spread.astype(jnp.bfloat16)
        low = (spread - high.astype(jnp.float32)).astype(jnp.bfloat16)
        flat = returned.reshape(experts * chunk_rows, -1)
        over_slots = (((0,), (0,)), ((), ()))
        return lax.dot_general(
            high, flat, over_slots, preferred_element_type=jnp.float32
        ) + lax.dot_general(low, flat, over_slots, preferred_element_type=jnp.float32)

    blocks = [dispatched(chunk) for chunk in range(chunks)]
    parts = [expert(block) for block in blocks]
    col_count = parts[0].shape[2]
    combined = sum(weighted(chunk, part) for chunk, part in enumerate(parts))
    squares = lax.psum(jnp.sum(combined * combined, axis=1), "tp")
    row_scale = lax.rsqrt(squares / model_width + epsilon)
    own_cols = lax.dynamic_slice_in_dim(
        mixed.astype(jnp.float32), lax.axis_index("tp") * col_count, col_count, 1
    )
    return (own_cols + combined * row_scale[:, None] * expert_norm).astype(jnp.bfloat16)


x_size = 2
core_count = 2
halves = 2
subs = 2
first_share = 16, 5
vmem_limit = 60 * 1024 * 1024
UP, DOWN, ACROSS, SIBLING = range(4)
XF, ZF = range(2)


def layer_kernel(
    nz,
    pool_in,
    pool_weight,
    pool_scale,
    pool_norm,
    out_weight_hbm,
    stream_hbm,
    mix_norm,
    ffn_norm,
    routes,
    route_weights,
    w_gate_hbm,
    w_up_hbm,
    gate_bias,
    up_bias,
    w_down_hbm,
    expert_norm,
    out_ref,
    tokens,
    w_gate,
    w_up,
    w_down,
    out_weight,
    stream,
    pool_all,
    pool_edges,
    weight_all,
    scale_all,
    padded,
    normed,
    mix_out,
    mixed,
    route_all,
    hidden,
    parts,
    parts_in,
    pair_out,
    pair_keep,
    pair_in,
    side_out,
    side_in,
    total,
    far_out,
    far_in,
    squares,
    load_sem,
    ag_send,
    ag_recv,
    front_send,
    front_recv,
    edge_send,
    edge_recv,
    route_send,
    route_recv,
    part_send,
    part_recv,
    pair_send,
    pair_recv,
    side_send,
    side_recv,
    far_send,
    far_recv,
    sq_send,
    sq_recv,
):
    sp, tp = lax.axis_index("sp"), lax.axis_index("tp")
    n_sp = nz * x_size
    n_tp = pool_all.shape[0]
    z, x = sp // x_size, sp % x_size
    y, core = tp // core_count, tp % core_count
    rows, width = stream.shape
    cols = out_ref.shape[1]
    group_width = pool_in.shape[1]
    half_rows = rows // halves
    core_rows = half_rows // core_count
    first_cols = width * first_share[1] // first_share[0]
    sibling = y * core_count + (1 - core)
    opposite = (1 - y) * core_count + core
    far_z = nz - 1

    def remote(src, dst, send, recv, to_sp, to_tp):
        return pltpu.make_async_remote_copy(
            src_ref=src,
            dst_ref=dst,
            send_sem=send,
            recv_sem=recv,
            device_id=(to_sp, to_tp),
            device_id_type=MESH,
        )

    def wait_bytes(ref, sem):
        pltpu.make_async_copy(ref, ref, sem).wait()

    loads = [
        pltpu.make_async_copy(src, dst, load_sem.at[i])
        for i, (src, dst) in enumerate(
            (
                (out_weight_hbm, out_weight),
                (stream_hbm, stream),
                (w_gate_hbm.at[0], w_gate),
                (w_up_hbm.at[0], w_up),
                (w_down_hbm.at[0], w_down),
            )
        )
    ]
    for load in loads:
        load.start()

    barrier = pltpu.get_barrier_semaphore()

    def greet(to_sp, to_tp):
        pl.semaphore_signal(barrier, inc=1, device_id=(to_sp, to_tp), device_id_type=MESH)

    for d in range(1, n_sp):
        greet((sp + d) % n_sp, tp)
    for d in range(1, n_tp):
        greet(sp, (tp + d) % n_tp)

    @pl.when(sp > 0)
    def _():
        for d in range(1, n_tp):
            greet(sp - 1, (tp + d) % n_tp)

    @pl.when(sp < n_sp - 1)
    def _():
        for d in range(1, n_tp):
            greet(sp + 1, (tp + d) % n_tp)

    near = (sp > 0).astype(jnp.int32) + (sp < n_sp - 1).astype(jnp.int32)
    pl.semaphore_wait(barrier, (n_sp - 1) + (n_tp - 1) * (1 + near))

    edge = pool_edges.shape[2]

    def edge_copy(side, to_tp):
        src = pool_in.at[pl.ds(rows - edge, edge)] if side == 0 else pool_in.at[pl.ds(0, edge)]
        return remote(
            src,
            pool_edges.at[tp, side],
            edge_send.at[side],
            edge_recv.at[side],
            sp + 1 if side == 0 else sp - 1,
            to_tp,
        )

    for side in range(2):

        @pl.when(sp < n_sp - 1 if side == 0 else sp > 0)
        def _():
            for d in range(n_tp):
                edge_copy(side, (tp + d) % n_tp).start()

    def front_copies(d):
        to = (tp + d) % n_tp
        return [
            remote(pool_in, pool_all.at[tp], front_send.at[0], front_recv.at[0], sp, to),
            remote(pool_weight.at[0], weight_all.at[tp], front_send.at[1], front_recv.at[1], sp, to),
            remote(pool_scale, scale_all.at[tp], front_send.at[2], front_recv.at[2], sp, to),
        ]

    for d in range(1, n_tp):
        for copy in front_copies(d):
            copy.start()
    pool_all[tp] = pool_in[...]
    weight_all[tp] = pool_weight[0]
    scale_all[tp] = pool_scale[...]

    route_rows = route_all.shape[1]
    names = lax.broadcasted_iota(jnp.int32, (route_rows, rows), 0)
    by_expert = jnp.zeros((route_rows, rows), jnp.float32)
    for k in range(routes.shape[0]):
        by_expert += jnp.where(routes[k : k + 1, :] == names, route_weights[k : k + 1, :], 0.0)
    route_all[sp] = by_expert

    def route_copy(d):
        to = (sp + d) % n_sp
        return remote(
            route_all.at[sp], route_all.at[sp], route_send.at[0], route_recv.at[0], to, tp
        )

    for d in range(1, n_sp):
        route_copy(d).start()

    others = pl.ds(0, n_tp - 1)
    front_all = (pool_all, weight_all, scale_all)
    for i, ref in enumerate(front_all):
        wait_bytes(ref.at[others], front_recv.at[i])

    @pl.when(sp > 0)
    def _():
        wait_bytes(pool_edges.at[:, 0], edge_recv.at[0])
        for g in range(n_tp):
            padded[g, 0:reach_rows, :] = pool_edges[g, 0].astype(jnp.float32)[edge - reach_rows :]

    @pl.when(sp == 0)
    def _():
        padded[:, 0:reach_rows, :] = jnp.zeros((n_tp, reach_rows, group_width), jnp.float32)

    @pl.when(sp < n_sp - 1)
    def _():
        wait_bytes(pool_edges.at[:, 1], edge_recv.at[1])
        for g in range(n_tp):
            padded[g, reach_rows + rows :, :] = pool_edges[g, 1].astype(jnp.float32)[:reach_rows]

    @pl.when(sp == n_sp - 1)
    def _():
        padded[:, reach_rows + rows :, :] = jnp.zeros((n_tp, reach_rows, group_width), jnp.float32)

    positions = sp * rows + lax.broadcasted_iota(jnp.int32, (rows, group_width), 0)
    mean_square = jnp.zeros((rows, 1), jnp.float32)
    for g in range(n_tp):
        radius = 1 << g
        values = pool_all[g].astype(jnp.float32)
        padded[g, reach_rows : reach_rows + rows, :] = values
        window_sum = values
        for offset in range(1, radius + 1):
            window_sum += padded[g, reach_rows + offset : reach_rows + offset + rows, :]
            window_sum += padded[g, reach_rows - offset : reach_rows - offset + rows, :]
        last = jnp.minimum(positions + radius, n_sp * rows - 1)
        counts = last - jnp.maximum(positions - radius, 0) + 1
        deviation = (window_sum / counts.astype(jnp.float32) - values).astype(jnp.bfloat16)
        pool_out = (
            jnp.dot(deviation, weight_all[g], preferred_element_type=jnp.float32) * scale_all[g]
        ).astype(jnp.bfloat16)
        normed[:, g * group_width : (g + 1) * group_width] = pool_out
        wide = pool_out.astype(jnp.float32)
        mean_square += jnp.sum(wide * wide, axis=1, keepdims=True)
    pool_width = n_tp * group_width
    row_scale = lax.rsqrt(mean_square / pool_width + epsilon)
    normed[...] = (normed[...].astype(jnp.float32) * row_scale * pool_norm[...]).astype(jnp.bfloat16)

    for load in loads[:2]:
        load.wait()
    for t in range(width // cols):
        mix_out[:, t * cols : (t + 1) * cols] = jnp.dot(
            normed[...], out_weight[:, t * cols : (t + 1) * cols], preferred_element_type=jnp.float32
        )

    tile = 32

    def mix_rows(first, count):
        def body(i, carry):
            part = pl.ds(pl.multiple_of(first + i * tile, tile), tile)
            value = mix_out[part, :]
            scaled = value * lax.rsqrt(jnp.mean(value * value, axis=1, keepdims=True) + epsilon)
            summed = stream[part, :].astype(jnp.float32) + scaled * mix_norm[...]
            summed = summed.astype(jnp.bfloat16)
            mixed[part, :] = summed
            wide = summed.astype(jnp.float32)
            wide = wide * lax.rsqrt(jnp.mean(wide * wide, axis=1, keepdims=True) + epsilon)
            tokens[sp, part, :] = (wide * ffn_norm[...]).astype(jnp.bfloat16)
            return carry

        lax.fori_loop(0, count // tile, body, 0)

    def piece(block, half, kind, whose):
        first = pl.multiple_of(half * half_rows + whose * core_rows, 16)
        span = pl.ds(0, first_cols) if kind == XF else pl.ds(first_cols, width - first_cols)
        return tokens.at[block, pl.ds(first, core_rows), span]

    def ag_copy(block, half, kind, way, lane_of=0):
        to_sp = {UP: sp + x_size, DOWN: sp - x_size, ACROSS: z * x_size + (1 - x), SIBLING: sp}[way]
        recv = ag_recv.at[block, half, 2 if way == SIBLING else kind]
        ref = piece(block, half, kind, core)
        to_tp = sibling if way == SIBLING else tp
        return remote(ref, ref, ag_send.at[way, lane_of], recv, to_sp, to_tp)

    def ag_arrived(block, half, kind):
        wait_bytes(piece(block, half, kind, core), ag_recv.at[block, half, kind])

    def sibling_arrived(block, half):
        first = pl.multiple_of(half * half_rows + (1 - core) * core_rows, 16)
        wait_bytes(tokens.at[block, pl.ds(first, core_rows), :], ag_recv.at[block, half, 2])

    def ag_start(zc, half, col_is_own, kind):
        block = zc * x_size + (x if col_is_own else 1 - x)

        if col_is_own and kind == XF:

            @pl.when(zc == z)
            def _():
                ag_copy(block, half, kind, ACROSS).start()

        lane_of = 0 if col_is_own else 1
        if col_is_own or kind == XF:

            @pl.when((zc <= z) & (z < far_z))
            def _():
                ag_copy(block, half, kind, UP, lane_of).start()

            @pl.when((zc >= z) & (z > 0))
            def _():
                ag_copy(block, half, kind, DOWN, lane_of).start()

        if col_is_own and kind == ZF:

            @pl.when(zc == z)
            def _():
                ag_copy(block, half, kind, ACROSS).start()

            @pl.when((zc != z) & ~from_end(zc))
            def _():
                ag_copy(block, half, kind, ACROSS, 1).start()

        if col_is_own:

            @pl.when(zc != z)
            def _():
                ag_copy(block, half, kind, SIBLING).start()

        else:
            ag_copy(block, half, kind, SIBLING).start()

        if not col_is_own and kind == ZF and nz > 2:

            @pl.when((zc == z) & (z == 0))
            def _():
                ag_copy(block, half, kind, UP, 2).start()

            @pl.when((zc == z) & (z == far_z))
            def _():
                ag_copy(block, half, kind, DOWN, 2).start()

    def from_end(zc):
        at_end = ((zc == 0) & (z == 1)) | ((zc == far_z) & (z == far_z - 1))
        return at_end & (z > 0) & (z < far_z)

    def ag_sent():
        carried = pl.ds(0, halves * core_rows)
        xf, zf = pl.ds(0, first_cols), pl.ds(first_cols, width - first_cols)
        wait_bytes(tokens.at[pl.ds(0, n_sp - 1), carried, :], ag_send.at[SIBLING, 0])
        wait_bytes(tokens.at[0, carried, :], ag_send.at[ACROSS, 0])
        for at_z in range(nz):

            @pl.when(z == at_z)
            def _():
                across = nz - 1
                if 0 < at_z < far_z:
                    across -= (at_z == 1) + (at_z == far_z - 1)
                if across > 0:
                    wait_bytes(tokens.at[pl.ds(0, across), carried, zf], ag_send.at[ACROSS, 1])
                if nz > 2 and at_z == 0:
                    wait_bytes(tokens.at[0, carried, zf], ag_send.at[UP, 2])
                if nz > 2 and at_z == far_z:
                    wait_bytes(tokens.at[0, carried, zf], ag_send.at[DOWN, 2])
                if at_z < far_z:
                    wait_bytes(tokens.at[pl.ds(0, at_z + 1), carried, :], ag_send.at[UP, 0])
                    wait_bytes(tokens.at[pl.ds(0, at_z + 1), carried, xf], ag_send.at[UP, 1])
                if at_z > 0:
                    wait_bytes(tokens.at[pl.ds(0, nz - at_z), carried, :], ag_send.at[DOWN, 0])
                    wait_bytes(tokens.at[pl.ds(0, nz - at_z), carried, xf], ag_send.at[DOWN, 1])

    def take(zc, half, col_is_own, kind):
        block = zc * x_size + (x if col_is_own else 1 - x)
        ag_arrived(block, half, kind)
        ag_start(zc, half, col_is_own, kind)

    for whose in range(core_count):
        for half in range(halves):
            mix_rows(half * half_rows + (core if whose == 0 else 1 - core) * core_rows, core_rows)
            if whose == 0:
                ag_start(z, half, True, XF)
                ag_start(z, half, True, ZF)

    wait_bytes(route_all.at[pl.ds(0, n_sp - 1)], route_recv.at[0])
    for load in loads[2:]:
        load.wait()

    upper = z >= (nz + 1) // 2
    low_z = jnp.where(upper, far_z - z, z)

    def plane_at(step):
        plane = jnp.where(step <= low_z, low_z - step, step)
        return jnp.where(upper, far_z - plane, plane)

    inner = low_z > 0

    inner_order = {2: (1, 0), 3: (2, 0), 4: (1, 1), 5: (2, 1)}
    if nz > 3:
        inner_order.update({5: (3, 0), 6: (3, 1), 7: (2, 1)})

    def unit_at(k):
        step, half = k // halves, k % halves
        for at, (inner_step, inner_half) in inner_order.items():
            step = jnp.where(inner & (k == at), inner_step, step)
            half = jnp.where(inner & (k == at), inner_half, half)
        return plane_at(step), half

    n_hidden = hidden.shape[1]
    hidden_tile = min(256, n_hidden)

    def span_of(half):
        return pl.ds(pl.multiple_of(half * half_rows, half_rows), half_rows)

    def part_copy(block, half, q_y):
        q = q_y * core_count + (1 - core)
        return remote(
            parts.at[block, q, span_of(half)],
            parts_in.at[block, q_y, span_of(half)],
            part_send.at[0],
            part_recv.at[block, half],
            sp,
            sibling,
        )

    sub_rows = half_rows // subs

    def sub_of(half, sub):
        return pl.ds(pl.multiple_of(half * half_rows + sub * sub_rows, sub_rows), sub_rows)

    def pair_copy(block, half, sub):
        at = sub_of(half, sub)
        return remote(
            pair_out.at[block, at],
            pair_in.at[block, at],
            pair_send.at[0],
            pair_recv.at[block, half, sub],
            sp,
            opposite,
        )

    def side_copy(zc, half, sub):
        at = sub_of(half, sub)
        return remote(
            side_out.at[zc, at],
            side_in.at[zc, at],
            side_send.at[0],
            side_recv.at[zc, half, sub],
            z * x_size + (1 - x),
            tp,
        )

    def far_copy(zc, half, sub):
        at = sub_of(half, sub)
        return remote(
            far_out.at[zc, at],
            far_in.at[z, at],
            far_send.at[0],
            far_recv.at[0],
            zc * x_size + x,
            tp,
        )

    def compute(block, half):
        own_row = lax.broadcasted_iota(jnp.int32, (route_rows, half_rows), 0) == sp
        weight = jnp.sum(
            jnp.where(own_row, route_all[block, :, span_of(half)], 0.0), axis=0, keepdims=True
        )
        weight = jnp.broadcast_to(weight, (128, half_rows)).T
        for j in range(n_hidden // hidden_tile):
            span = slice(j * hidden_tile, (j + 1) * hidden_tile)
            data = tokens[block, span_of(half), :]
            gate = jnp.dot(data, w_gate[:, span], preferred_element_type=jnp.float32)
            up = jnp.dot(data, w_up[:, span], preferred_element_type=jnp.float32)
            gate_cut = jnp.minimum(gate + gate_bias[:, span], clamp_limit)
            up_cut = jnp.clip(up + up_bias[:, span], -clamp_limit, clamp_limit)
            active = (up_cut + 1.0) * (gate_cut * jax.nn.sigmoid(sigmoid_alpha * gate_cut))
            for i in range(hidden_tile // 128):
                lane = slice(i * 128, (i + 1) * 128)
                at = j * hidden_tile + i * 128
                hidden[:, at : at + 128] = (active[:, lane] * weight).astype(jnp.bfloat16)

        def down(i, carry):
            whose = jnp.where(i < 2, 1 - core, core)
            q = (i % 2) * core_count + whose
            at = pl.ds(pl.multiple_of(q * cols, cols), cols)
            parts[block, q, span_of(half), :] = jnp.dot(
                hidden[...], w_down[:, at], preferred_element_type=jnp.float32
            ).astype(jnp.bfloat16)

            @pl.when(i < 2)
            def _():
                part_copy(block, half, i % 2).start()

            return carry

        lax.fori_loop(0, n_tp, down, 0)

    def wide_of(ref, *at):
        return ref[at].astype(jnp.float32)

    def join_cores(block, half):
        wait_bytes(parts_in.at[block, :, span_of(half)], part_recv.at[block, half])
        for sub in range(subs):
            at = sub_of(half, sub)
            away = wide_of(parts, block, opposite, at) + wide_of(parts_in, block, 1 - y, at)
            pair_out[block, at, :] = away.astype(jnp.bfloat16)
            pair_copy(block, half, sub).start()
        at = span_of(half)
        pair_keep[block, at, :] = wide_of(parts, block, tp, at) + wide_of(parts_in, block, y, at)

    def join_own_cores(k):
        zc, half = unit_at(k)
        join_cores(zc * x_size + x, half)

    def join_other_cores(k):
        zc, half = unit_at(k)
        join_cores(zc * x_size + (1 - x), half)

    def join_pair_other(k):
        zc, half = unit_at(k)
        block = zc * x_size + (1 - x)
        for sub in range(subs):
            at = sub_of(half, sub)
            pair_copy(block, half, sub).wait_recv()
            both = pair_keep[block, at, :] + wide_of(pair_in, block, at)
            side_out[zc, at, :] = both.astype(jnp.bfloat16)
            side_copy(zc, half, sub).start()

    def join_pair_own(k):
        zc, half = unit_at(k)
        block = zc * x_size + x
        for sub in range(subs):
            pair_copy(block, half, sub).wait_recv()
        at = span_of(half)
        total[zc, at, :] = pair_keep[block, at, :] + wide_of(pair_in, block, at)

    def join_sides(k):
        zc, half = unit_at(k)
        for sub in range(subs):
            at = sub_of(half, sub)
            side_copy(zc, half, sub).wait_recv()
            value = total[zc, at, :] + wide_of(side_in, zc, at)

            @pl.when(zc != z)
            def _():
                far_out[zc, at, :] = value.astype(jnp.bfloat16)
                far_copy(zc, half, sub).start()

            @pl.when(zc == z)
            def _():
                total[zc, at, :] = value

    units = nz * halves

    def take_first(k):
        z_next, half_next = unit_at(k)
        take(z_next, half_next, True, ZF)

    def take_rest(k):
        z_next, half_next = unit_at(k)
        take(z_next, half_next, True, XF)
        take(z_next, half_next, False, XF)

    def take_ahead(k):
        take_first(k)
        take_rest(k)

    def compute_own(k):
        zc, half = unit_at(k)
        block = zc * x_size + x

        @pl.when(k >= halves)
        def _():
            sibling_arrived(block, half)

        compute(block, half)

    def compute_other(k):
        zc, half = unit_at(k)
        block = zc * x_size + (1 - x)
        sibling_arrived(block, half)
        compute(block, half)

    def take_other(k):
        zc, half = unit_at(k)
        take(zc, half, False, ZF)

    compute_own(0)
    take(z, 0, False, XF)
    compute_own(1)
    join_own_cores(0)
    take_other(0)
    join_own_cores(1)
    compute_other(0)
    take(z, 1, False, XF)
    if units > halves:

        take_first(2)

        @pl.when(inner)
        def _():
            take_first(3)

    join_other_cores(0)
    take_other(1)
    join_pair_own(0)

    def sides(k, carry):
        join_sides(k)
        return carry

    def unit_body(k, carry):
        zc, half = unit_at(k)

        @pl.when(~inner)
        def _():
            take(zc, half, True, XF)

        compute_other(k - 1)

        @pl.when((~inner) & (k <= 3) & (k + 1 < units))
        def _():
            take_first(k + 1)

        @pl.when(inner & (k == 2))
        def _():
            take_rest(2)
            take_rest(3)

        compute_own(k)
        join_other_cores(k - 1)

        @pl.when(~inner)
        def _():
            take(zc, half, False, XF)

        for at, ahead in ((2, (4, 7)), (3, (5,)), (4, (6,))) if nz > 3 else ((2, (4, 5)),):

            @pl.when(inner & (k == at))
            def _():
                for unit in ahead:
                    take_ahead(unit)

        if units > 8:

            @pl.when(inner & (k >= 6) & (k + 2 < units))
            def _():
                take_ahead(k + 2)

        take_other(k)
        join_own_cores(k)

        @pl.when((~inner) & (k > 3) & (k + 1 < units))
        def _():
            take_first(k + 1)

        join_pair_other(k - 2)

        @pl.when(k < units - 1)
        def _():
            join_pair_own(k - 1)

        @pl.when((~inner) & (k >= 3))
        def _():
            join_sides(k - 3)

        @pl.when(inner & (k >= 6))
        def _():
            join_sides(k - 4)

        @pl.when(inner & (k >= 6) & (k == units - 1))
        def _():
            join_sides(k - 3)

        return carry

    lax.fori_loop(halves, units, unit_body, 0)
    compute_other(units - 1)
    join_other_cores(units - 1)
    if units > halves:
        join_pair_own(units - 2)
    join_pair_other(units - 2)

    @pl.when(inner)
    def _():
        lax.fori_loop(0, halves, sides, 0)
        if units <= 6:
            lax.fori_loop(max(units - 4, halves), units - 3, sides, 0)

    if units > halves:
        join_sides(units - 3)
    join_pair_own(units - 1)
    join_pair_other(units - 1)
    join_sides(units - 2)
    join_sides(units - 1)

    for side in range(2):

        @pl.when(sp < n_sp - 1 if side == 0 else sp > 0)
        def _():
            wait_bytes(pool_edges.at[:, side], edge_send.at[side])

    for i, ref in enumerate(front_all):
        wait_bytes(ref.at[others], front_send.at[i])
    wait_bytes(route_all.at[pl.ds(0, n_sp - 1)], route_send.at[0])
    ag_sent()
    wait_bytes(parts_in, part_send.at[0])
    wait_bytes(pair_out, pair_send.at[0])
    wait_bytes(side_out, side_send.at[0])

    combined = total[z]
    if nz > 1:
        wait_bytes(far_in.at[pl.ds(0, nz - 1)], far_recv.at[0])
    for d in range(1, nz):
        combined += far_in[(z + d) % nz].astype(jnp.float32)
    total[z] = combined

    own_squares = jnp.sum(combined * combined, axis=1, keepdims=True)
    squares[tp] = jnp.broadcast_to(own_squares, (rows, 128)).T[:8]

    def squares_copy(d):
        return remote(
            squares.at[tp], squares.at[tp], sq_send.at[0], sq_recv.at[0], sp, (tp + d) % n_tp
        )

    for d in range(1, n_tp):
        squares_copy(d).start()
    wait_bytes(squares.at[others], sq_recv.at[0])
    summed = squares[0]
    for i in range(1, n_tp):
        summed += squares[i]
    row_scale = lax.rsqrt(summed[:1] / width + epsilon)
    row_scale = jnp.broadcast_to(row_scale, (128, rows)).T
    for i in range(cols // 128):
        lane = slice(i * 128, (i + 1) * 128)
        own = mixed[:, pl.ds(pl.multiple_of(tp * cols + i * 128, 128), 128)].astype(jnp.float32)
        out_ref[:, lane] = (own + total[z, :, lane] * row_scale * expert_norm[:, lane]).astype(
            jnp.bfloat16
        )

    wait_bytes(squares.at[others], sq_send.at[0])
    if nz > 1:
        wait_bytes(far_out.at[pl.ds(0, nz - 1)], far_send.at[0])


def gathered_shards(*args):
    pool_in, pool_norm, out_weight, stream = args[0], args[3], args[4], args[5]
    w_gate, w_down = args[10], args[14]
    n_sp, n_tp = lax.axis_size("sp"), lax.axis_size("tp")
    nz = n_sp // x_size
    rows, width = stream.shape
    n_hidden = w_gate.shape[2]
    cols = width // n_tp
    group_width = pool_in.shape[1]
    bf16, f32 = jnp.bfloat16, jnp.float32
    row_args = (2, 3, 6, 7, 15)
    args = [a.reshape(1, -1) if i in row_args else a for i, a in enumerate(args)]
    args[8], args[9] = args[8].T, args[9].T
    in_hbm = (4, 5, 10, 11, 14)
    in_specs = [
        pl.BlockSpec(memory_space=pl.ANY if i in in_hbm else pltpu.VMEM) for i in range(len(args))
    ]
    edge = 2 * reach_rows
    route_rows = -(-n_sp // 8) * 8
    dma = pltpu.SemaphoreType.DMA
    scratch = [
        pltpu.VMEM((n_sp, rows, width), bf16),
        pltpu.VMEM((width, n_hidden), bf16),
        pltpu.VMEM((width, n_hidden), bf16),
        pltpu.VMEM((n_hidden, width), bf16),
        pltpu.VMEM(out_weight.shape, bf16),
        pltpu.VMEM((rows, width), bf16),
        pltpu.VMEM((n_tp, rows, group_width), bf16),
        pltpu.VMEM((n_tp, 2, edge, group_width), bf16),
        pltpu.VMEM((n_tp, group_width, group_width), bf16),
        pltpu.VMEM((n_tp, 1, group_width), f32),
        pltpu.VMEM((n_tp, rows + 2 * reach_rows, group_width), f32),
        pltpu.VMEM((rows, n_tp * group_width), bf16),
        pltpu.VMEM((rows, width), f32),
        pltpu.VMEM((rows, width), bf16),
        pltpu.VMEM((n_sp, route_rows, rows), f32),
        pltpu.VMEM((rows // halves, n_hidden), bf16),
        pltpu.VMEM((n_sp, n_tp, rows, cols), bf16),
        pltpu.VMEM((n_sp, n_tp // core_count, rows, cols), bf16),
        pltpu.VMEM((n_sp, rows, cols), bf16),
        pltpu.VMEM((n_sp, rows, cols), f32),
        pltpu.VMEM((n_sp, rows, cols), bf16),
        pltpu.VMEM((nz, rows, cols), bf16),
        pltpu.VMEM((nz, rows, cols), bf16),
        pltpu.VMEM((nz, rows, cols), f32),
        pltpu.VMEM((nz, rows, cols), bf16),
        pltpu.VMEM((nz, rows, cols), bf16),
        pltpu.VMEM((n_tp, 8, rows), f32),
        dma((5,)),
        dma((4, 3)),
        dma((n_sp, halves, 3)),
        dma((3,)),
        dma((3,)),
        dma((2,)),
        dma((2,)),
        dma((1,)),
        dma((1,)),
        dma((1,)),
        dma((n_sp, halves)),
        dma((1,)),
        dma((n_sp, halves, subs)),
        dma((1,)),
        dma((nz, halves, subs)),
        dma((1,)),
        dma((1,)),
        dma((1,)),
        dma((1,)),
    ]
    return pl.pallas_call(
        functools.partial(layer_kernel, nz),
        out_shape=jax.ShapeDtypeStruct((rows, cols), bf16),
        in_specs=in_specs,
        out_specs=pl.BlockSpec(memory_space=pltpu.VMEM),
        scratch_shapes=scratch,
        compiler_params=pltpu.CompilerParams(
            collective_id=0, has_side_effects=True, vmem_limit_bytes=vmem_limit
        ),
        name="layer",
    )(*args)


def shards(*args):
    pool_in, out_weight, stream, w_gate = args[0], args[4], args[5], args[10]
    n_sp, n_tp = lax.axis_size("sp"), lax.axis_size("tp")
    rows, width = stream.shape
    cols, n_hidden = width // n_tp, w_gate.shape[2]
    slots = n_sp * rows * (2 * width + (2 + 1 + 1 + 2 + 1) * 2 * cols + 2 * width + 2 * width)
    fixed = 2 * (3 * width * n_hidden + out_weight.size) + 10 * rows * width
    fits = slots + fixed < vmem_limit * 9 // 10
    shaped = (
        n_tp == 2 * core_count
        and n_sp % x_size == 0
        and w_gate.shape[0] == 1
        and rows % (128 * halves) == 0
        and width % (128 * first_share[0]) == 0
        and cols % 128 == 0
        and n_hidden % 256 == 0
        and pool_in.shape[1] == 128
        and n_sp <= 128
    )
    return (gathered_shards if fits and shaped else routed_shards)(*args)


def solution(mesh):
    in_specs = (
        P("sp", "tp"),
        P("tp", None, None),
        P("tp"),
        P(),
        P(),
        P("sp", None),
        P(),
        P(),
        P("sp", None),
        P("sp", None),
        P("sp", None, "tp"),
        P("sp", None, "tp"),
        P("sp", "tp"),
        P("sp", "tp"),
        P("sp", "tp", None),
        P("tp"),
    )
    out_specs = P("sp", "tp")
    return jax.shard_map(shards, mesh=mesh, in_specs=in_specs, out_specs=out_specs, check_vma=False)
```

```python
import functools

import jax
import jax.numpy as jnp
from jax import lax
from jax.experimental import pallas as pl
from jax.experimental.pallas import tpu as pltpu
from jax.sharding import PartitionSpec as P

MESH = pl.DeviceIdType.MESH

epsilon = 1e-06
reach_rows = 8
clamp_limit = 7.0
sigmoid_alpha = 1.702
chunk_counts = (2,)


def extended_2(shard, sides, width):
    for axis, dim in sides:
        count, length = (lax.axis_size(axis), shard.shape[dim])
        up = [(i, (i + 1) % count) for i in range(count - 1)]
        down = [(j, i) for i, j in up]
        last = lax.slice_in_dim(shard, length - width, length, axis=dim)
        leading = lax.slice_in_dim(shard, 0, width, axis=dim)
        before = lax.ppermute(last, axis, up)
        after = lax.ppermute(leading, axis, down)
        shard = jnp.concatenate([before, shard, after], axis=dim)
    return shard


def rms_scale(values):
    return values * lax.rsqrt(jnp.mean(values * values, axis=-1, keepdims=True) + epsilon)


def routed_shards(
    pool_in,
    pool_weight,
    pool_scale,
    pool_norm,
    out_weight,
    stream,
    mix_norm,
    ffn_norm,
    routes,
    route_weights,
    w_gate,
    w_up,
    gate_bias,
    up_bias,
    w_down,
    expert_norm,
):
    rows_dev = pool_in.shape[0]
    length = rows_dev * lax.axis_size("sp")
    radius = jnp.left_shift(1, lax.axis_index("tp"))
    positions = lax.axis_index("sp") * rows_dev + jnp.arange(rows_dev)
    padded = extended_2(pool_in, (("sp", 0),), reach_rows).astype(jnp.float32)
    window_sum = jnp.zeros((rows_dev, pool_in.shape[1]), jnp.float32)
    counts = jnp.zeros((rows_dev,), jnp.float32)
    for offset in range(-reach_rows, reach_rows + 1):
        inside = (positions + offset >= 0) & (positions + offset < length) & (abs(offset) <= radius)
        window_sum = window_sum + jnp.where(
            inside[:, None], padded[reach_rows + offset : reach_rows + offset + rows_dev], 0.0
        )
        counts = counts + inside.astype(jnp.float32)
    deviation = (window_sum / counts[:, None] - padded[reach_rows : reach_rows + rows_dev]).astype(
        jnp.bfloat16
    )
    pool_out = (
        jnp.dot(deviation, pool_weight[0], preferred_element_type=jnp.float32) * pool_scale
    ).astype(jnp.bfloat16)
    all_groups = lax.all_gather(pool_out, "tp", axis=1, tiled=True)
    normed = (rms_scale(all_groups.astype(jnp.float32)) * pool_norm).astype(jnp.bfloat16)
    mix_out = jnp.dot(normed, out_weight, preferred_element_type=jnp.float32)
    mixed = (stream.astype(jnp.float32) + rms_scale(mix_out) * mix_norm).astype(jnp.bfloat16)
    expert_in = (rms_scale(mixed.astype(jnp.float32)) * ffn_norm).astype(jnp.bfloat16)
    model_width = mixed.shape[1]
    experts = lax.axis_size("sp") * w_gate.shape[0]
    top_count = routes.shape[1]
    capacity = rows_dev * top_count * 3 // (2 * experts)
    quarter = capacity // lax.axis_size("tp")
    chunks = next((n for n in chunk_counts if quarter % (8 * n) == 0), 1)
    chunk_rows, own_rows = capacity // chunks, quarter // chunks

    names = routes.T[:, None, :] == jnp.arange(experts, dtype=jnp.int32)[None, :, None]
    member = jnp.any(names, axis=0)
    weight = jnp.sum(jnp.where(names, route_weights.T[:, None, :], 0.0), axis=0)
    order = jnp.arange(rows_dev)
    earlier = (order[:, None] < order[None, :]).astype(jnp.bfloat16)
    place = jnp.dot(
        member.astype(jnp.bfloat16), earlier, preferred_element_type=jnp.float32
    ).astype(jnp.int32)
    place = jnp.where(member, place, -1)

    def dispatched(chunk):
        first = chunk * chunk_rows + lax.axis_index("tp") * own_rows
        slots = first + jnp.arange(own_rows, dtype=jnp.int32)
        pick = (place[:, None, :] == slots[None, :, None]).astype(jnp.bfloat16)
        rows = jnp.dot(pick.reshape(experts * own_rows, rows_dev), expert_in)
        own_slots = rows.reshape(experts, own_rows, model_width)
        arrived = lax.all_to_all(own_slots, "sp", split_axis=0, concat_axis=0, tiled=True)
        return lax.all_gather(arrived, "tp", axis=1, tiled=True)

    def expert(slot_block):
        row_block = slot_block.reshape(-1, model_width)
        gate_pre = jnp.dot(row_block, w_gate[0], preferred_element_type=jnp.float32) + gate_bias[0]
        up_pre = jnp.dot(row_block, w_up[0], preferred_element_type=jnp.float32) + up_bias[0]
        gate_cut = jnp.minimum(gate_pre, clamp_limit)
        up_cut = jnp.clip(up_pre, -clamp_limit, clamp_limit)
        activation = (
            (up_cut + 1.0) * (gate_cut * jax.nn.sigmoid(sigmoid_alpha * gate_cut))
        ).astype(jnp.bfloat16)
        partial_value = jnp.dot(activation, w_down[0], preferred_element_type=jnp.float32).astype(
            jnp.bfloat16
        )
        partial_value = partial_value.reshape(slot_block.shape)
        summed = lax.psum_scatter(partial_value, "tp", scatter_dimension=2, tiled=True)
        return lax.all_to_all(summed, "sp", split_axis=0, concat_axis=0, tiled=True)

    def weighted(chunk, returned):
        slots = chunk * chunk_rows + jnp.arange(chunk_rows, dtype=jnp.int32)
        spread = jnp.where(place[:, None, :] == slots[None, :, None], weight[:, None, :], 0.0)
        spread = spread.reshape(experts * chunk_rows, rows_dev)
        high = spread.astype(jnp.bfloat16)
        low = (spread - high.astype(jnp.float32)).astype(jnp.bfloat16)
        flat = returned.reshape(experts * chunk_rows, -1)
        over_slots = (((0,), (0,)), ((), ()))
        return lax.dot_general(
            high, flat, over_slots, preferred_element_type=jnp.float32
        ) + lax.dot_general(low, flat, over_slots, preferred_element_type=jnp.float32)

    blocks = [dispatched(chunk) for chunk in range(chunks)]
    parts = [expert(block) for block in blocks]
    col_count = parts[0].shape[2]
    combined = sum(weighted(chunk, part) for chunk, part in enumerate(parts))
    squares = lax.psum(jnp.sum(combined * combined, axis=1), "tp")
    row_scale = lax.rsqrt(squares / model_width + epsilon)
    own_cols = lax.dynamic_slice_in_dim(
        mixed.astype(jnp.float32), lax.axis_index("tp") * col_count, col_count, 1
    )
    return (own_cols + combined * row_scale[:, None] * expert_norm).astype(jnp.bfloat16)


x_size = 2
core_count = 2
halves = 2
subs = 2
first_share = 16, 5
vmem_limit = 60 * 1024 * 1024
UP, DOWN, ACROSS, SIBLING = range(4)
XF, ZF = range(2)


def layer_kernel(
    nz,
    pool_in,
    pool_weight,
    pool_scale,
    pool_norm,
    out_weight_hbm,
    stream_hbm,
    mix_norm,
    ffn_norm,
    routes,
    route_weights,
    w_gate_hbm,
    w_up_hbm,
    gate_bias,
    up_bias,
    w_down_hbm,
    expert_norm,
    out_ref,
    tokens,
    w_gate,
    w_up,
    w_down,
    out_weight,
    stream,
    pool_all,
    pool_edges,
    weight_all,
    scale_all,
    padded,
    normed,
    mix_out,
    mixed,
    route_all,
    hidden,
    parts,
    parts_in,
    pair_out,
    pair_keep,
    pair_in,
    side_out,
    side_in,
    total,
    far_out,
    far_in,
    mid_in,
    squares,
    load_sem,
    ag_send,
    ag_recv,
    front_send,
    front_recv,
    edge_send,
    edge_recv,
    route_send,
    route_recv,
    part_send,
    part_recv,
    pair_send,
    pair_recv,
    side_send,
    side_recv,
    far_send,
    far_recv,
    mid_recv,
    sq_send,
    sq_recv,
):
    sp, tp = lax.axis_index("sp"), lax.axis_index("tp")
    n_sp = nz * x_size
    n_tp = pool_all.shape[0]
    z, x = sp // x_size, sp % x_size
    y, core = tp // core_count, tp % core_count
    rows, width = stream.shape
    cols = out_ref.shape[1]
    group_width = pool_in.shape[1]
    half_rows = rows // halves
    core_rows = half_rows // core_count
    first_cols = width * first_share[1] // first_share[0]
    sibling = y * core_count + (1 - core)
    opposite = (1 - y) * core_count + core
    far_z = nz - 1

    def remote(src, dst, send, recv, to_sp, to_tp):
        return pltpu.make_async_remote_copy(
            src_ref=src,
            dst_ref=dst,
            send_sem=send,
            recv_sem=recv,
            device_id=(to_sp, to_tp),
            device_id_type=MESH,
        )

    def wait_bytes(ref, sem):
        pltpu.make_async_copy(ref, ref, sem).wait()

    loads = [
        pltpu.make_async_copy(src, dst, load_sem.at[i])
        for i, (src, dst) in enumerate(
            (
                (out_weight_hbm, out_weight),
                (stream_hbm, stream),
                (w_gate_hbm.at[0], w_gate),
                (w_up_hbm.at[0], w_up),
                (w_down_hbm.at[0], w_down),
            )
        )
    ]
    for load in loads:
        load.start()

    barrier = pltpu.get_barrier_semaphore()

    def greet(to_sp, to_tp):
        pl.semaphore_signal(barrier, inc=1, device_id=(to_sp, to_tp), device_id_type=MESH)

    for d in range(1, n_sp):
        greet((sp + d) % n_sp, tp)
    for d in range(1, n_tp):
        greet(sp, (tp + d) % n_tp)

    @pl.when(sp > 0)
    def _():
        for d in range(1, n_tp):
            greet(sp - 1, (tp + d) % n_tp)

    @pl.when(sp < n_sp - 1)
    def _():
        for d in range(1, n_tp):
            greet(sp + 1, (tp + d) % n_tp)

    near = (sp > 0).astype(jnp.int32) + (sp < n_sp - 1).astype(jnp.int32)
    pl.semaphore_wait(barrier, (n_sp - 1) + (n_tp - 1) * (1 + near))

    edge = pool_edges.shape[2]

    def edge_copy(side, to_tp):
        src = pool_in.at[pl.ds(rows - edge, edge)] if side == 0 else pool_in.at[pl.ds(0, edge)]
        return remote(
            src,
            pool_edges.at[tp, side],
            edge_send.at[side],
            edge_recv.at[side],
            sp + 1 if side == 0 else sp - 1,
            to_tp,
        )

    for side in range(2):

        @pl.when(sp < n_sp - 1 if side == 0 else sp > 0)
        def _():
            for d in range(n_tp):
                edge_copy(side, (tp + d) % n_tp).start()

    def front_copies(d):
        to = (tp + d) % n_tp
        return [
            remote(pool_in, pool_all.at[tp], front_send.at[0], front_recv.at[0], sp, to),
            remote(pool_weight.at[0], weight_all.at[tp], front_send.at[1], front_recv.at[1], sp, to),
            remote(pool_scale, scale_all.at[tp], front_send.at[2], front_recv.at[2], sp, to),
        ]

    for d in range(1, n_tp):
        for copy in front_copies(d):
            copy.start()
    pool_all[tp] = pool_in[...]
    weight_all[tp] = pool_weight[0]
    scale_all[tp] = pool_scale[...]

    route_rows = route_all.shape[1]
    names = lax.broadcasted_iota(jnp.int32, (route_rows, rows), 0)
    by_expert = jnp.zeros((route_rows, rows), jnp.float32)
    for k in range(routes.shape[0]):
        by_expert += jnp.where(routes[k : k + 1, :] == names, route_weights[k : k + 1, :], 0.0)
    route_all[sp] = by_expert

    def route_copy(d):
        to = (sp + d) % n_sp
        return remote(
            route_all.at[sp], route_all.at[sp], route_send.at[0], route_recv.at[0], to, tp
        )

    for d in range(1, n_sp):
        route_copy(d).start()

    others = pl.ds(0, n_tp - 1)
    front_all = (pool_all, weight_all, scale_all)
    for i, ref in enumerate(front_all):
        wait_bytes(ref.at[others], front_recv.at[i])

    @pl.when(sp > 0)
    def _():
        wait_bytes(pool_edges.at[:, 0], edge_recv.at[0])
        for g in range(n_tp):
            padded[g, 0:reach_rows, :] = pool_edges[g, 0].astype(jnp.float32)[edge - reach_rows :]

    @pl.when(sp == 0)
    def _():
        padded[:, 0:reach_rows, :] = jnp.zeros((n_tp, reach_rows, group_width), jnp.float32)

    @pl.when(sp < n_sp - 1)
    def _():
        wait_bytes(pool_edges.at[:, 1], edge_recv.at[1])
        for g in range(n_tp):
            padded[g, reach_rows + rows :, :] = pool_edges[g, 1].astype(jnp.float32)[:reach_rows]

    @pl.when(sp == n_sp - 1)
    def _():
        padded[:, reach_rows + rows :, :] = jnp.zeros((n_tp, reach_rows, group_width), jnp.float32)

    positions = sp * rows + lax.broadcasted_iota(jnp.int32, (rows, group_width), 0)
    mean_square = jnp.zeros((rows, 1), jnp.float32)
    for g in range(n_tp):
        radius = 1 << g
        values = pool_all[g].astype(jnp.float32)
        padded[g, reach_rows : reach_rows + rows, :] = values
        window_sum = values
        for offset in range(1, radius + 1):
            window_sum += padded[g, reach_rows + offset : reach_rows + offset + rows, :]
            window_sum += padded[g, reach_rows - offset : reach_rows - offset + rows, :]
        last = jnp.minimum(positions + radius, n_sp * rows - 1)
        counts = last - jnp.maximum(positions - radius, 0) + 1
        deviation = (window_sum / counts.astype(jnp.float32) - values).astype(jnp.bfloat16)
        pool_out = (
            jnp.dot(deviation, weight_all[g], preferred_element_type=jnp.float32) * scale_all[g]
        ).astype(jnp.bfloat16)
        normed[:, g * group_width : (g + 1) * group_width] = pool_out
        wide = pool_out.astype(jnp.float32)
        mean_square += jnp.sum(wide * wide, axis=1, keepdims=True)
    pool_width = n_tp * group_width
    row_scale = lax.rsqrt(mean_square / pool_width + epsilon)
    normed[...] = (normed[...].astype(jnp.float32) * row_scale * pool_norm[...]).astype(jnp.bfloat16)

    for load in loads[:2]:
        load.wait()
    for t in range(width // cols):
        mix_out[:, t * cols : (t + 1) * cols] = jnp.dot(
            normed[...], out_weight[:, t * cols : (t + 1) * cols], preferred_element_type=jnp.float32
        )

    tile = 32

    def mix_rows(first, count):
        def body(i, carry):
            part = pl.ds(pl.multiple_of(first + i * tile, tile), tile)
            value = mix_out[part, :]
            scaled = value * lax.rsqrt(jnp.mean(value * value, axis=1, keepdims=True) + epsilon)
            summed = stream[part, :].astype(jnp.float32) + scaled * mix_norm[...]
            summed = summed.astype(jnp.bfloat16)
            mixed[part, :] = summed
            wide = summed.astype(jnp.float32)
            wide = wide * lax.rsqrt(jnp.mean(wide * wide, axis=1, keepdims=True) + epsilon)
            tokens[sp, part, :] = (wide * ffn_norm[...]).astype(jnp.bfloat16)
            return carry

        lax.fori_loop(0, count // tile, body, 0)

    def piece(block, half, kind, whose):
        first = pl.multiple_of(half * half_rows + whose * core_rows, 16)
        span = pl.ds(0, first_cols) if kind == XF else pl.ds(first_cols, width - first_cols)
        return tokens.at[block, pl.ds(first, core_rows), span]

    def ag_copy(block, half, kind, way, lane_of=0):
        to_sp = {UP: sp + x_size, DOWN: sp - x_size, ACROSS: z * x_size + (1 - x), SIBLING: sp}[way]
        recv = ag_recv.at[block, half, 2 if way == SIBLING else kind]
        ref = piece(block, half, kind, core)
        to_tp = sibling if way == SIBLING else tp
        return remote(ref, ref, ag_send.at[way, lane_of], recv, to_sp, to_tp)

    def ag_arrived(block, half, kind):
        wait_bytes(piece(block, half, kind, core), ag_recv.at[block, half, kind])

    def sibling_arrived(block, half):
        first = pl.multiple_of(half * half_rows + (1 - core) * core_rows, 16)
        wait_bytes(tokens.at[block, pl.ds(first, core_rows), :], ag_recv.at[block, half, 2])

    def ag_start(zc, half, col_is_own, kind):
        block = zc * x_size + (x if col_is_own else 1 - x)

        if col_is_own and kind == XF:

            @pl.when(zc == z)
            def _():
                ag_copy(block, half, kind, ACROSS).start()

        lane_of = 0 if col_is_own else 1
        if col_is_own or kind == XF:

            @pl.when((zc <= z) & (z < far_z))
            def _():
                ag_copy(block, half, kind, UP, lane_of).start()

            @pl.when((zc >= z) & (z > 0))
            def _():
                ag_copy(block, half, kind, DOWN, lane_of).start()

        if col_is_own and kind == ZF:

            @pl.when(zc == z)
            def _():
                ag_copy(block, half, kind, ACROSS).start()

            @pl.when((zc != z) & ~from_end(zc))
            def _():
                ag_copy(block, half, kind, ACROSS, 1).start()

        if col_is_own:

            @pl.when(zc != z)
            def _():
                ag_copy(block, half, kind, SIBLING).start()

        else:
            ag_copy(block, half, kind, SIBLING).start()

        if not col_is_own and kind == ZF and nz > 2:

            @pl.when((zc == z) & (z == 0))
            def _():
                ag_copy(block, half, kind, UP, 2).start()

            @pl.when((zc == z) & (z == far_z))
            def _():
                ag_copy(block, half, kind, DOWN, 2).start()

    def from_end(zc):
        at_end = ((zc == 0) & (z == 1)) | ((zc == far_z) & (z == far_z - 1))
        return at_end & (z > 0) & (z < far_z)

    def ag_sent():
        carried = pl.ds(0, halves * core_rows)
        xf, zf = pl.ds(0, first_cols), pl.ds(first_cols, width - first_cols)
        wait_bytes(tokens.at[pl.ds(0, n_sp - 1), carried, :], ag_send.at[SIBLING, 0])
        wait_bytes(tokens.at[0, carried, :], ag_send.at[ACROSS, 0])
        for at_z in range(nz):

            @pl.when(z == at_z)
            def _():
                across = nz - 1
                if 0 < at_z < far_z:
                    across -= (at_z == 1) + (at_z == far_z - 1)
                if across > 0:
                    wait_bytes(tokens.at[pl.ds(0, across), carried, zf], ag_send.at[ACROSS, 1])
                if nz > 2 and at_z == 0:
                    wait_bytes(tokens.at[0, carried, zf], ag_send.at[UP, 2])
                if nz > 2 and at_z == far_z:
                    wait_bytes(tokens.at[0, carried, zf], ag_send.at[DOWN, 2])
                if at_z < far_z:
                    wait_bytes(tokens.at[pl.ds(0, at_z + 1), carried, :], ag_send.at[UP, 0])
                    wait_bytes(tokens.at[pl.ds(0, at_z + 1), carried, xf], ag_send.at[UP, 1])
                if at_z > 0:
                    wait_bytes(tokens.at[pl.ds(0, nz - at_z), carried, :], ag_send.at[DOWN, 0])
                    wait_bytes(tokens.at[pl.ds(0, nz - at_z), carried, xf], ag_send.at[DOWN, 1])

    def take(zc, half, col_is_own, kind):
        block = zc * x_size + (x if col_is_own else 1 - x)
        ag_arrived(block, half, kind)
        ag_start(zc, half, col_is_own, kind)

    for whose in range(core_count):
        for half in range(halves):
            mix_rows(half * half_rows + (core if whose == 0 else 1 - core) * core_rows, core_rows)
            if whose == 0:
                ag_start(z, half, True, XF)
                ag_start(z, half, True, ZF)

    wait_bytes(route_all.at[pl.ds(0, n_sp - 1)], route_recv.at[0])
    for load in loads[2:]:
        load.wait()

    upper = z >= (nz + 1) // 2
    low_z = jnp.where(upper, far_z - z, z)

    def plane_at(step):
        plane = jnp.where(step <= low_z, low_z - step, step)
        return jnp.where(upper, far_z - plane, plane)

    inner = low_z > 0

    inner_order = {2: (1, 0), 3: (2, 0), 4: (1, 1), 5: (2, 1)}
    if nz > 3:
        inner_order.update({5: (3, 0), 6: (3, 1), 7: (2, 1)})

    def unit_at(k):
        step, half = k // halves, k % halves
        for at, (inner_step, inner_half) in inner_order.items():
            step = jnp.where(inner & (k == at), inner_step, step)
            half = jnp.where(inner & (k == at), inner_half, half)
        return plane_at(step), half

    n_hidden = hidden.shape[1]
    hidden_tile = min(256, n_hidden)

    def span_of(half):
        return pl.ds(pl.multiple_of(half * half_rows, half_rows), half_rows)

    def part_copy(block, half, q_y):
        q = q_y * core_count + (1 - core)
        return remote(
            parts.at[block, q, span_of(half)],
            parts_in.at[block, q_y, span_of(half)],
            part_send.at[0],
            part_recv.at[block, half],
            sp,
            sibling,
        )

    sub_rows = half_rows // subs

    def sub_of(half, sub):
        return pl.ds(pl.multiple_of(half * half_rows + sub * sub_rows, sub_rows), sub_rows)

    def pair_copy(block, half, sub):
        at = sub_of(half, sub)
        return remote(
            pair_out.at[block, at],
            pair_in.at[block, at],
            pair_send.at[0],
            pair_recv.at[block, half, sub],
            sp,
            opposite,
        )

    def side_copy(zc, half, sub):
        at = sub_of(half, sub)
        return remote(
            side_out.at[zc, at],
            side_in.at[zc, at],
            side_send.at[0],
            side_recv.at[zc, half, sub],
            z * x_size + (1 - x),
            tp,
        )

    def far_copy(zc, half, sub):
        at = sub_of(half, sub)
        return remote(
            far_out.at[zc, at],
            far_in.at[z, at],
            far_send.at[0],
            far_recv.at[0],
            zc * x_size + x,
            tp,
        )

    end = (z == 0) | (z == far_z)

    def goes_by_mid(from_z, to_z):
        from_end_z = (from_z == 0) | (from_z == far_z)
        return from_end_z & ((from_z - to_z == 2) | (to_z - from_z == 2))

    def mid_copy(zc, half, sub):
        at = sub_of(half, sub)
        side = jnp.where(z == 0, 0, 1)
        return remote(
            far_out.at[zc, at],
            mid_in.at[side, at],
            far_send.at[0],
            mid_recv.at[side, half, sub],
            jnp.where(z == 0, 1, far_z - 1) * x_size + x,
            tp,
        )

    def compute(block, half):
        own_row = lax.broadcasted_iota(jnp.int32, (route_rows, half_rows), 0) == sp
        weight = jnp.sum(
            jnp.where(own_row, route_all[block, :, span_of(half)], 0.0), axis=0, keepdims=True
        )
        weight = jnp.broadcast_to(weight, (128, half_rows)).T
        for j in range(n_hidden // hidden_tile):
            span = slice(j * hidden_tile, (j + 1) * hidden_tile)
            data = tokens[block, span_of(half), :]
            gate = jnp.dot(data, w_gate[:, span], preferred_element_type=jnp.float32)
            up = jnp.dot(data, w_up[:, span], preferred_element_type=jnp.float32)
            gate_cut = jnp.minimum(gate + gate_bias[:, span], clamp_limit)
            up_cut = jnp.clip(up + up_bias[:, span], -clamp_limit, clamp_limit)
            active = (up_cut + 1.0) * (gate_cut * jax.nn.sigmoid(sigmoid_alpha * gate_cut))
            for i in range(hidden_tile // 128):
                lane = slice(i * 128, (i + 1) * 128)
                at = j * hidden_tile + i * 128
                hidden[:, at : at + 128] = (active[:, lane] * weight).astype(jnp.bfloat16)

        def down(i, carry):
            whose = jnp.where(i < 2, 1 - core, core)
            q = (i % 2) * core_count + whose
            at = pl.ds(pl.multiple_of(q * cols, cols), cols)
            parts[block, q, span_of(half), :] = jnp.dot(
                hidden[...], w_down[:, at], preferred_element_type=jnp.float32
            ).astype(jnp.bfloat16)

            @pl.when(i < 2)
            def _():
                part_copy(block, half, i % 2).start()

            return carry

        lax.fori_loop(0, n_tp, down, 0)

    def wide_of(ref, *at):
        return ref[at].astype(jnp.float32)

    def join_cores(block, half):
        wait_bytes(parts_in.at[block, :, span_of(half)], part_recv.at[block, half])
        for sub in range(subs):
            at = sub_of(half, sub)
            away = wide_of(parts, block, opposite, at) + wide_of(parts_in, block, 1 - y, at)
            pair_out[block, at, :] = away.astype(jnp.bfloat16)
            pair_copy(block, half, sub).start()
        at = span_of(half)
        pair_keep[block, at, :] = wide_of(parts, block, tp, at) + wide_of(parts_in, block, y, at)

    def join_own_cores(k):
        zc, half = unit_at(k)
        join_cores(zc * x_size + x, half)

    def join_other_cores(k):
        zc, half = unit_at(k)
        join_cores(zc * x_size + (1 - x), half)

    def join_pair_other(k):
        zc, half = unit_at(k)
        block = zc * x_size + (1 - x)
        for sub in range(subs):
            at = sub_of(half, sub)
            pair_copy(block, half, sub).wait_recv()
            both = pair_keep[block, at, :] + wide_of(pair_in, block, at)
            side_out[zc, at, :] = both.astype(jnp.bfloat16)
            side_copy(zc, half, sub).start()

    def join_pair_own(k):
        zc, half = unit_at(k)
        block = zc * x_size + x
        for sub in range(subs):
            pair_copy(block, half, sub).wait_recv()
        at = span_of(half)
        total[zc, at, :] = pair_keep[block, at, :] + wide_of(pair_in, block, at)

    def join_sides(k):
        zc, half = unit_at(k)
        for sub in range(subs):
            at = sub_of(half, sub)
            side_copy(zc, half, sub).wait_recv()
            total[zc, at, :] += wide_of(side_in, zc, at)
            for side, end_z in enumerate((0, far_z)):

                @pl.when((~end) & goes_by_mid(end_z, zc) & (2 * z == zc + end_z))
                def _():
                    wait_bytes(mid_in.at[side, at], mid_recv.at[side, half, sub])
                    total[zc, at, :] += wide_of(mid_in, side, at)

            @pl.when(zc != z)
            def _():
                far_out[zc, at, :] = total[zc, at, :].astype(jnp.bfloat16)

            @pl.when((zc != z) & goes_by_mid(z, zc))
            def _():
                mid_copy(zc, half, sub).start()

            @pl.when((zc != z) & ~goes_by_mid(z, zc))
            def _():
                far_copy(zc, half, sub).start()

    units = nz * halves

    def take_first(k):
        z_next, half_next = unit_at(k)
        take(z_next, half_next, True, ZF)

    def take_rest(k):
        z_next, half_next = unit_at(k)
        take(z_next, half_next, True, XF)
        take(z_next, half_next, False, XF)

    def take_ahead(k):
        take_first(k)
        take_rest(k)

    def compute_own(k):
        zc, half = unit_at(k)
        block = zc * x_size + x

        @pl.when(k >= halves)
        def _():
            sibling_arrived(block, half)

        compute(block, half)

    def compute_other(k):
        zc, half = unit_at(k)
        block = zc * x_size + (1 - x)
        sibling_arrived(block, half)
        compute(block, half)

    def take_other(k):
        zc, half = unit_at(k)
        take(zc, half, False, ZF)

    compute_own(0)
    take(z, 0, False, XF)
    compute_own(1)
    join_own_cores(0)
    take_other(0)
    join_own_cores(1)
    compute_other(0)
    take(z, 1, False, XF)
    if units > halves:

        take_first(2)

        @pl.when(inner)
        def _():
            take_first(3)

    join_other_cores(0)
    take_other(1)
    join_pair_own(0)

    def sides(k, carry):
        join_sides(k)
        return carry

    def unit_body(k, carry):
        zc, half = unit_at(k)

        @pl.when(~inner)
        def _():
            take(zc, half, True, XF)

        compute_other(k - 1)

        @pl.when((~inner) & (k <= 3) & (k + 1 < units))
        def _():
            take_first(k + 1)

        @pl.when(inner & (k == 2))
        def _():
            take_rest(2)
            take_rest(3)

        compute_own(k)
        join_other_cores(k - 1)

        @pl.when(~inner)
        def _():
            take(zc, half, False, XF)

        for at, ahead in ((2, (4, 7)), (3, (5,)), (4, (6,))) if nz > 3 else ((2, (4, 5)),):

            @pl.when(inner & (k == at))
            def _():
                for unit in ahead:
                    take_ahead(unit)

        if units > 8:

            @pl.when(inner & (k >= 6) & (k + 2 < units))
            def _():
                take_ahead(k + 2)

        take_other(k)
        join_own_cores(k)

        @pl.when((~inner) & (k > 3) & (k + 1 < units))
        def _():
            take_first(k + 1)

        join_pair_other(k - 2)

        @pl.when(k < units - 1)
        def _():
            join_pair_own(k - 1)

        @pl.when((~inner) & (k >= 3))
        def _():
            join_sides(k - 3)

        @pl.when(inner & (k >= 6) & (k != 7))
        def _():
            join_sides(k - 4)

        @pl.when(inner & (k >= 6) & (k == units - 1))
        def _():
            join_sides(k - 3)

        return carry

    lax.fori_loop(halves, units, unit_body, 0)
    compute_other(units - 1)
    join_other_cores(units - 1)
    if units > halves:
        join_pair_own(units - 2)
    join_pair_other(units - 2)

    @pl.when(inner)
    def _():
        lax.fori_loop(0, halves, sides, 0)
        if units <= 6:
            lax.fori_loop(max(units - 4, halves), units - 3, sides, 0)

    if units > halves:
        join_sides(units - 3)

        if units > 7:

            @pl.when(inner)
            def _():
                join_sides(3)

    join_pair_own(units - 1)
    join_pair_other(units - 1)
    join_sides(units - 2)
    join_sides(units - 1)

    for side in range(2):

        @pl.when(sp < n_sp - 1 if side == 0 else sp > 0)
        def _():
            wait_bytes(pool_edges.at[:, side], edge_send.at[side])

    for i, ref in enumerate(front_all):
        wait_bytes(ref.at[others], front_send.at[i])
    wait_bytes(route_all.at[pl.ds(0, n_sp - 1)], route_send.at[0])
    ag_sent()
    wait_bytes(parts_in, part_send.at[0])
    wait_bytes(pair_out, pair_send.at[0])
    wait_bytes(side_out, side_send.at[0])

    for at_z in range(nz):
        direct = [
            i
            for i in range(nz)
            if i != at_z and not (i in (0, far_z) and abs(i - at_z) == 2)
        ]

        @pl.when(z == at_z)
        def _():
            if direct:
                wait_bytes(far_in.at[pl.ds(0, len(direct))], far_recv.at[0])
            for i in direct:
                total[at_z] += far_in[i].astype(jnp.float32)

    combined = total[z]

    own_squares = jnp.sum(combined * combined, axis=1, keepdims=True)
    squares[tp] = jnp.broadcast_to(own_squares, (rows, 128)).T[:8]

    def squares_copy(d):
        return remote(
            squares.at[tp], squares.at[tp], sq_send.at[0], sq_recv.at[0], sp, (tp + d) % n_tp
        )

    for d in range(1, n_tp):
        squares_copy(d).start()
    wait_bytes(squares.at[others], sq_recv.at[0])
    summed = squares[0]
    for i in range(1, n_tp):
        summed += squares[i]
    row_scale = lax.rsqrt(summed[:1] / width + epsilon)
    row_scale = jnp.broadcast_to(row_scale, (128, rows)).T
    for i in range(cols // 128):
        lane = slice(i * 128, (i + 1) * 128)
        own = mixed[:, pl.ds(pl.multiple_of(tp * cols + i * 128, 128), 128)].astype(jnp.float32)
        out_ref[:, lane] = (own + total[z, :, lane] * row_scale * expert_norm[:, lane]).astype(
            jnp.bfloat16
        )

    wait_bytes(squares.at[others], sq_send.at[0])
    if nz > 1:
        wait_bytes(far_out.at[pl.ds(0, nz - 1)], far_send.at[0])


def gathered_shards(*args):
    pool_in, pool_norm, out_weight, stream = args[0], args[3], args[4], args[5]
    w_gate, w_down = args[10], args[14]
    n_sp, n_tp = lax.axis_size("sp"), lax.axis_size("tp")
    nz = n_sp // x_size
    rows, width = stream.shape
    n_hidden = w_gate.shape[2]
    cols = width // n_tp
    group_width = pool_in.shape[1]
    bf16, f32 = jnp.bfloat16, jnp.float32
    row_args = (2, 3, 6, 7, 15)
    args = [a.reshape(1, -1) if i in row_args else a for i, a in enumerate(args)]
    args[8], args[9] = args[8].T, args[9].T
    in_hbm = (4, 5, 10, 11, 14)
    in_specs = [
        pl.BlockSpec(memory_space=pl.ANY if i in in_hbm else pltpu.VMEM) for i in range(len(args))
    ]
    edge = 2 * reach_rows
    route_rows = -(-n_sp // 8) * 8
    dma = pltpu.SemaphoreType.DMA
    scratch = [
        pltpu.VMEM((n_sp, rows, width), bf16),
        pltpu.VMEM((width, n_hidden), bf16),
        pltpu.VMEM((width, n_hidden), bf16),
        pltpu.VMEM((n_hidden, width), bf16),
        pltpu.VMEM(out_weight.shape, bf16),
        pltpu.VMEM((rows, width), bf16),
        pltpu.VMEM((n_tp, rows, group_width), bf16),
        pltpu.VMEM((n_tp, 2, edge, group_width), bf16),
        pltpu.VMEM((n_tp, group_width, group_width), bf16),
        pltpu.VMEM((n_tp, 1, group_width), f32),
        pltpu.VMEM((n_tp, rows + 2 * reach_rows, group_width), f32),
        pltpu.VMEM((rows, n_tp * group_width), bf16),
        pltpu.VMEM((rows, width), f32),
        pltpu.VMEM((rows, width), bf16),
        pltpu.VMEM((n_sp, route_rows, rows), f32),
        pltpu.VMEM((rows // halves, n_hidden), bf16),
        pltpu.VMEM((n_sp, n_tp, rows, cols), bf16),
        pltpu.VMEM((n_sp, n_tp // core_count, rows, cols), bf16),
        pltpu.VMEM((n_sp, rows, cols), bf16),
        pltpu.VMEM((n_sp, rows, cols), f32),
        pltpu.VMEM((n_sp, rows, cols), bf16),
        pltpu.VMEM((nz, rows, cols), bf16),
        pltpu.VMEM((nz, rows, cols), bf16),
        pltpu.VMEM((nz, rows, cols), f32),
        pltpu.VMEM((nz, rows, cols), bf16),
        pltpu.VMEM((nz, rows, cols), bf16),
        pltpu.VMEM((2, rows, cols), bf16),
        pltpu.VMEM((n_tp, 8, rows), f32),
        dma((5,)),
        dma((4, 3)),
        dma((n_sp, halves, 3)),
        dma((3,)),
        dma((3,)),
        dma((2,)),
        dma((2,)),
        dma((1,)),
        dma((1,)),
        dma((1,)),
        dma((n_sp, halves)),
        dma((1,)),
        dma((n_sp, halves, subs)),
        dma((1,)),
        dma((nz, halves, subs)),
        dma((1,)),
        dma((1,)),
        dma((2, halves, subs)),
        dma((1,)),
        dma((1,)),
    ]
    return pl.pallas_call(
        functools.partial(layer_kernel, nz),
        out_shape=jax.ShapeDtypeStruct((rows, cols), bf16),
        in_specs=in_specs,
        out_specs=pl.BlockSpec(memory_space=pltpu.VMEM),
        scratch_shapes=scratch,
        compiler_params=pltpu.CompilerParams(
            collective_id=0, has_side_effects=True, vmem_limit_bytes=vmem_limit
        ),
        name="layer",
    )(*args)


def shards(*args):
    pool_in, out_weight, stream, w_gate = args[0], args[4], args[5], args[10]
    n_sp, n_tp = lax.axis_size("sp"), lax.axis_size("tp")
    rows, width = stream.shape
    cols, n_hidden = width // n_tp, w_gate.shape[2]
    slots = n_sp * rows * (2 * width + (2 + 1 + 1 + 2 + 1) * 2 * cols + 2 * width + 2 * width)
    fixed = 2 * (3 * width * n_hidden + out_weight.size) + 10 * rows * width
    fits = slots + fixed < vmem_limit * 9 // 10
    shaped = (
        n_tp == 2 * core_count
        and n_sp % x_size == 0
        and w_gate.shape[0] == 1
        and rows % (128 * halves) == 0
        and width % (128 * first_share[0]) == 0
        and cols % 128 == 0
        and n_hidden % 256 == 0
        and pool_in.shape[1] == 128
        and n_sp <= 128
    )
    return (gathered_shards if fits and shaped else routed_shards)(*args)


def solution(mesh):
    in_specs = (
        P("sp", "tp"),
        P("tp", None, None),
        P("tp"),
        P(),
        P(),
        P("sp", None),
        P(),
        P(),
        P("sp", None),
        P("sp", None),
        P("sp", None, "tp"),
        P("sp", None, "tp"),
        P("sp", "tp"),
        P("sp", "tp"),
        P("sp", "tp", None),
        P("tp"),
    )
    out_specs = P("sp", "tp")
    return jax.shard_map(shards, mesh=mesh, in_specs=in_specs, out_specs=out_specs, check_vma=False)
```

```python
import functools

import jax
import jax.numpy as jnp
from jax import lax
from jax.experimental import pallas as pl
from jax.experimental.pallas import tpu as pltpu
from jax.sharding import PartitionSpec as P

MESH = pl.DeviceIdType.MESH

epsilon = 1e-06
reach_rows = 8
clamp_limit = 7.0
sigmoid_alpha = 1.702
chunk_counts = (2,)


def extended_2(shard, sides, width):
    for axis, dim in sides:
        count, length = (lax.axis_size(axis), shard.shape[dim])
        up = [(i, (i + 1) % count) for i in range(count - 1)]
        down = [(j, i) for i, j in up]
        last = lax.slice_in_dim(shard, length - width, length, axis=dim)
        leading = lax.slice_in_dim(shard, 0, width, axis=dim)
        before = lax.ppermute(last, axis, up)
        after = lax.ppermute(leading, axis, down)
        shard = jnp.concatenate([before, shard, after], axis=dim)
    return shard


def rms_scale(values):
    return values * lax.rsqrt(jnp.mean(values * values, axis=-1, keepdims=True) + epsilon)


def routed_shards(
    pool_in,
    pool_weight,
    pool_scale,
    pool_norm,
    out_weight,
    stream,
    mix_norm,
    ffn_norm,
    routes,
    route_weights,
    w_gate,
    w_up,
    gate_bias,
    up_bias,
    w_down,
    expert_norm,
):
    rows_dev = pool_in.shape[0]
    length = rows_dev * lax.axis_size("sp")
    radius = jnp.left_shift(1, lax.axis_index("tp"))
    positions = lax.axis_index("sp") * rows_dev + jnp.arange(rows_dev)
    padded = extended_2(pool_in, (("sp", 0),), reach_rows).astype(jnp.float32)
    window_sum = jnp.zeros((rows_dev, pool_in.shape[1]), jnp.float32)
    counts = jnp.zeros((rows_dev,), jnp.float32)
    for offset in range(-reach_rows, reach_rows + 1):
        inside = (positions + offset >= 0) & (positions + offset < length) & (abs(offset) <= radius)
        window_sum = window_sum + jnp.where(
            inside[:, None], padded[reach_rows + offset : reach_rows + offset + rows_dev], 0.0
        )
        counts = counts + inside.astype(jnp.float32)
    deviation = (window_sum / counts[:, None] - padded[reach_rows : reach_rows + rows_dev]).astype(
        jnp.bfloat16
    )
    pool_out = (
        jnp.dot(deviation, pool_weight[0], preferred_element_type=jnp.float32) * pool_scale
    ).astype(jnp.bfloat16)
    all_groups = lax.all_gather(pool_out, "tp", axis=1, tiled=True)
    normed = (rms_scale(all_groups.astype(jnp.float32)) * pool_norm).astype(jnp.bfloat16)
    mix_out = jnp.dot(normed, out_weight, preferred_element_type=jnp.float32)
    mixed = (stream.astype(jnp.float32) + rms_scale(mix_out) * mix_norm).astype(jnp.bfloat16)
    expert_in = (rms_scale(mixed.astype(jnp.float32)) * ffn_norm).astype(jnp.bfloat16)
    model_width = mixed.shape[1]
    experts = lax.axis_size("sp") * w_gate.shape[0]
    top_count = routes.shape[1]
    capacity = rows_dev * top_count * 3 // (2 * experts)
    quarter = capacity // lax.axis_size("tp")
    chunks = next((n for n in chunk_counts if quarter % (8 * n) == 0), 1)
    chunk_rows, own_rows = capacity // chunks, quarter // chunks

    names = routes.T[:, None, :] == jnp.arange(experts, dtype=jnp.int32)[None, :, None]
    member = jnp.any(names, axis=0)
    weight = jnp.sum(jnp.where(names, route_weights.T[:, None, :], 0.0), axis=0)
    order = jnp.arange(rows_dev)
    earlier = (order[:, None] < order[None, :]).astype(jnp.bfloat16)
    place = jnp.dot(
        member.astype(jnp.bfloat16), earlier, preferred_element_type=jnp.float32
    ).astype(jnp.int32)
    place = jnp.where(member, place, -1)

    def dispatched(chunk):
        first = chunk * chunk_rows + lax.axis_index("tp") * own_rows
        slots = first + jnp.arange(own_rows, dtype=jnp.int32)
        pick = (place[:, None, :] == slots[None, :, None]).astype(jnp.bfloat16)
        rows = jnp.dot(pick.reshape(experts * own_rows, rows_dev), expert_in)
        own_slots = rows.reshape(experts, own_rows, model_width)
        arrived = lax.all_to_all(own_slots, "sp", split_axis=0, concat_axis=0, tiled=True)
        return lax.all_gather(arrived, "tp", axis=1, tiled=True)

    def expert(slot_block):
        row_block = slot_block.reshape(-1, model_width)
        gate_pre = jnp.dot(row_block, w_gate[0], preferred_element_type=jnp.float32) + gate_bias[0]
        up_pre = jnp.dot(row_block, w_up[0], preferred_element_type=jnp.float32) + up_bias[0]
        gate_cut = jnp.minimum(gate_pre, clamp_limit)
        up_cut = jnp.clip(up_pre, -clamp_limit, clamp_limit)
        activation = (
            (up_cut + 1.0) * (gate_cut * jax.nn.sigmoid(sigmoid_alpha * gate_cut))
        ).astype(jnp.bfloat16)
        partial_value = jnp.dot(activation, w_down[0], preferred_element_type=jnp.float32).astype(
            jnp.bfloat16
        )
        partial_value = partial_value.reshape(slot_block.shape)
        summed = lax.psum_scatter(partial_value, "tp", scatter_dimension=2, tiled=True)
        return lax.all_to_all(summed, "sp", split_axis=0, concat_axis=0, tiled=True)

    def weighted(chunk, returned):
        slots = chunk * chunk_rows + jnp.arange(chunk_rows, dtype=jnp.int32)
        spread = jnp.where(place[:, None, :] == slots[None, :, None], weight[:, None, :], 0.0)
        spread = spread.reshape(experts * chunk_rows, rows_dev)
        high = spread.astype(jnp.bfloat16)
        low = (spread - high.astype(jnp.float32)).astype(jnp.bfloat16)
        flat = returned.reshape(experts * chunk_rows, -1)
        over_slots = (((0,), (0,)), ((), ()))
        return lax.dot_general(
            high, flat, over_slots, preferred_element_type=jnp.float32
        ) + lax.dot_general(low, flat, over_slots, preferred_element_type=jnp.float32)

    blocks = [dispatched(chunk) for chunk in range(chunks)]
    parts = [expert(block) for block in blocks]
    col_count = parts[0].shape[2]
    combined = sum(weighted(chunk, part) for chunk, part in enumerate(parts))
    squares = lax.psum(jnp.sum(combined * combined, axis=1), "tp")
    row_scale = lax.rsqrt(squares / model_width + epsilon)
    own_cols = lax.dynamic_slice_in_dim(
        mixed.astype(jnp.float32), lax.axis_index("tp") * col_count, col_count, 1
    )
    return (own_cols + combined * row_scale[:, None] * expert_norm).astype(jnp.bfloat16)


x_size = 2
core_count = 2
halves = 2
subs = 2
first_share = 16, 5
vmem_limit = 60 * 1024 * 1024
UP, DOWN, ACROSS, SIBLING = range(4)
XF, ZF = range(2)


def layer_kernel(
    nz,
    pool_in,
    pool_weight,
    pool_scale,
    pool_norm,
    out_weight_hbm,
    stream_hbm,
    mix_norm,
    ffn_norm,
    routes,
    route_weights,
    w_gate_hbm,
    w_up_hbm,
    gate_bias,
    up_bias,
    w_down_hbm,
    expert_norm,
    out_ref,
    tokens,
    w_gate,
    w_up,
    w_down,
    out_weight,
    stream,
    pool_all,
    pool_edges,
    weight_all,
    scale_all,
    padded,
    normed,
    mix_out,
    mixed,
    route_all,
    hidden,
    parts,
    parts_in,
    pair_out,
    pair_keep,
    pair_in,
    side_out,
    side_in,
    total,
    far_out,
    far_in,
    mid_in,
    squares,
    load_sem,
    ag_send,
    ag_recv,
    front_send,
    front_recv,
    edge_send,
    edge_recv,
    route_send,
    route_recv,
    part_send,
    part_recv,
    pair_send,
    pair_recv,
    side_send,
    side_recv,
    far_send,
    far_recv,
    mid_recv,
    sq_send,
    sq_recv,
):
    sp, tp = lax.axis_index("sp"), lax.axis_index("tp")
    n_sp = nz * x_size
    n_tp = pool_all.shape[0]
    z, x = sp // x_size, sp % x_size
    y, core = tp // core_count, tp % core_count
    rows, width = stream.shape
    cols = out_ref.shape[1]
    group_width = pool_in.shape[1]
    half_rows = rows // halves
    core_rows = half_rows // core_count
    first_cols = width * first_share[1] // first_share[0]
    sibling = y * core_count + (1 - core)
    opposite = (1 - y) * core_count + core
    far_z = nz - 1

    def remote(src, dst, send, recv, to_sp, to_tp):
        return pltpu.make_async_remote_copy(
            src_ref=src,
            dst_ref=dst,
            send_sem=send,
            recv_sem=recv,
            device_id=(to_sp, to_tp),
            device_id_type=MESH,
        )

    def wait_bytes(ref, sem):
        pltpu.make_async_copy(ref, ref, sem).wait()

    loads = [
        pltpu.make_async_copy(src, dst, load_sem.at[i])
        for i, (src, dst) in enumerate(
            (
                (out_weight_hbm, out_weight),
                (stream_hbm, stream),
                (w_gate_hbm.at[0], w_gate),
                (w_up_hbm.at[0], w_up),
                (w_down_hbm.at[0], w_down),
            )
        )
    ]
    for load in loads:
        load.start()

    barrier = pltpu.get_barrier_semaphore()

    def greet(to_sp, to_tp):
        pl.semaphore_signal(barrier, inc=1, device_id=(to_sp, to_tp), device_id_type=MESH)

    for d in range(1, n_sp):
        greet((sp + d) % n_sp, tp)
    for d in range(1, n_tp):
        greet(sp, (tp + d) % n_tp)

    @pl.when(sp > 0)
    def _():
        for d in range(1, n_tp):
            greet(sp - 1, (tp + d) % n_tp)

    @pl.when(sp < n_sp - 1)
    def _():
        for d in range(1, n_tp):
            greet(sp + 1, (tp + d) % n_tp)

    near = (sp > 0).astype(jnp.int32) + (sp < n_sp - 1).astype(jnp.int32)
    pl.semaphore_wait(barrier, (n_sp - 1) + (n_tp - 1) * (1 + near))

    edge = pool_edges.shape[2]

    def edge_copy(side, to_tp):
        src = pool_in.at[pl.ds(rows - edge, edge)] if side == 0 else pool_in.at[pl.ds(0, edge)]
        return remote(
            src,
            pool_edges.at[tp, side],
            edge_send.at[side],
            edge_recv.at[side],
            sp + 1 if side == 0 else sp - 1,
            to_tp,
        )

    third = (1 - y) * core_count + (1 - core)
    front_all = (pool_all, weight_all, scale_all)
    front_own = (pool_in, pool_weight.at[0], pool_scale)

    def front_copy(i, src, owner, source, to_tp):
        return remote(
            src, front_all[i].at[owner], front_send.at[i], front_recv.at[i, source], sp, to_tp
        )

    for i, src in enumerate(front_own):
        front_copy(i, src, tp, 0, opposite).start()
    for i, src in enumerate(front_own):
        front_copy(i, src, tp, 1, sibling).start()
    for side in range(2):

        @pl.when(sp < n_sp - 1 if side == 0 else sp > 0)
        def _():
            for d in range(n_tp):
                edge_copy(side, (tp + d) % n_tp).start()

    pool_all[tp] = pool_in[...]
    weight_all[tp] = pool_weight[0]
    scale_all[tp] = pool_scale[...]

    route_rows = route_all.shape[1]
    names = lax.broadcasted_iota(jnp.int32, (route_rows, rows), 0)
    by_expert = jnp.zeros((route_rows, rows), jnp.float32)
    for k in range(routes.shape[0]):
        by_expert += jnp.where(routes[k : k + 1, :] == names, route_weights[k : k + 1, :], 0.0)
    route_all[sp] = by_expert

    def route_copy(d):
        to = (sp + d) % n_sp
        return remote(
            route_all.at[sp], route_all.at[sp], route_send.at[0], route_recv.at[0], to, tp
        )

    for d in range(1, n_sp):
        route_copy(d).start()

    others = pl.ds(0, n_tp - 1)
    for i, ref in enumerate(front_all):
        wait_bytes(ref.at[opposite], front_recv.at[i, 0])
        front_copy(i, ref.at[opposite], opposite, 2, sibling).start()
    for i, ref in enumerate(front_all):
        wait_bytes(ref.at[sibling], front_recv.at[i, 1])
        wait_bytes(ref.at[third], front_recv.at[i, 2])

    @pl.when(sp > 0)
    def _():
        wait_bytes(pool_edges.at[:, 0], edge_recv.at[0])
        for g in range(n_tp):
            padded[g, 0:reach_rows, :] = pool_edges[g, 0].astype(jnp.float32)[edge - reach_rows :]

    @pl.when(sp == 0)
    def _():
        padded[:, 0:reach_rows, :] = jnp.zeros((n_tp, reach_rows, group_width), jnp.float32)

    @pl.when(sp < n_sp - 1)
    def _():
        wait_bytes(pool_edges.at[:, 1], edge_recv.at[1])
        for g in range(n_tp):
            padded[g, reach_rows + rows :, :] = pool_edges[g, 1].astype(jnp.float32)[:reach_rows]

    @pl.when(sp == n_sp - 1)
    def _():
        padded[:, reach_rows + rows :, :] = jnp.zeros((n_tp, reach_rows, group_width), jnp.float32)

    positions = sp * rows + lax.broadcasted_iota(jnp.int32, (rows, group_width), 0)
    mean_square = jnp.zeros((rows, 1), jnp.float32)
    for g in range(n_tp):
        radius = 1 << g
        values = pool_all[g].astype(jnp.float32)
        padded[g, reach_rows : reach_rows + rows, :] = values
        window_sum = values
        for offset in range(1, radius + 1):
            window_sum += padded[g, reach_rows + offset : reach_rows + offset + rows, :]
            window_sum += padded[g, reach_rows - offset : reach_rows - offset + rows, :]
        last = jnp.minimum(positions + radius, n_sp * rows - 1)
        counts = last - jnp.maximum(positions - radius, 0) + 1
        deviation = (window_sum / counts.astype(jnp.float32) - values).astype(jnp.bfloat16)
        pool_out = (
            jnp.dot(deviation, weight_all[g], preferred_element_type=jnp.float32) * scale_all[g]
        ).astype(jnp.bfloat16)
        normed[:, g * group_width : (g + 1) * group_width] = pool_out
        wide = pool_out.astype(jnp.float32)
        mean_square += jnp.sum(wide * wide, axis=1, keepdims=True)
    pool_width = n_tp * group_width
    row_scale = lax.rsqrt(mean_square / pool_width + epsilon)
    normed[...] = (normed[...].astype(jnp.float32) * row_scale * pool_norm[...]).astype(jnp.bfloat16)

    for load in loads[:2]:
        load.wait()
    for t in range(width // cols):
        mix_out[:, t * cols : (t + 1) * cols] = jnp.dot(
            normed[...], out_weight[:, t * cols : (t + 1) * cols], preferred_element_type=jnp.float32
        )

    tile = 32

    def mix_rows(first, count):
        def body(i, carry):
            part = pl.ds(pl.multiple_of(first + i * tile, tile), tile)
            value = mix_out[part, :]
            scaled = value * lax.rsqrt(jnp.mean(value * value, axis=1, keepdims=True) + epsilon)
            summed = stream[part, :].astype(jnp.float32) + scaled * mix_norm[...]
            summed = summed.astype(jnp.bfloat16)
            mixed[part, :] = summed
            wide = summed.astype(jnp.float32)
            wide = wide * lax.rsqrt(jnp.mean(wide * wide, axis=1, keepdims=True) + epsilon)
            tokens[sp, part, :] = (wide * ffn_norm[...]).astype(jnp.bfloat16)
            return carry

        lax.fori_loop(0, count // tile, body, 0)

    def piece(block, half, kind, whose):
        first = pl.multiple_of(half * half_rows + whose * core_rows, 16)
        span = pl.ds(0, first_cols) if kind == XF else pl.ds(first_cols, width - first_cols)
        return tokens.at[block, pl.ds(first, core_rows), span]

    def ag_copy(block, half, kind, way, lane_of=0):
        to_sp = {UP: sp + x_size, DOWN: sp - x_size, ACROSS: z * x_size + (1 - x), SIBLING: sp}[way]
        recv = ag_recv.at[block, half, 2 if way == SIBLING else kind]
        ref = piece(block, half, kind, core)
        to_tp = sibling if way == SIBLING else tp
        return remote(ref, ref, ag_send.at[way, lane_of], recv, to_sp, to_tp)

    def ag_arrived(block, half, kind):
        wait_bytes(piece(block, half, kind, core), ag_recv.at[block, half, kind])

    def sibling_arrived(block, half):
        first = pl.multiple_of(half * half_rows + (1 - core) * core_rows, 16)
        wait_bytes(tokens.at[block, pl.ds(first, core_rows), :], ag_recv.at[block, half, 2])

    def ag_start(zc, half, col_is_own, kind):
        block = zc * x_size + (x if col_is_own else 1 - x)

        if col_is_own and kind == XF:

            @pl.when(zc == z)
            def _():
                ag_copy(block, half, kind, ACROSS).start()

        lane_of = 0 if col_is_own else 1
        if col_is_own or kind == XF:

            @pl.when((zc <= z) & (z < far_z))
            def _():
                ag_copy(block, half, kind, UP, lane_of).start()

            @pl.when((zc >= z) & (z > 0))
            def _():
                ag_copy(block, half, kind, DOWN, lane_of).start()

        if col_is_own and kind == ZF:

            @pl.when(zc == z)
            def _():
                ag_copy(block, half, kind, ACROSS).start()

            @pl.when((zc != z) & ~from_end(zc))
            def _():
                ag_copy(block, half, kind, ACROSS, 1).start()

        if col_is_own:

            @pl.when(zc != z)
            def _():
                ag_copy(block, half, kind, SIBLING).start()

        else:
            ag_copy(block, half, kind, SIBLING).start()

        if not col_is_own and kind == ZF and nz > 2:

            @pl.when((zc == z) & (z == 0))
            def _():
                ag_copy(block, half, kind, UP, 2).start()

            @pl.when((zc == z) & (z == far_z))
            def _():
                ag_copy(block, half, kind, DOWN, 2).start()

    def from_end(zc):
        at_end = ((zc == 0) & (z == 1)) | ((zc == far_z) & (z == far_z - 1))
        return at_end & (z > 0) & (z < far_z)

    def ag_sent():
        carried = pl.ds(0, halves * core_rows)
        xf, zf = pl.ds(0, first_cols), pl.ds(first_cols, width - first_cols)
        wait_bytes(tokens.at[pl.ds(0, n_sp - 1), carried, :], ag_send.at[SIBLING, 0])
        wait_bytes(tokens.at[0, carried, :], ag_send.at[ACROSS, 0])
        for at_z in range(nz):

            @pl.when(z == at_z)
            def _():
                across = nz - 1
                if 0 < at_z < far_z:
                    across -= (at_z == 1) + (at_z == far_z - 1)
                if across > 0:
                    wait_bytes(tokens.at[pl.ds(0, across), carried, zf], ag_send.at[ACROSS, 1])
                if nz > 2 and at_z == 0:
                    wait_bytes(tokens.at[0, carried, zf], ag_send.at[UP, 2])
                if nz > 2 and at_z == far_z:
                    wait_bytes(tokens.at[0, carried, zf], ag_send.at[DOWN, 2])
                if at_z < far_z:
                    wait_bytes(tokens.at[pl.ds(0, at_z + 1), carried, :], ag_send.at[UP, 0])
                    wait_bytes(tokens.at[pl.ds(0, at_z + 1), carried, xf], ag_send.at[UP, 1])
                if at_z > 0:
                    wait_bytes(tokens.at[pl.ds(0, nz - at_z), carried, :], ag_send.at[DOWN, 0])
                    wait_bytes(tokens.at[pl.ds(0, nz - at_z), carried, xf], ag_send.at[DOWN, 1])

    def take(zc, half, col_is_own, kind):
        block = zc * x_size + (x if col_is_own else 1 - x)
        ag_arrived(block, half, kind)
        ag_start(zc, half, col_is_own, kind)

    for whose in range(core_count):
        for half in range(halves):
            mix_rows(half * half_rows + (core if whose == 0 else 1 - core) * core_rows, core_rows)
            if whose == 0:
                ag_start(z, half, True, XF)
                ag_start(z, half, True, ZF)

    wait_bytes(route_all.at[pl.ds(0, n_sp - 1)], route_recv.at[0])
    for load in loads[2:]:
        load.wait()

    upper = z >= (nz + 1) // 2
    low_z = jnp.where(upper, far_z - z, z)

    def plane_at(step):
        plane = jnp.where(step <= low_z, low_z - step, step)
        return jnp.where(upper, far_z - plane, plane)

    inner = low_z > 0

    inner_order = {2: (1, 0), 3: (2, 0), 4: (1, 1), 5: (2, 1)}
    if nz > 3:
        inner_order.update({5: (3, 0), 6: (3, 1), 7: (2, 1)})

    def unit_at(k):
        step, half = k // halves, k % halves
        for at, (inner_step, inner_half) in inner_order.items():
            step = jnp.where(inner & (k == at), inner_step, step)
            half = jnp.where(inner & (k == at), inner_half, half)
        return plane_at(step), half

    n_hidden = hidden.shape[1]
    hidden_tile = min(256, n_hidden)

    def span_of(half):
        return pl.ds(pl.multiple_of(half * half_rows, half_rows), half_rows)

    def part_copy(block, half, q_y):
        q = q_y * core_count + (1 - core)
        return remote(
            parts.at[block, q, span_of(half)],
            parts_in.at[block, q_y, span_of(half)],
            part_send.at[0],
            part_recv.at[block, half],
            sp,
            sibling,
        )

    sub_rows = half_rows // subs

    def sub_of(half, sub):
        return pl.ds(pl.multiple_of(half * half_rows + sub * sub_rows, sub_rows), sub_rows)

    def pair_copy(block, half, sub):
        at = sub_of(half, sub)
        return remote(
            pair_out.at[block, at],
            pair_in.at[block, at],
            pair_send.at[0],
            pair_recv.at[block, half, sub],
            sp,
            opposite,
        )

    def side_copy(zc, half, sub):
        at = sub_of(half, sub)
        return remote(
            side_out.at[zc, at],
            side_in.at[zc, at],
            side_send.at[0],
            side_recv.at[zc, half, sub],
            z * x_size + (1 - x),
            tp,
        )

    def far_copy(zc, half, sub):
        at = sub_of(half, sub)
        return remote(
            far_out.at[zc, at],
            far_in.at[z, at],
            far_send.at[0],
            far_recv.at[0],
            zc * x_size + x,
            tp,
        )

    end = (z == 0) | (z == far_z)

    def goes_by_mid(from_z, to_z):
        from_end_z = (from_z == 0) | (from_z == far_z)
        return from_end_z & ((from_z - to_z == 2) | (to_z - from_z == 2))

    def mid_copy(zc, half, sub):
        at = sub_of(half, sub)
        side = jnp.where(z == 0, 0, 1)
        return remote(
            far_out.at[zc, at],
            mid_in.at[side, at],
            far_send.at[0],
            mid_recv.at[side, half, sub],
            jnp.where(z == 0, 1, far_z - 1) * x_size + x,
            tp,
        )

    def compute(block, half):
        own_row = lax.broadcasted_iota(jnp.int32, (route_rows, half_rows), 0) == sp
        weight = jnp.sum(
            jnp.where(own_row, route_all[block, :, span_of(half)], 0.0), axis=0, keepdims=True
        )
        weight = jnp.broadcast_to(weight, (128, half_rows)).T
        for j in range(n_hidden // hidden_tile):
            span = slice(j * hidden_tile, (j + 1) * hidden_tile)
            data = tokens[block, span_of(half), :]
            gate = jnp.dot(data, w_gate[:, span], preferred_element_type=jnp.float32)
            up = jnp.dot(data, w_up[:, span], preferred_element_type=jnp.float32)
            gate_cut = jnp.minimum(gate + gate_bias[:, span], clamp_limit)
            up_cut = jnp.clip(up + up_bias[:, span], -clamp_limit, clamp_limit)
            active = (up_cut + 1.0) * (gate_cut * jax.nn.sigmoid(sigmoid_alpha * gate_cut))
            for i in range(hidden_tile // 128):
                lane = slice(i * 128, (i + 1) * 128)
                at = j * hidden_tile + i * 128
                hidden[:, at : at + 128] = (active[:, lane] * weight).astype(jnp.bfloat16)

        def down(i, carry):
            whose = jnp.where(i < 2, 1 - core, core)
            q = (i % 2) * core_count + whose
            at = pl.ds(pl.multiple_of(q * cols, cols), cols)
            parts[block, q, span_of(half), :] = jnp.dot(
                hidden[...], w_down[:, at], preferred_element_type=jnp.float32
            ).astype(jnp.bfloat16)

            @pl.when(i < 2)
            def _():
                part_copy(block, half, i % 2).start()

            return carry

        lax.fori_loop(0, n_tp, down, 0)

    def wide_of(ref, *at):
        return ref[at].astype(jnp.float32)

    def join_cores(block, half):
        wait_bytes(parts_in.at[block, :, span_of(half)], part_recv.at[block, half])
        for sub in range(subs):
            at = sub_of(half, sub)
            away = wide_of(parts, block, opposite, at) + wide_of(parts_in, block, 1 - y, at)
            pair_out[block, at, :] = away.astype(jnp.bfloat16)
            pair_copy(block, half, sub).start()
        at = span_of(half)
        pair_keep[block, at, :] = wide_of(parts, block, tp, at) + wide_of(parts_in, block, y, at)

    def join_own_cores(k):
        zc, half = unit_at(k)
        join_cores(zc * x_size + x, half)

    def join_other_cores(k):
        zc, half = unit_at(k)
        join_cores(zc * x_size + (1 - x), half)

    def join_pair_other(k):
        zc, half = unit_at(k)
        block = zc * x_size + (1 - x)
        for sub in range(subs):
            at = sub_of(half, sub)
            pair_copy(block, half, sub).wait_recv()
            both = pair_keep[block, at, :] + wide_of(pair_in, block, at)
            side_out[zc, at, :] = both.astype(jnp.bfloat16)
            side_copy(zc, half, sub).start()

    def join_pair_own(k):
        zc, half = unit_at(k)
        block = zc * x_size + x
        for sub in range(subs):
            pair_copy(block, half, sub).wait_recv()
        at = span_of(half)
        total[zc, at, :] = pair_keep[block, at, :] + wide_of(pair_in, block, at)

    def join_sides(k):
        zc, half = unit_at(k)
        for sub in range(subs):
            at = sub_of(half, sub)
            side_copy(zc, half, sub).wait_recv()
            total[zc, at, :] += wide_of(side_in, zc, at)
            for side, end_z in enumerate((0, far_z)):

                @pl.when((~end) & goes_by_mid(end_z, zc) & (2 * z == zc + end_z))
                def _():
                    wait_bytes(mid_in.at[side, at], mid_recv.at[side, half, sub])
                    total[zc, at, :] += wide_of(mid_in, side, at)

            @pl.when(zc != z)
            def _():
                far_out[zc, at, :] = total[zc, at, :].astype(jnp.bfloat16)

            @pl.when((zc != z) & goes_by_mid(z, zc))
            def _():
                mid_copy(zc, half, sub).start()

            @pl.when((zc != z) & ~goes_by_mid(z, zc))
            def _():
                far_copy(zc, half, sub).start()

    units = nz * halves

    def take_first(k):
        z_next, half_next = unit_at(k)
        take(z_next, half_next, True, ZF)

    def take_rest(k):
        z_next, half_next = unit_at(k)
        take(z_next, half_next, True, XF)
        take(z_next, half_next, False, XF)

    def take_ahead(k):
        take_first(k)
        take_rest(k)

    def compute_own(k):
        zc, half = unit_at(k)
        block = zc * x_size + x

        @pl.when(k >= halves)
        def _():
            sibling_arrived(block, half)

        compute(block, half)

    def compute_other(k):
        zc, half = unit_at(k)
        block = zc * x_size + (1 - x)
        sibling_arrived(block, half)
        compute(block, half)

    def take_other(k):
        zc, half = unit_at(k)
        take(zc, half, False, ZF)

    compute_own(0)
    take(z, 0, False, XF)
    compute_own(1)
    join_own_cores(0)
    take_other(0)
    join_own_cores(1)
    compute_other(0)
    take(z, 1, False, XF)
    if units > halves:

        take_first(2)

        @pl.when(inner)
        def _():
            take_first(3)

    join_other_cores(0)
    take_other(1)
    join_pair_own(0)

    def sides(k, carry):
        join_sides(k)
        return carry

    def unit_body(k, carry):
        zc, half = unit_at(k)

        @pl.when(~inner)
        def _():
            take(zc, half, True, XF)

        compute_other(k - 1)

        @pl.when((~inner) & (k <= 3) & (k + 1 < units))
        def _():
            take_first(k + 1)

        @pl.when(inner & (k == 2))
        def _():
            take_rest(2)
            take_rest(3)

        compute_own(k)
        join_other_cores(k - 1)

        @pl.when(~inner)
        def _():
            take(zc, half, False, XF)

        for at, ahead in ((2, (4, 7)), (3, (5,)), (4, (6,))) if nz > 3 else ((2, (4, 5)),):

            @pl.when(inner & (k == at))
            def _():
                for unit in ahead:
                    take_ahead(unit)

        if units > 8:

            @pl.when(inner & (k >= 6) & (k + 2 < units))
            def _():
                take_ahead(k + 2)

        take_other(k)
        join_own_cores(k)

        @pl.when((~inner) & (k > 3) & (k + 1 < units))
        def _():
            take_first(k + 1)

        join_pair_other(k - 2)

        @pl.when(k < units - 1)
        def _():
            join_pair_own(k - 1)

        @pl.when((~inner) & (k >= 3))
        def _():
            join_sides(k - 3)

        @pl.when(inner & (k >= 6) & (k != 7))
        def _():
            join_sides(k - 4)

        @pl.when(inner & (k >= 6) & (k == units - 1))
        def _():
            join_sides(k - 3)

        return carry

    lax.fori_loop(halves, units, unit_body, 0)
    compute_other(units - 1)
    join_other_cores(units - 1)
    if units > halves:
        join_pair_own(units - 2)
    join_pair_other(units - 2)

    @pl.when(inner)
    def _():
        lax.fori_loop(0, halves, sides, 0)
        if units <= 6:
            lax.fori_loop(max(units - 4, halves), units - 3, sides, 0)

    if units > halves:
        join_sides(units - 3)

        if units > 7:

            @pl.when(inner)
            def _():
                join_sides(3)

    join_pair_own(units - 1)
    join_pair_other(units - 1)
    join_sides(units - 2)
    join_sides(units - 1)

    for side in range(2):

        @pl.when(sp < n_sp - 1 if side == 0 else sp > 0)
        def _():
            wait_bytes(pool_edges.at[:, side], edge_send.at[side])

    for i, ref in enumerate(front_all):
        wait_bytes(ref.at[others], front_send.at[i])
    wait_bytes(route_all.at[pl.ds(0, n_sp - 1)], route_send.at[0])
    ag_sent()
    wait_bytes(parts_in, part_send.at[0])
    wait_bytes(pair_out, pair_send.at[0])
    wait_bytes(side_out, side_send.at[0])

    for at_z in range(nz):
        direct = [
            i
            for i in range(nz)
            if i != at_z and not (i in (0, far_z) and abs(i - at_z) == 2)
        ]

        @pl.when(z == at_z)
        def _():
            if direct:
                wait_bytes(far_in.at[pl.ds(0, len(direct))], far_recv.at[0])
            for i in direct:
                total[at_z] += far_in[i].astype(jnp.float32)

    combined = total[z]

    own_squares = jnp.sum(combined * combined, axis=1, keepdims=True)
    squares[tp] = jnp.broadcast_to(own_squares, (rows, 128)).T[:8]

    def squares_copy(d):
        return remote(
            squares.at[tp], squares.at[tp], sq_send.at[0], sq_recv.at[0], sp, (tp + d) % n_tp
        )

    for d in range(1, n_tp):
        squares_copy(d).start()
    wait_bytes(squares.at[others], sq_recv.at[0])
    summed = squares[0]
    for i in range(1, n_tp):
        summed += squares[i]
    row_scale = lax.rsqrt(summed[:1] / width + epsilon)
    row_scale = jnp.broadcast_to(row_scale, (128, rows)).T
    for i in range(cols // 128):
        lane = slice(i * 128, (i + 1) * 128)
        own = mixed[:, pl.ds(pl.multiple_of(tp * cols + i * 128, 128), 128)].astype(jnp.float32)
        out_ref[:, lane] = (own + total[z, :, lane] * row_scale * expert_norm[:, lane]).astype(
            jnp.bfloat16
        )

    wait_bytes(squares.at[others], sq_send.at[0])
    if nz > 1:
        wait_bytes(far_out.at[pl.ds(0, nz - 1)], far_send.at[0])


def gathered_shards(*args):
    pool_in, pool_norm, out_weight, stream = args[0], args[3], args[4], args[5]
    w_gate, w_down = args[10], args[14]
    n_sp, n_tp = lax.axis_size("sp"), lax.axis_size("tp")
    nz = n_sp // x_size
    rows, width = stream.shape
    n_hidden = w_gate.shape[2]
    cols = width // n_tp
    group_width = pool_in.shape[1]
    bf16, f32 = jnp.bfloat16, jnp.float32
    row_args = (2, 3, 6, 7, 15)
    args = [a.reshape(1, -1) if i in row_args else a for i, a in enumerate(args)]
    args[8], args[9] = args[8].T, args[9].T
    in_hbm = (4, 5, 10, 11, 14)
    in_specs = [
        pl.BlockSpec(memory_space=pl.ANY if i in in_hbm else pltpu.VMEM) for i in range(len(args))
    ]
    edge = 2 * reach_rows
    route_rows = -(-n_sp // 8) * 8
    dma = pltpu.SemaphoreType.DMA
    scratch = [
        pltpu.VMEM((n_sp, rows, width), bf16),
        pltpu.VMEM((width, n_hidden), bf16),
        pltpu.VMEM((width, n_hidden), bf16),
        pltpu.VMEM((n_hidden, width), bf16),
        pltpu.VMEM(out_weight.shape, bf16),
        pltpu.VMEM((rows, width), bf16),
        pltpu.VMEM((n_tp, rows, group_width), bf16),
        pltpu.VMEM((n_tp, 2, edge, group_width), bf16),
        pltpu.VMEM((n_tp, group_width, group_width), bf16),
        pltpu.VMEM((n_tp, 1, group_width), f32),
        pltpu.VMEM((n_tp, rows + 2 * reach_rows, group_width), f32),
        pltpu.VMEM((rows, n_tp * group_width), bf16),
        pltpu.VMEM((rows, width), f32),
        pltpu.VMEM((rows, width), bf16),
        pltpu.VMEM((n_sp, route_rows, rows), f32),
        pltpu.VMEM((rows // halves, n_hidden), bf16),
        pltpu.VMEM((n_sp, n_tp, rows, cols), bf16),
        pltpu.VMEM((n_sp, n_tp // core_count, rows, cols), bf16),
        pltpu.VMEM((n_sp, rows, cols), bf16),
        pltpu.VMEM((n_sp, rows, cols), f32),
        pltpu.VMEM((n_sp, rows, cols), bf16),
        pltpu.VMEM((nz, rows, cols), bf16),
        pltpu.VMEM((nz, rows, cols), bf16),
        pltpu.VMEM((nz, rows, cols), f32),
        pltpu.VMEM((nz, rows, cols), bf16),
        pltpu.VMEM((nz, rows, cols), bf16),
        pltpu.VMEM((2, rows, cols), bf16),
        pltpu.VMEM((n_tp, 8, rows), f32),
        dma((5,)),
        dma((4, 3)),
        dma((n_sp, halves, 3)),
        dma((3,)),
        dma((3, 3)),
        dma((2,)),
        dma((2,)),
        dma((1,)),
        dma((1,)),
        dma((1,)),
        dma((n_sp, halves)),
        dma((1,)),
        dma((n_sp, halves, subs)),
        dma((1,)),
        dma((nz, halves, subs)),
        dma((1,)),
        dma((1,)),
        dma((2, halves, subs)),
        dma((1,)),
        dma((1,)),
    ]
    return pl.pallas_call(
        functools.partial(layer_kernel, nz),
        out_shape=jax.ShapeDtypeStruct((rows, cols), bf16),
        in_specs=in_specs,
        out_specs=pl.BlockSpec(memory_space=pltpu.VMEM),
        scratch_shapes=scratch,
        compiler_params=pltpu.CompilerParams(
            collective_id=0, has_side_effects=True, vmem_limit_bytes=vmem_limit
        ),
        name="layer",
    )(*args)


def shards(*args):
    pool_in, out_weight, stream, w_gate = args[0], args[4], args[5], args[10]
    n_sp, n_tp = lax.axis_size("sp"), lax.axis_size("tp")
    rows, width = stream.shape
    cols, n_hidden = width // n_tp, w_gate.shape[2]
    slots = n_sp * rows * (2 * width + (2 + 1 + 1 + 2 + 1) * 2 * cols + 2 * width + 2 * width)
    fixed = 2 * (3 * width * n_hidden + out_weight.size) + 10 * rows * width
    fits = slots + fixed < vmem_limit * 9 // 10
    shaped = (
        n_tp == 2 * core_count
        and n_sp % x_size == 0
        and w_gate.shape[0] == 1
        and rows % (128 * halves) == 0
        and width % (128 * first_share[0]) == 0
        and cols % 128 == 0
        and n_hidden % 256 == 0
        and pool_in.shape[1] == 128
        and n_sp <= 128
    )
    return (gathered_shards if fits and shaped else routed_shards)(*args)


def solution(mesh):
    in_specs = (
        P("sp", "tp"),
        P("tp", None, None),
        P("tp"),
        P(),
        P(),
        P("sp", None),
        P(),
        P(),
        P("sp", None),
        P("sp", None),
        P("sp", None, "tp"),
        P("sp", None, "tp"),
        P("sp", "tp"),
        P("sp", "tp"),
        P("sp", "tp", None),
        P("tp"),
    )
    out_specs = P("sp", "tp")
    return jax.shard_map(shards, mesh=mesh, in_specs=in_specs, out_specs=out_specs, check_vma=False)
```
